32 devices in a mesh: grp: 2 (over y), sp: 4 (over z), tp: 4 (over x, core).
Axes of the slice: x: 2, y: 2, z: 4, core: 2. Of those that a mesh axis runs over, the one named last changes fastest.
Arguments:
- target: bfloat16 [1024, 2048], P(('grp', 'sp', 'tp')), parts along dimension 0, may hold values from -6 to 6
- source: bfloat16 [8192, 2048], P(('grp', 'sp', 'tp')), parts along dimension 0, may hold values from -6 to 6
- norm_gain: float32 [2048], replicated, may hold values from 0.1 to 1.9
- query_weight: bfloat16 [2048, 2048], P(None, 'tp'), may hold values from -0.125 to 0.125
- key_weight: bfloat16 [2048, 256], replicated, may hold values from -0.125 to 0.125
- value_weight: bfloat16 [2048, 256], replicated, may hold values from -0.125 to 0.125
- output_weight: bfloat16 [2048, 2048], P('tp'), may hold values from -0.125 to 0.125
- saved_out: bfloat16 [1024, 2048], P(('grp', 'sp'), 'tp'), parts along dimension 0, may hold values from -3 to 3
- log_shift: float32 [16, 1024], P('tp', ('grp', 'sp')), parts along dimension 1, may hold values from 0 to 2
- out_grad: bfloat16 [1024, 2048], P(('grp', 'sp', 'tp')), parts along dimension 0, may hold values from -48 to 48
Outputs:
- target_grad: float32 [1024, 2048], P(('grp', 'sp', 'tp')), parts along dimension 0
- source_grad: float32 [8192, 2048], P(('grp', 'sp', 'tp')), parts along dimension 0
- query_weight_grad: float32 [4096, 2048], P(('grp', 'sp'), 'tp'), parts along dimension 0
The draws below stay inside these ranges and needn't reach their ends.
There are 2 independent parts, one for each index of `grp`. The reference program is written for one: setup_inputs(seed, part) draws one part's arguments, and reference() takes and returns one part's arrays. A program takes and returns all parts, laid end to end along the dimension named above; an argument that names none is the same for every part. Nothing has to cross between parts.
All inputs are finite; a program needn't handle non-finite values.
Results may differ from the reference program's by a relative error of at most 0.02.
Values may be sent and summed in bfloat16 or wider, within the bound.
A program may use at most 64 MiB of HBM per device.

```python
import jax
import jax.numpy as jnp
from jax import lax

D = 2048
HEADS = 16
HEAD_DIM = 128
KV_HEADS = 2
SRC = 4096
TGT = 512


def shard_levels(stream_key, extent, shards, low, top_value):
    def one(axis_at, shards_of):
        steps = jax.random.uniform(jax.random.fold_in(jax.random.fold_in(stream_key, 6), axis_at), (shards_of,), jnp.float32, low / len(shards), top_value / len(shards))
        return jnp.repeat(jnp.exp(steps), extent[axis_at] // shards_of).reshape((-1,) + (1,) * (len(extent) - axis_at - 1))

    gain = one(*shards[0])
    for cut in shards[1:]:
        gain = gain * one(*cut)
    return gain


def centred(rng, shape, spread, reach, pieces=(), kind=jnp.bfloat16):
    loudness = shard_levels(rng, shape, pieces, -0.22, 0.18) if pieces else 1.0
    entries = jax.random.normal(rng, shape, jnp.float32) * spread * loudness
    return jnp.minimum(jnp.maximum(entries, -reach), reach).astype(kind)


def setup_inputs(seed: int = 0, part: int = 0) -> dict:
    splits = jax.random.split(jax.random.key(seed), 11)
    part_splits = jax.random.split(jax.random.fold_in(splits[10], part), 11)
    target = centred(part_splits[0], (TGT, D), 1.0, 6.0, ((0, 16),))
    source = centred(part_splits[1], (SRC, D), 1.0, 6.0, ((0, 16),))
    norm_gain = jnp.clip(1.0 + 0.18 * jax.random.normal(splits[2], (D,), jnp.float32), 0.1, 1.9)
    query_weight = centred(splits[3], (D, HEADS * HEAD_DIM), D ** -0.5, 0.125, ((1, 4),))
    key_weight = centred(splits[4], (D, KV_HEADS * HEAD_DIM), D ** -0.5, 0.125)
    value_weight = centred(splits[5], (D, KV_HEADS * HEAD_DIM), D ** -0.5, 0.125)
    output_weight = centred(splits[6], (HEADS * HEAD_DIM, D), (HEADS * HEAD_DIM) ** -0.5, 0.125, ((0, 4),))
    saved_out = centred(part_splits[7], (TGT, HEADS * HEAD_DIM), 0.5, 3.0, ((0, 4), (1, 4)))
    log_shift = jnp.clip(2.0 * jax.random.uniform(part_splits[8], (HEADS, TGT), jnp.float32) ** shard_levels(part_splits[8], (HEADS, TGT), ((0, 4), (1, 4)), -0.2, 0.2), 0.0, 2.0)
    out_grad = centred(part_splits[9], (TGT, D), 8.0, 48.0, ((0, 16),))
    return dict(target=target, source=source, norm_gain=norm_gain, query_weight=query_weight, key_weight=key_weight, value_weight=value_weight, output_weight=output_weight, saved_out=saved_out, log_shift=log_shift, out_grad=out_grad)


def reference(target, source, norm_gain, query_weight, key_weight, value_weight, output_weight, saved_out, log_shift, out_grad):
    group_size = HEADS // KV_HEADS
    factor = HEAD_DIM ** (-0.5)
    offset = jnp.log(jnp.float32(SRC))
    target_wide = target.astype(jnp.float32)
    root_mean = jnp.sqrt(lax.optimization_barrier(jnp.mean(target_wide * target_wide, axis=1, keepdims=True)) + 1e-06)
    normed = (target_wide / root_mean * norm_gain).astype(jnp.bfloat16)
    queries = jnp.dot(normed, query_weight, preferred_element_type=jnp.float32).astype(jnp.bfloat16)
    key_rows = jnp.dot(source, key_weight, preferred_element_type=jnp.float32).astype(jnp.bfloat16)
    values = jnp.dot(source, value_weight, preferred_element_type=jnp.float32).astype(jnp.bfloat16)
    out_back = jnp.dot(out_grad, output_weight.T, preferred_element_type=jnp.float32).astype(jnp.bfloat16)
    products = out_back.astype(jnp.float32) * saved_out.astype(jnp.float32)
    drop_term = lax.optimization_barrier(jnp.sum(products.reshape(TGT, HEADS, HEAD_DIM), axis=2))

    def one_head(head_id):
        pair_index = head_id // group_size
        query_head = lax.dynamic_slice_in_dim(queries, head_id * HEAD_DIM, HEAD_DIM, 1)
        back_head = lax.dynamic_slice_in_dim(out_back, head_id * HEAD_DIM, HEAD_DIM, 1)
        key_head = lax.dynamic_slice_in_dim(key_rows, pair_index * HEAD_DIM, HEAD_DIM, 1)
        value_head = lax.dynamic_slice_in_dim(values, pair_index * HEAD_DIM, HEAD_DIM, 1)
        shift_row = lax.dynamic_index_in_dim(log_shift, head_id, 0, keepdims=False)
        drop_row = lax.dynamic_index_in_dim(drop_term, head_id, 1, keepdims=False)
        scores = jnp.dot(query_head, key_head.T, preferred_element_type=jnp.float32) * factor
        prob = jnp.exp(scores - shift_row[:, None] - offset)
        prob_grad = jnp.dot(back_head, value_head.T, preferred_element_type=jnp.float32)
        score_grad = (prob * (prob_grad - drop_row[:, None]) * factor).astype(jnp.bfloat16)
        prob_low = prob.astype(jnp.bfloat16)
        query_part = jnp.dot(score_grad, key_head, preferred_element_type=jnp.float32)
        key_part = jnp.dot(score_grad.T, query_head, preferred_element_type=jnp.float32)
        value_part = jnp.dot(prob_low.T, back_head, preferred_element_type=jnp.float32)
        return (query_part, key_part, value_part)
    head_ids = jnp.arange(HEADS, dtype=jnp.int32)
    query_all, key_all, value_all = lax.map(one_head, head_ids)
    query_grad = jnp.transpose(query_all, (1, 0, 2)).reshape(TGT, HEADS * HEAD_DIM).astype(jnp.bfloat16)
    key_sum = lax.optimization_barrier(jnp.sum(key_all.reshape(KV_HEADS, group_size, SRC, HEAD_DIM), axis=1))
    value_sum = lax.optimization_barrier(jnp.sum(value_all.reshape(KV_HEADS, group_size, SRC, HEAD_DIM), axis=1))
    key_grad = jnp.transpose(key_sum, (1, 0, 2)).reshape(SRC, KV_HEADS * HEAD_DIM).astype(jnp.bfloat16)
    value_grad = jnp.transpose(value_sum, (1, 0, 2)).reshape(SRC, KV_HEADS * HEAD_DIM).astype(jnp.bfloat16)
    source_grad = jnp.dot(key_grad, key_weight.T, preferred_element_type=jnp.float32) + jnp.dot(value_grad, value_weight.T, preferred_element_type=jnp.float32)
    normed_grad = jnp.dot(query_grad, query_weight.T, preferred_element_type=jnp.float32)
    scaled_grad = normed_grad * norm_gain
    target_grad = scaled_grad / root_mean - target_wide * lax.optimization_barrier(jnp.mean(scaled_grad * target_wide, axis=1, keepdims=True)) / root_mean ** 3
    query_weight_grad = jnp.dot(normed.T, query_grad, preferred_element_type=jnp.float32)
    return (target_grad, source_grad, query_weight_grad)
```

```python
import functools
import math

import jax
import jax.numpy as jnp
from jax import lax
from jax.experimental import pallas as pl
from jax.experimental.pallas import tpu as pltpu
from jax.sharding import PartitionSpec as P

HEADS = 16
HEAD_DIM = 128
KV_HEADS = 2
LOG2E = 1.4426950408889634
BF16 = jnp.bfloat16
F32 = jnp.float32


def rows_split(sp_count):
    keys = 2 if sp_count % 2 == 0 else 1
    while keys * keys * 4 <= sp_count:
        keys *= 2
    return keys, sp_count // keys


def dot_nt(a, b):
    return lax.dot_general(a, b, (((1,), (1,)), ((), ())), preferred_element_type=F32)


def dot_tn(a, b):
    return lax.dot_general(a, b, (((0,), (0,)), ((), ())), preferred_element_type=F32)


def flat_rows(block):
    count = block.shape[-2]
    shape = (-1, block.shape[-1])
    if count % 16:
        return block.astype(F32).reshape(shape).astype(BF16)
    return block.reshape(shape)


def kernel(
    sp_count,
    tp_count,
    log_rows,
    target,
    source,
    norm_gain,
    query_weight,
    key_weight,
    value_weight,
    output_weight,
    saved_out,
    log_shift,
    out_grad,
    target_grad,
    source_grad,
    query_weight_grad,
    tgt,
    src,
    gain,
    wq,
    wkv,
    wo,
    saved,
    shift,
    nbuf,
    obuf,
    kvown,
    kvbuf,
    qob,
    stat,
    nall,
    kacc,
    qacc,
    qfull,
    qsend,
    qrecv,
    qgall,
    ngf,
    ngs,
    ngr,
    ngx,
    ngin,
    kvs,
    kvr,
    kz,
    kzr,
    kfin,
    fin,
    ksum,
    in_sem,
    send_sem,
    recv_sem,
):
    nA, nB, nS, nT = kvbuf.shape[0], qob.shape[0], sp_count, tp_count
    nX = nT // 2
    nR = nT // KV_HEADS
    nr, width = tgt.shape
    sr = src.shape[0]
    lh = shift.shape[0]
    tr = saved.shape[0]
    trx = tr // nX
    ds_width = width // nS
    factor = HEAD_DIM ** (-0.5)
    s = lax.axis_index("sp")
    t = lax.axis_index("tp")
    x, c = t // 2, t % 2
    other = 1 - c
    part, pair = t % nR, t // nR
    zh, zl = s % nA, s // nA

    pending = []
    counts = {"send": 0, "recv": 0, "in": 0}

    def take(kind, n=1):
        first = counts[kind]
        counts[kind] += n
        return first

    def remote(src_ref, dst_ref, recv, where, keep=True):
        copy = pltpu.make_async_remote_copy(
            src_ref=src_ref,
            dst_ref=dst_ref,
            send_sem=send_sem.at[take("send")],
            recv_sem=recv_sem.at[recv],
            device_id=where,
            device_id_type=pl.DeviceIdType.MESH,
        )
        if keep:
            copy.start()
            pending.append(copy)
        return copy

    def arrive(dst_ref, recv, where):
        pltpu.make_async_remote_copy(
            src_ref=dst_ref,
            dst_ref=dst_ref,
            send_sem=send_sem.at[0],
            recv_sem=recv_sem.at[recv],
            device_id=where,
            device_id_type=pl.DeviceIdType.MESH,
        ).wait_recv()

    def fetch(src_ref, dst_ref):
        copy = pltpu.make_async_copy(src_ref, dst_ref, in_sem.at[take("in")])
        copy.start()
        return copy

    def tp_at(xx, cc):
        return {"tp": xx * 2 + cc}

    sibling = tp_at(x, other)

    got_t = fetch(target, tgt)
    got_g = fetch(norm_gain, gain)
    got_o = fetch(out_grad, obuf.at[x, c])
    got_kv = [fetch(source, src)]
    for g in range(KV_HEADS):
        cols = pl.ds(g * HEAD_DIM, HEAD_DIM)
        got_kv.append(fetch(key_weight.at[:, cols], wkv.at[:, pl.ds(2 * g * HEAD_DIM, HEAD_DIM)]))
        got_kv.append(
            fetch(value_weight.at[:, cols], wkv.at[:, pl.ds((2 * g + 1) * HEAD_DIM, HEAD_DIM)])
        )
    got_q = [
        fetch(query_weight, wq),
        fetch(output_weight, wo),
        fetch(saved_out, saved),
        fetch(log_shift, shift),
    ]

    barrier = pltpu.get_barrier_semaphore()
    for k in range(1, nT):
        pl.semaphore_signal(
            barrier, 1, device_id={"tp": (t + k) % nT}, device_id_type=pl.DeviceIdType.MESH
        )
    for k in range(1, nS):
        pl.semaphore_signal(
            barrier, 1, device_id={"sp": (s + k) % nS}, device_id_type=pl.DeviceIdType.MESH
        )

    got_t.wait()
    got_g.wait()
    wide = tgt[...].astype(F32)
    root = jnp.sqrt(jnp.mean(wide * wide, axis=1, keepdims=True) + 1e-06)
    nbuf[x, c] = (wide / root * gain[...]).astype(BF16)
    got_o.wait()
    pl.semaphore_wait(barrier, nT - 1 + nS - 1)

    n_recv = take("recv", 2 * nX)
    o_recv = take("recv", 2 * nX)
    bufs = ((nbuf, n_recv), (obuf, o_recv))
    for k in range(1, nX):
        for buf, base in bufs:
            remote(buf.at[x, c], buf.at[x, c], base + k, tp_at((x + k) % nX, c))
    for buf, base in bufs:
        remote(buf.at[x, c], buf.at[x, c], base, sibling)

    for copy in got_kv:
        copy.wait()
    own = jnp.dot(src[...], wkv[...], preferred_element_type=F32).astype(BF16)
    for g in range(KV_HEADS):
        kvown[g] = own[:, 2 * g * HEAD_DIM : 2 * (g + 1) * HEAD_DIM]
    kvbuf[0, t] = kvown[pair]
    kv_recv = take("recv", 2 * nX)
    for k in range(1, nX):
        xx = (x + k) % nX
        remote(kvown.at[xx * 2 // nR], kvbuf.at[0, t], kv_recv + k, tp_at(xx, c))
    remote(kvown.at[pair], kvbuf.at[0, t], kv_recv, sibling)
    kz_recv = take("recv", 2 * nA * nX)

    def keys_along(a_x, slot):
        for a in range(1, nA):
            remote(
                kvbuf.at[0, slot],
                kvbuf.at[a, slot],
                kz_recv + a * nX + a_x,
                {"sp": zl * nA + (zh + a) % nA},
            )

    keys_along(0, t)

    got_q[-1].wait()
    for xx in range(nX):
        for h in range(lh):
            cols = slice(h * trx, (h + 1) * trx)
            row = (shift[h : h + 1, xx * trx : (xx + 1) * trx] + log_rows) * LOG2E
            stat[0, xx, 0:1, cols] = row
    q_recv = take("recv", 2 * nB * nX)
    st_recv = take("recv", nB * nX)

    def project(k):
        xx = (x + nX - k) % nX
        q_rows = jnp.dot(flat_rows(nbuf[xx]), wq[...], preferred_element_type=F32).astype(BF16)
        for h in range(lh):
            cols = slice(h * HEAD_DIM, (h + 1) * HEAD_DIM)
            qob[0, xx, 0, h * trx : (h + 1) * trx, :] = q_rows[:, cols]
        for b in range(1, nB):
            where = {"sp": (zl + b) % nB * nA + zh}
            remote(qob.at[0, xx, 0], qob.at[b, xx, 0], q_recv + b * nX + k, where)
        o_rows = dot_nt(flat_rows(obuf[xx]), wo[...]).astype(BF16)
        keep = saved[pl.ds(pl.multiple_of(xx * trx, trx), trx), :].astype(F32)
        lane = lax.broadcasted_iota(jnp.int32, (trx, HEAD_DIM), 1)
        drops = jnp.zeros((trx, HEAD_DIM), F32)
        for h in range(lh):
            cols = slice(h * HEAD_DIM, (h + 1) * HEAD_DIM)
            rows = slice(h * trx, (h + 1) * trx)
            qob[0, xx, 1, rows, :] = o_rows[:, cols]
            term = jnp.sum(o_rows[:, cols].astype(F32) * keep[:, cols], axis=1, keepdims=True)
            drops = jnp.where(lane == h, term, drops)
        if trx < HEAD_DIM:
            drops = jnp.concatenate([drops, jnp.zeros((HEAD_DIM - trx, HEAD_DIM), F32)], axis=0)
        drops = drops.T
        for h in range(lh):
            stat[0, xx, 1:2, h * trx : (h + 1) * trx] = drops[h : h + 1, :trx]
        for b in range(1, nB):
            where = {"sp": (zl + b) % nB * nA + zh}
            remote(stat.at[0, xx], stat.at[b, xx], st_recv + b * nX + k, where)
            remote(qob.at[0, xx, 1], qob.at[b, xx, 1], q_recv + (nB + b) * nX + k, where)

    for copy in got_q[:-1]:
        copy.wait()
    for buf, base in bufs:
        arrive(buf.at[x, other], base, sibling)
    project(0)

    slots = [(b, a) for b in range(nB) for a in range(nA)]
    nz_recv = take("recv", nS * (1 + 2 * nX))

    def ahead(b, a):
        return (zl + b) % nB * nA + (zh + a) % nA

    def behind(b, a):
        return (zl + nB - b) % nB * nA + (zh + nA - a) % nA

    for n, (b, a) in enumerate(slots[1:], 1):
        to = ahead(b, a)
        cols = pl.ds(pl.multiple_of(to * ds_width, HEAD_DIM), ds_width)
        remote(nbuf.at[x, c, :, cols], nall.at[n, x, c], nz_recv + n, {"sp": to})

    for k in range(1, nX):
        xx = (x + nX - k) % nX
        for buf, base in bufs:
            arrive(buf.at[xx, c], base + k, tp_at(xx, c))
            remote(buf.at[xx, c], buf.at[xx, c], base + nX + k, sibling)
    for k in range(1, nX):
        xx = (x + nX - k) % nX
        for buf, base in bufs:
            arrive(buf.at[xx, other], base + nX + k, sibling)
        project(k)

    for k in range(1, nX):
        xx = (x + nX - k) % nX
        slot = xx * 2 + c
        arrive(kvbuf.at[0, slot], kv_recv + k, tp_at(xx, c))
        keys_along(k, slot)
        remote(kvbuf.at[0, slot], kvbuf.at[0, slot], kv_recv + nX + k, sibling)
    nall[0] = nbuf[:, :, :, pl.ds(pl.multiple_of(s * ds_width, HEAD_DIM), ds_width)]
    for k in range(1, nX):
        xx = (x + nX - k) % nX
        arrive(kvbuf.at[0, xx * 2 + other], kv_recv + nX + k, sibling)
    arrive(kvbuf.at[0, x * 2 + other], kv_recv, sibling)

    def attend(b, k, a):
        xx = (x + nX - k) % nX

        def step(i, carry):
            keys = kvbuf[a, i, :, :HEAD_DIM]
            values = kvbuf[a, i, :, HEAD_DIM:]
            queries = qob[b, xx, 0]
            backs = qob[b, xx, 1]
            score = dot_nt(keys, queries)
            prob = jnp.exp2(score * (factor * LOG2E) - stat[b, xx, 0:1, :])
            grad = (prob * (dot_nt(values, backs) - stat[b, xx, 1:2, :])).astype(BF16)
            key_part = jnp.dot(grad, queries, preferred_element_type=F32)
            value_part = jnp.dot(prob.astype(BF16), backs, preferred_element_type=F32)
            if b == 0 and k == 0:
                kacc[a, i, :, :HEAD_DIM] = key_part
                kacc[a, i, :, HEAD_DIM:] = value_part
            else:
                kacc[a, i, :, :HEAD_DIM] += key_part
                kacc[a, i, :, HEAD_DIM:] += value_part
            qacc[b, xx] += dot_tn(keys, grad)
            return carry

        lax.fori_loop(0, nT, step, 0, unroll=min(nT, 4))

    qs_recv = take("recv", nB * nB * nX)

    def send_queries(b, k):
        xx = (x + nX - k) % nX
        block = (qacc[b, xx] * factor).T
        qfull[b, xx] = block
        qsend[b, xx] = block.astype(BF16)
        for n in range(1, nB):
            slot = (n + b) % nB
            remote(
                qsend.at[b, xx],
                qrecv.at[n, slot, xx],
                qs_recv + (n * nB + slot) * nX + k,
                {"sp": (zl + n) % nB * nA + zh},
            )

    qacc[...] = jnp.zeros(qacc.shape, F32)
    for k in range(nX):
        attend(0, k, 0)

    for a in range(1, nA):
        for a_x in range(nX):
            slot = (x + nX - a_x) % nX * 2 + c
            idx = kz_recv + a * nX + a_x
            where = {"sp": zl * nA + (zh + nA - a) % nA}
            arrive(kvbuf.at[a, slot], idx, where)
            remote(kvbuf.at[a, slot], kvbuf.at[a, slot], idx + nA * nX, sibling)
        if a == 1:
            for n, (b, aa) in enumerate(slots[1:], 1):
                arrive(nall.at[n, x, c], nz_recv + n, {"sp": behind(b, aa)})
                base = nz_recv + nS + n * 2 * nX
                for j in range(1, nX):
                    remote(nall.at[n, x, c], nall.at[n, x, c], base + j, tp_at((x + j) % nX, c))
                remote(nall.at[n, x, c], nall.at[n, x, c], base, sibling)
        for a_x in range(nX):
            slot = (x + nX - a_x) % nX * 2 + other
            arrive(kvbuf.at[a, slot], kz_recv + a * nX + a_x + nA * nX, sibling)
        for k in range(nX):
            attend(0, k, a)
            if a == nA - 1:
                send_queries(0, k)

    kr_recv = take("recv", nA * nR)

    def send_keys(a):
        def convert(i, carry):
            kvs[a, i, :, :HEAD_DIM] = (kacc[a, i, :, :HEAD_DIM] * factor).astype(BF16)
            kvs[a, i, :, HEAD_DIM:] = kacc[a, i, :, HEAD_DIM:].astype(BF16)
            return carry

        lax.fori_loop(0, nT, convert, 0)
        for k in range(1, nR):
            to = (part + k) % nR
            remote(
                kvs.at[a, pl.ds(to * KV_HEADS, KV_HEADS)],
                kvr.at[k, a],
                kr_recv + a * nR + k,
                {"tp": pair * nR + to},
            )

    for k in range(nX):
        for b in range(1, nB):
            xx = (x + nX - k) % nX
            where = {"sp": (zl + nB - b) % nB * nA + zh}
            arrive(stat.at[b, xx], st_recv + b * nX + k, where)
            arrive(qob.at[b, xx, 0], q_recv + b * nX + k, where)
            arrive(qob.at[b, xx, 1], q_recv + (nB + b) * nX + k, where)
            last = k == nX - 1 and b == nB - 1
            for a in range(nA - 1, -1, -1):
                attend(b, k, a)
                if a == 0:
                    send_queries(b, k)
                if last:
                    send_keys(a)

    qg_recv = take("recv", nS)

    def finish_queries(b):
        for k in range(nX):
            xx = (x + nX - k) % nX
            total = qfull[b, xx]
            for n in range(1, nB):
                base = qs_recv + (n * nB + b) * nX + k
                arrive(qrecv.at[n, b, xx], base, {"sp": (zl + nB - n) % nB * nA + zh})
                total += qrecv[n, b, xx].astype(F32)
            total = total.astype(BF16)
            rows = pl.ds(pl.multiple_of(xx * trx, trx), trx)
            for h in range(lh):
                cols = slice(h * HEAD_DIM, (h + 1) * HEAD_DIM)
                qgall[b * nA, rows, cols] = total[h * trx : (h + 1) * trx, :]
        for a in range(1, nA):
            remote(
                qgall.at[b * nA],
                qgall.at[b * nA + a],
                qg_recv + b * nA + a,
                {"sp": zl * nA + (zh + a) % nA},
            )

    def portion(a, i):
        block = kacc[a, part * KV_HEADS + i]
        k_lane = lax.broadcasted_iota(jnp.int32, block.shape, 1) < HEAD_DIM
        block = jnp.where(k_lane, block * factor, block)
        for k in range(1, nR):
            block += kvr[k, a, i].astype(F32)
        return block

    ka_recv = take("recv", nA)
    for a in range(nA - 1, 0, -1):
        for k in range(1, nR):
            where = {"tp": pair * nR + (part + nR - k) % nR}
            arrive(kvr.at[k, a], kr_recv + a * nR + k, where)
        for i in range(KV_HEADS):
            kz[a, i] = portion(a, i).astype(BF16)
        remote(kz.at[a], kzr.at[a], ka_recv + a, {"sp": zl * nA + (zh + nA - a) % nA})

    for b in range(1, nB):
        finish_queries(b)

    for n, (b, a) in enumerate(slots[1:], 1):
        base = nz_recv + nS + n * 2 * nX
        for j in range(1, nX):
            xx = (x + nX - j) % nX
            arrive(nall.at[n, xx, c], base + j, tp_at(xx, c))
            remote(nall.at[n, xx, c], nall.at[n, xx, c], base + nX + j, sibling)

    finish_queries(0)

    step_cols = min(512, width)
    for i in range(width // step_cols):
        cols = slice(i * step_cols, (i + 1) * step_cols)
        share = dot_nt(qgall[0], wq[cols, :])
        ngf[:, :, :, cols] = share.reshape(nX, 2, nr, step_cols)
    for xx in range(nX):
        ngs[xx] = ngf[xx, other].astype(BF16)
    ng_recv = take("recv", nX)
    remote(ngs, ngr, ng_recv, sibling)

    for k in range(1, nR):
        arrive(kvr.at[k, 0], kr_recv + k, {"tp": pair * nR + (part + nR - k) % nR})
    for i in range(KV_HEADS):
        ksum[i] = portion(0, i)

    arrive(ngr, ng_recv, sibling)
    for k in range(1, nX):
        xx = (x + k) % nX
        ngx[k] = (ngf[xx, c] + ngr[xx].astype(F32)).astype(BF16)
        remote(ngx.at[k], ngin.at[k], ng_recv + k, tp_at(xx, c))

    for a in range(1, nA):
        arrive(kzr.at[a], ka_recv + a, {"sp": zl * nA + (zh + a) % nA})
    f_recv = take("recv", KV_HEADS)
    owner_sends = []
    for i in range(KV_HEADS):
        block = ksum[i]
        for a in range(1, nA):
            block += kzr[a, i].astype(F32)
        kfin[i] = block.astype(BF16)
        owner = part * KV_HEADS + i
        copy = remote(kfin.at[i], fin.at[pair], f_recv + pair, {"tp": owner}, keep=False)
        owner_sends.append((owner, copy))

        @pl.when(owner != t)
        def _():
            copy.start()

        @pl.when(owner == t)
        def _():
            fin[pair] = kfin[i]

    for n, (b, a) in enumerate(slots):
        if n:
            base = nz_recv + nS + n * 2 * nX
            arrive(nall.at[n, x, other], base, sibling)
            for j in range(1, nX):
                arrive(nall.at[n, (x + nX - j) % nX, other], base + nX + j, sibling)
    order = [b * nA for b in range(nB)] + [b * nA + a for b in list(range(1, nB)) + [0] for a in range(1, nA)]
    for n in order:
        if n % nA:
            arrive(qgall.at[n], qg_recv + n, {"sp": zl * nA + (zh + nA - n % nA) % nA})
        piece = dot_tn(flat_rows(nall[n]), qgall[n])
        if n == 0:
            query_weight_grad[...] = piece
        else:
            query_weight_grad[...] += piece

    grad = ngf[x, c] + ngr[x].astype(F32)
    for k in range(1, nX):
        arrive(ngin.at[k], ng_recv + k, tp_at((x + nX - k) % nX, c))
        grad += ngin[k].astype(F32)
    scaled = grad * gain[...]
    wide = tgt[...].astype(F32)
    root = jnp.sqrt(jnp.mean(wide * wide, axis=1, keepdims=True) + 1e-06)
    target_grad[...] = scaled / root - wide * jnp.mean(scaled * wide, axis=1, keepdims=True) / (
        root * root * root
    )

    for g in range(KV_HEADS):
        giver = g * nR + t // KV_HEADS

        @pl.when(giver != t)
        def _():
            arrive(fin.at[g], f_recv + g, {"tp": giver})

    for i in range(width // step_cols):
        rows = pl.ds(i * step_cols, step_cols)
        part_sum = dot_nt(fin[0], wkv[rows, 0 : 2 * HEAD_DIM])
        for g in range(1, KV_HEADS):
            part_sum += dot_nt(fin[g], wkv[rows, 2 * g * HEAD_DIM : 2 * (g + 1) * HEAD_DIM])
        source_grad[:, rows] = part_sum

    for copy in pending:
        copy.wait_send()
    for owner, copy in owner_sends:

        @pl.when(owner != t)
        def _():
            copy.wait_send()


def square_kernel(
    log_rows,
    target,
    source,
    norm_gain,
    query_weight,
    key_weight,
    value_weight,
    output_weight,
    saved_out,
    log_shift,
    out_grad,
    target_grad,
    source_grad,
    query_weight_grad,
    tgt,
    src,
    gain,
    wq,
    wkv,
    wo,
    saved,
    shift,
    nbuf,
    obuf,
    kvown,
    kvbuf,
    kvpeer,
    qob,
    stat,
    nall,
    kacc,
    qacc,
    qfull,
    qsend,
    qrecv,
    qgall,
    ngf,
    ngs,
    ngr,
    ngx,
    ngin,
    kvs,
    kvr,
    kz,
    kzr,
    kfin,
    fin,
    in_sem,
    send_sem,
    recv_sem,
):
    nr, width = tgt.shape
    lh = shift.shape[0]
    tr = saved.shape[0]
    nS, nT = 4, 4
    trx = tr // 2
    ds_width = width // nS
    factor = HEAD_DIM ** (-0.5)
    s = lax.axis_index("sp")
    t = lax.axis_index("tp")
    x, c = t // 2, t % 2
    ox, other = 1 - x, 1 - c
    peer = s + 1 - 2 * (s % 2)
    far = (s + 2) % nS
    diag = (peer + 2) % nS
    sib = {"tp": x * 2 + other}
    across = {"tp": ox * 2 + c}
    to_peer = {"sp": peer}
    to_far = {"sp": far}
    to_diag = {"sp": diag}

    keys = {("fin", 0): 0, ("fin", 1): 1}
    counts = {"in": 0}

    def sem(*key):
        return keys.setdefault(key, len(keys))

    def fetch(src_ref, dst_ref):
        copy = pltpu.make_async_copy(src_ref, dst_ref, in_sem.at[counts["in"]])
        counts["in"] += 1
        copy.start()
        return copy

    got_t = fetch(target, tgt)
    got_g = fetch(norm_gain, gain)
    got_shift = fetch(log_shift, shift)
    got_o = fetch(out_grad, obuf.at[x, c])
    got_kv = [fetch(source, src)]
    for g in range(KV_HEADS):
        cols = pl.ds(g * HEAD_DIM, HEAD_DIM)
        got_kv.append(fetch(key_weight.at[:, cols], wkv.at[:, pl.ds(2 * g * HEAD_DIM, HEAD_DIM)]))
        got_kv.append(
            fetch(value_weight.at[:, cols], wkv.at[:, pl.ds((2 * g + 1) * HEAD_DIM, HEAD_DIM)])
        )
    got_q = fetch(query_weight, wq)
    got_w = fetch(output_weight, wo)
    got_saved = fetch(saved_out, saved)

    barrier = pltpu.get_barrier_semaphore()
    for k in range(1, nT):
        pl.semaphore_signal(
            barrier, 1, device_id={"tp": (t + k) % nT}, device_id_type=pl.DeviceIdType.MESH
        )
    for k in range(1, nS):
        pl.semaphore_signal(
            barrier, 1, device_id={"sp": (s + k) % nS}, device_id_type=pl.DeviceIdType.MESH
        )

    got_t.wait()
    got_g.wait()
    wide = tgt[...].astype(F32)
    root = jnp.sqrt(jnp.mean(wide * wide, axis=1, keepdims=True) + 1e-06)
    nbuf[x, c] = (wide / root * gain[...]).astype(BF16)
    got_o.wait()
    pl.semaphore_wait(barrier, nT - 1 + nS - 1)

    pending = []

    def remote(src_ref, dst_ref, key, where, keep=True):
        copy = pltpu.make_async_remote_copy(
            src_ref=src_ref,
            dst_ref=dst_ref,
            send_sem=send_sem.at[len(pending)],
            recv_sem=recv_sem.at[sem(*key) if isinstance(key, tuple) else key],
            device_id=where,
            device_id_type=pl.DeviceIdType.MESH,
        )
        if keep:
            copy.start()
        pending.append((copy, keep))
        return copy

    def arrive(dst_ref, key, where):
        pltpu.make_async_remote_copy(
            src_ref=dst_ref,
            dst_ref=dst_ref,
            send_sem=send_sem.at[0],
            recv_sem=recv_sem.at[sem(*key)],
            device_id=where,
            device_id_type=pl.DeviceIdType.MESH,
        ).wait_recv()

    def scope(name):
        return jax.named_scope(name)

    remote(nbuf.at[x, c], nbuf.at[x, c], ("n", "x"), across)
    remote(nbuf.at[x, c], nbuf.at[x, c], ("n", "s"), sib)
    remote(obuf.at[x, c], obuf.at[x, c], ("o", "s"), sib)
    remote(obuf.at[x, c], obuf.at[x, c], ("o", "x"), across)
    for copy in got_kv:
        copy.wait()
    with scope("kvproj"):
        own = jnp.dot(src[...], wkv[...], preferred_element_type=F32).astype(BF16)
        for g in range(KV_HEADS):
            kvown[g] = own[:, 2 * g * HEAD_DIM : 2 * (g + 1) * HEAD_DIM]
        kvbuf[0, t] = kvown[x]
    remote(kvown.at[x], kvbuf.at[0, t], ("kv", "s"), sib)
    remote(kvown.at[ox], kvbuf.at[0, t], ("kv", "x"), across)
    got_shift.wait()
    for k in range(2):
        xx = x if k == 0 else ox
        for h in range(lh):
            row = jnp.where(xx == 0, shift[h : h + 1, 0:trx], shift[h : h + 1, trx : 2 * trx])
            stat[0, k, 0:1, h * trx : (h + 1) * trx] = (row + log_rows) * LOG2E

    def send_far(ref, kind, k):
        remote(ref.at[0, k], ref.at[1, k], (kind, k), to_far)

    def send_part(i, kind, k):
        remote(qob.at[0, k, i], qob.at[1, k, i], (kind, k), to_far)

    def project_q(k):
        with scope(f"project_q{k}"):
            xx = x if k == 0 else ox
            rows = jnp.dot(flat_rows(nbuf[xx]), wq[...], preferred_element_type=F32).astype(BF16)
            for h in range(lh):
                cols = slice(h * HEAD_DIM, (h + 1) * HEAD_DIM)
                qob[0, k, 0, h * trx : (h + 1) * trx, :] = rows[:, cols]
        send_part(0, "q", k)

    def project_o(k):
        with scope(f"project_o{k}"):
            xx = x if k == 0 else ox
            o_rows = dot_nt(flat_rows(obuf[xx]), wo[...]).astype(BF16)
            for h in range(lh):
                cols = slice(h * HEAD_DIM, (h + 1) * HEAD_DIM)
                qob[0, k, 1, h * trx : (h + 1) * trx, :] = o_rows[:, cols]
        send_part(1, "ob", k)
        with scope(f"drop{k}"):
            keep = saved[pl.ds(pl.multiple_of(xx * trx, trx), trx), :].astype(F32)
            lane = lax.broadcasted_iota(jnp.int32, (trx, HEAD_DIM), 1)
            drops = jnp.zeros((trx, HEAD_DIM), F32)
            for h in range(lh):
                cols = slice(h * HEAD_DIM, (h + 1) * HEAD_DIM)
                term = jnp.sum(o_rows[:, cols].astype(F32) * keep[:, cols], axis=1, keepdims=True)
                drops = jnp.where(lane == h, term, drops)
            drops = jnp.concatenate([drops, jnp.zeros((HEAD_DIM - trx, HEAD_DIM), F32)], axis=0)
            drops = drops.T
            for h in range(lh):
                stat[0, k, 1:2, h * trx : (h + 1) * trx] = drops[h : h + 1, :trx]
        send_far(stat, "st", k)

    def need(k):
        with scope(f"w_q{k}"):
            arrive(qob.at[1, k, 0], ("q", k), to_far)
        with scope(f"w_ob{k}"):
            arrive(qob.at[1, k, 1], ("ob", k), to_far)
            arrive(stat.at[1, k], ("st", k), to_far)

    got = {"kacc": set(), "qacc": set()}

    def attend(v, k, a, g):
        with scope(f"attend_{v}{k}{a}{g}"):
            attend_rows(v, k, a, g)

    def attend_rows(v, k, a, g):
        pair = pl.ds(2 * (x if g == 0 else ox), 2)
        sr = kvbuf.shape[2]
        k_rows = kvbuf[a, pair, :, :HEAD_DIM].reshape(2 * sr, HEAD_DIM)
        v_rows = kvbuf[a, pair, :, HEAD_DIM:].reshape(2 * sr, HEAD_DIM)
        queries = qob[v, k, 0]
        backs = qob[v, k, 1]
        score = dot_nt(k_rows, queries)
        prob = jnp.exp2(score * (factor * LOG2E) - stat[v, k, 0:1, :])
        grad = (prob * (dot_nt(v_rows, backs) - stat[v, k, 1:2, :])).astype(BF16)
        key_part = jnp.dot(grad, queries, preferred_element_type=F32)
        value_part = jnp.dot(prob.astype(BF16), backs, preferred_element_type=F32)
        key_part = key_part.reshape(2, sr, HEAD_DIM)
        value_part = value_part.reshape(2, sr, HEAD_DIM)
        if (a, g) not in got["kacc"]:
            kacc[a, pair, :, :HEAD_DIM] = key_part
            kacc[a, pair, :, HEAD_DIM:] = value_part
        else:
            kacc[a, pair, :, :HEAD_DIM] += key_part
            kacc[a, pair, :, HEAD_DIM:] += value_part
        if (v, k) not in got["qacc"]:
            qacc[v, k] = dot_tn(k_rows, grad)
            got["qacc"].add((v, k))
        else:
            qacc[v, k] += dot_tn(k_rows, grad)
        got["kacc"].add((a, g))

    def query_part(v, k):
        return (qacc[v, k] * factor).T

    def send_keys(a):
        with scope(f"keys{a}"):
            for i in range(2):
                slot = 2 * other + i
                kvs[a, i, :, :HEAD_DIM] = (kacc[a, slot, :, :HEAD_DIM] * factor).astype(BF16)
                kvs[a, i, :, HEAD_DIM:] = kacc[a, slot, :, HEAD_DIM:].astype(BF16)
        remote(kvs.at[a], kvr.at[a], ("kp", a), sib)

    def key_sum(a, i):
        block = kacc[a, 2 * c + i]
        k_lane = lax.broadcasted_iota(jnp.int32, block.shape, 1) < HEAD_DIM
        return jnp.where(k_lane, block * factor, block) + kvr[a, i].astype(F32)

    def keys_back():
        with scope("w_kp1"):
            arrive(kvr.at[1], ("kp", 1), sib)
        with scope("kz"):
            for i in range(2):
                kz[i] = key_sum(1, i).astype(BF16)
        remote(kz, kzr, ("kz",), to_peer)

    def slice_sends():
        for v, where, to in ((2, to_peer, peer), (1, to_far, far), (3, to_diag, diag)):
            cols = pl.ds(pl.multiple_of(to * ds_width, HEAD_DIM), ds_width)
            remote(nbuf.at[x, c, :, cols], nall.at[v, x, c], ("na", v), where)

    def slice_from(v):
        return (None, to_far, to_peer, to_diag)[v]

    def slice_pass(v):
        with scope(f"w_na{v}"):
            arrive(nall.at[v, x, c], ("na", v), slice_from(v))
        remote(nall.at[v, x, c], nall.at[v, x, c], ("na", v, "x"), across)
        remote(nall.at[v, x, c], nall.at[v, x, c], ("na", v, "s"), sib)

    def slice_turn(v):
        with scope(f"w_nx{v}"):
            arrive(nall.at[v, ox, c], ("na", v, "x"), across)
        remote(nall.at[v, ox, c], nall.at[v, ox, c], ("na", v, "t"), sib)

    def slice_end(v):
        with scope(f"w_ns{v}"):
            arrive(nall.at[v, x, other], ("na", v, "s"), sib)
            arrive(nall.at[v, ox, other], ("na", v, "t"), sib)

    def total_rows(v, k):
        xx = x if k == 0 else ox
        return qgall.at[v, pl.ds(pl.multiple_of(xx * trx, trx), trx), :]

    pieces = []

    def weight_piece(v):
        with scope(f"piece{v}"):
            piece = dot_tn(flat_rows(nall[v]), qgall[v])
            if not pieces:
                query_weight_grad[...] = piece
            else:
                query_weight_grad[...] += piece
            pieces.append(v)

    step_cols = min(512, width)

    def normed_share():
        with scope("ng_share"):
            for i in range(width // step_cols):
                cols = slice(i * step_cols, (i + 1) * step_cols)
                share = dot_nt(qgall[0], wq[cols, :])
                ngf[:, :, :, cols] = share.reshape(2, 2, nr, step_cols)
            for xx in range(2):
                ngs[xx] = ngf[xx, other].astype(BF16)
        remote(ngs, ngr, ("ng", "s"), sib)

    def normed_cross():
        with scope("w_ngs"):
            arrive(ngr, ("ng", "s"), sib)
        ngx[...] = (ngf[ox, c] + ngr[ox].astype(F32)).astype(BF16)
        remote(ngx, ngin, ("ng", "x"), across)

    def normed_end():
        with scope("w_ngx"):
            arrive(ngin, ("ng", "x"), across)
        with scope("target"):
            grad = ngf[x, c] + ngr[x].astype(F32) + ngin[...].astype(F32)
            scaled = grad * gain[...]
            wide = tgt[...].astype(F32)
            root = jnp.sqrt(jnp.mean(wide * wide, axis=1, keepdims=True) + 1e-06)
            target_grad[...] = scaled / root - wide * jnp.mean(
                scaled * wide, axis=1, keepdims=True
            ) / (root * root * root)

    owner_sends = []

    def keys_out():
        with scope("w_kp0"):
            arrive(kvr.at[0], ("kp", 0), sib)
        with scope("w_kz"):
            arrive(kzr, ("kz",), to_peer)
        with scope("keys_out"):
            for i in range(2):
                block = key_sum(0, i) + kzr[i].astype(F32)
                kfin[i] = block.astype(BF16)
                owner = c * 2 + i
                copy = remote(kfin.at[i], fin.at[x], x, {"tp": owner}, keep=False)
                owner_sends.append((owner, copy))

                @pl.when(owner != t)
                def _():
                    copy.start()

                @pl.when(owner == t)
                def _():
                    fin[x] = kfin[i]

    def source_end():
        for g in range(KV_HEADS):
            giver = g * 2 + t // 2

            @pl.when(giver != t)
            def _():
                with scope("w_fin"):
                    arrive(fin.at[g], ("fin", g), {"tp": giver})

        with scope("source"):
            for i in range(width // step_cols):
                rows = pl.ds(i * step_cols, step_cols)
                part_sum = dot_nt(fin[0], wkv[rows, 0 : 2 * HEAD_DIM])
                for g in range(1, KV_HEADS):
                    part_sum += dot_nt(fin[g], wkv[rows, 2 * g * HEAD_DIM : 2 * (g + 1) * HEAD_DIM])
                source_grad[:, rows] = part_sum

    def pass_on(buf, kind):
        with scope(f"w_{kind}x"):
            arrive(buf.at[ox, c], (kind, "x"), across)
        remote(buf.at[ox, c], buf.at[ox, c], (kind, "t"), sib)

    def passed(buf, kind):
        with scope(f"w_{kind}t"):
            arrive(buf.at[ox, other], (kind, "t"), sib)

    def grad_out(b, k):
        with scope(f"dq_{b}{k}"):
            block = query_part(b, k)
            qfull[b, k] = block
            qsend[b, k] = block.astype(BF16)
        remote(qsend.at[b, k], qrecv.at[1 - b, k], ("dq", 1 - b, k), to_far)

    def total_out(b, k):
        with scope(f"w_dq{b}{k}"):
            arrive(qrecv.at[b, k], ("dq", b, k), to_far)
        with scope(f"total_{b}{k}"):
            total = (qfull[b, k] + qrecv[b, k].astype(F32)).astype(BF16)
            rows = pl.ds(pl.multiple_of((x if k == 0 else ox) * trx, trx), trx)
            for h in range(lh):
                cols = slice(h * HEAD_DIM, (h + 1) * HEAD_DIM)
                qgall[b, rows, cols] = total[h * trx : (h + 1) * trx, :]
        remote(total_rows(b, k), total_rows(2 + b, k), ("tot", b, k), to_peer)

    def total_in(b, k):
        with scope(f"w_tot{b}{k}"):
            arrive(total_rows(2 + b, k), ("tot", b, k), to_peer)

    def peer_keys(chip, kind):
        with scope(f"w_{kind}"):
            arrive(kvbuf.at[1, 2 * chip + c], (kind,), to_peer if chip is x else across)
        remote(kvbuf.at[1, 2 * chip + c], kvbuf.at[1, 2 * chip + c], (kind, "s"), sib)

    def peer_keys_end(chip, kind):
        with scope(f"w_{kind}s"):
            arrive(kvbuf.at[1, 2 * chip + other], (kind, "s"), sib)

    remote(kvown.at[x], kvbuf.at[1, t], ("ke",), to_peer)
    remote(kvown.at[ox], kvpeer, ("kp",), to_peer)
    with scope("w_ns"):
        arrive(nbuf.at[x, other], ("n", "s"), sib)
    got_q.wait()
    project_q(0)
    with scope("w_os"):
        arrive(obuf.at[x, other], ("o", "s"), sib)
    got_w.wait()
    got_saved.wait()
    project_o(0)
    with scope("w_kvs"):
        arrive(kvbuf.at[0, x * 2 + other], ("kv", "s"), sib)
    attend(0, 0, 0, 0)
    pass_on(nbuf, "n")
    peer_keys(x, "ke")
    passed(nbuf, "n")
    project_q(1)
    peer_keys_end(x, "ke")
    attend(0, 0, 1, 0)
    pass_on(obuf, "o")
    with scope("w_kpx"):
        arrive(kvpeer, ("kp",), to_peer)
    remote(kvpeer, kvbuf.at[1, t], ("kx",), across)
    passed(obuf, "o")
    project_o(1)
    slice_sends()
    attend(0, 1, 0, 0)
    attend(0, 1, 1, 0)
    with scope("w_kvx"):
        arrive(kvbuf.at[0, 2 * ox + c], ("kv", "x"), across)
    remote(kvbuf.at[0, 2 * ox + c], kvbuf.at[0, 2 * ox + c], ("kv", "t"), sib)
    need(0)
    attend(1, 0, 0, 0)
    attend(1, 0, 1, 0)
    with scope("w_kvt"):
        arrive(kvbuf.at[0, 2 * ox + other], ("kv", "t"), sib)
    attend(1, 0, 0, 1)
    attend(0, 0, 0, 1)
    peer_keys(ox, "kx")
    attend(0, 1, 0, 1)
    peer_keys_end(ox, "kx")
    attend(1, 0, 1, 1)
    grad_out(1, 0)
    attend(0, 0, 1, 1)
    grad_out(0, 0)
    attend(0, 1, 1, 1)
    need(1)
    attend(1, 1, 1, 0)
    attend(1, 1, 1, 1)
    send_keys(1)
    attend(1, 1, 0, 0)
    attend(1, 1, 0, 1)
    grad_out(1, 1)
    send_keys(0)
    keys_back()
    grad_out(0, 1)
    for v in (1, 2, 3):
        slice_pass(v)
    nall[0] = nbuf[:, :, :, pl.ds(pl.multiple_of(s * ds_width, HEAD_DIM), ds_width)]
    total_out(0, 0)
    total_out(1, 0)
    for v in (1, 2, 3):
        slice_turn(v)
    total_out(0, 1)
    normed_share()
    for v in (1, 2, 3):
        slice_end(v)
    weight_piece(0)
    normed_cross()
    total_out(1, 1)
    weight_piece(1)
    keys_out()
    total_in(0, 0)
    total_in(1, 0)
    total_in(0, 1)
    weight_piece(2)
    normed_end()
    source_end()
    total_in(1, 1)
    weight_piece(3)

    with scope("w_send"):
        for copy, kept in pending:
            if kept:
                copy.wait_send()
        for owner, copy in owner_sends:

            @pl.when(owner != t)
            def _():
                copy.wait_send()


def square_scratch(nr, width, sr, tr, lh, head_width):
    vm = pltpu.VMEM
    m = lh * tr // 2
    ds_width = width // 4
    kv = 2 * HEAD_DIM
    return [
        vm((nr, width), BF16),
        vm((sr, width), BF16),
        vm((1, width), F32),
        vm((width, head_width), BF16),
        vm((width, KV_HEADS * kv), BF16),
        vm((head_width, width), BF16),
        vm((tr, head_width), BF16),
        vm((lh, tr), F32),
        vm((2, 2, nr, width), BF16),
        vm((2, 2, nr, width), BF16),
        vm((KV_HEADS, sr, kv), BF16),
        vm((2, 4, sr, kv), BF16),
        vm((sr, kv), BF16),
        vm((2, 2, 2, m, HEAD_DIM), BF16),
        vm((2, 2, 2, m), F32),
        vm((4, 2, 2, nr, ds_width), BF16),
        vm((2, 4, sr, kv), F32),
        vm((2, 2, HEAD_DIM, m), F32),
        vm((2, 2, m, HEAD_DIM), F32),
        vm((2, 2, m, HEAD_DIM), BF16),
        vm((2, 2, m, HEAD_DIM), BF16),
        vm((4, tr, head_width), BF16),
        vm((2, 2, nr, width), F32),
        vm((2, nr, width), BF16),
        vm((2, nr, width), BF16),
        vm((nr, width), BF16),
        vm((nr, width), BF16),
        vm((2, 2, sr, kv), BF16),
        vm((2, 2, sr, kv), BF16),
        vm((2, sr, kv), BF16),
        vm((2, sr, kv), BF16),
        vm((2, sr, kv), BF16),
        vm((2, sr, kv), BF16),
        pltpu.SemaphoreType.DMA((12,)),
        pltpu.SemaphoreType.DMA((74,)),
        pltpu.SemaphoreType.DMA((80,)),
    ]


def shards(
    target,
    source,
    norm_gain,
    query_weight,
    key_weight,
    value_weight,
    output_weight,
    saved_out,
    log_shift,
    out_grad,
):
    nT = lax.axis_size("tp")
    nS = lax.axis_size("sp")
    nA, nB = rows_split(nS)
    nX, nR = nT // 2, nT // KV_HEADS
    nr, width = target.shape
    sr = source.shape[0]
    tr, head_width = saved_out.shape
    lh = head_width // HEAD_DIM
    m = lh * tr // nX
    ds_width = width // nS
    kv = 2 * HEAD_DIM
    log_rows = math.log(sr * nT * nS)
    vm = pltpu.VMEM
    outputs = 4 * (nr * width + sr * width + ds_width * head_width)
    limit = 67043328 - outputs - 65536
    sems = min(8 * nS * nT, 1024)
    scratch = [
        vm((nr, width), BF16),
        vm((sr, width), BF16),
        vm((1, width), F32),
        vm((width, head_width), BF16),
        vm((width, KV_HEADS * kv), BF16),
        vm((head_width, width), BF16),
        vm((tr, head_width), BF16),
        vm((lh, tr), F32),
        vm((nX, 2, nr, width), BF16),
        vm((nX, 2, nr, width), BF16),
        vm((KV_HEADS, sr, kv), BF16),
        vm((nA, nT, sr, kv), BF16),
        vm((nB, nX, 2, m, HEAD_DIM), BF16),
        vm((nB, nX, 2, m), F32),
        vm((nS, nX, 2, nr, ds_width), BF16),
        vm((nA, nT, sr, kv), F32),
        vm((nB, nX, HEAD_DIM, m), F32),
        vm((nB, nX, m, HEAD_DIM), F32),
        vm((nB, nX, m, HEAD_DIM), BF16),
        vm((nB, nB, nX, m, HEAD_DIM), BF16),
        vm((nS, tr, head_width), BF16),
        vm((nX, 2, nr, width), F32),
        vm((nX, nr, width), BF16),
        vm((nX, nr, width), BF16),
        vm((nX, nr, width), BF16),
        vm((nX, nr, width), BF16),
        vm((nA, nT, sr, kv), BF16),
        vm((nR, nA, KV_HEADS, sr, kv), BF16),
        vm((nA, KV_HEADS, sr, kv), BF16),
        vm((nA, KV_HEADS, sr, kv), BF16),
        vm((KV_HEADS, sr, kv), BF16),
        vm((KV_HEADS, sr, kv), BF16),
        vm((KV_HEADS, sr, kv), F32),
        pltpu.SemaphoreType.DMA((16,)),
        pltpu.SemaphoreType.DMA((sems,)),
        pltpu.SemaphoreType.DMA((sems,)),
    ]
    body = functools.partial(kernel, nS, nT, log_rows)
    if nS == 4 and nT == 4:
        body = functools.partial(square_kernel, log_rows)
        scratch = square_scratch(nr, width, sr, tr, lh, head_width)
    anywhere = pl.BlockSpec(memory_space=pltpu.HBM)
    return pl.pallas_call(
        body,
        out_shape=(
            pltpu.VMEM((nr, width), F32),
            pltpu.VMEM((sr, width), F32),
            pltpu.VMEM((ds_width, head_width), F32),
        ),
        in_specs=[anywhere] * 10,
        out_specs=(pl.BlockSpec(memory_space=pltpu.VMEM),) * 3,
        scratch_shapes=scratch,
        compiler_params=pltpu.CompilerParams(
            collective_id=0, has_side_effects=True, vmem_limit_bytes=limit
        ),
        name="cross_back",
    )(
        target,
        source,
        norm_gain.reshape(1, width),
        query_weight,
        key_weight,
        value_weight,
        output_weight,
        saved_out,
        log_shift,
        out_grad,
    )


def solution(mesh):
    return jax.shard_map(
        shards,
        mesh=mesh,
        in_specs=(
            P(("grp", "sp", "tp"), None),
            P(("grp", "sp", "tp"), None),
            P(),
            P(None, "tp"),
            P(),
            P(),
            P("tp", None),
            P(("grp", "sp"), "tp"),
            P("tp", ("grp", "sp")),
            P(("grp", "sp", "tp"), None),
        ),
        out_specs=(
            P(("grp", "sp", "tp"), None),
            P(("grp", "sp", "tp"), None),
            P(("grp", "sp"), "tp"),
        ),
        check_vma=False,
    )
```

```python
import functools
import math

import jax
import jax.numpy as jnp
from jax import lax
from jax.experimental import pallas as pl
from jax.experimental.pallas import tpu as pltpu
from jax.sharding import PartitionSpec as P

HEADS = 16
HEAD_DIM = 128
KV_HEADS = 2
LOG2E = 1.4426950408889634
BF16 = jnp.bfloat16
F32 = jnp.float32


def rows_split(sp_count):
    keys = 2 if sp_count % 2 == 0 else 1
    while keys * keys * 4 <= sp_count:
        keys *= 2
    return keys, sp_count // keys


def dot_nt(a, b):
    return lax.dot_general(a, b, (((1,), (1,)), ((), ())), preferred_element_type=F32)


def dot_tn(a, b):
    return lax.dot_general(a, b, (((0,), (0,)), ((), ())), preferred_element_type=F32)


def flat_rows(block):
    count = block.shape[-2]
    shape = (-1, block.shape[-1])
    if count % 16:
        return block.astype(F32).reshape(shape).astype(BF16)
    return block.reshape(shape)


def kernel(
    sp_count,
    tp_count,
    log_rows,
    target,
    source,
    norm_gain,
    query_weight,
    key_weight,
    value_weight,
    output_weight,
    saved_out,
    log_shift,
    out_grad,
    target_grad,
    source_grad,
    query_weight_grad,
    tgt,
    src,
    gain,
    wq,
    wkv,
    wo,
    saved,
    shift,
    nbuf,
    obuf,
    kvown,
    kvbuf,
    qob,
    stat,
    nall,
    kacc,
    qacc,
    qfull,
    qsend,
    qrecv,
    qgall,
    ngf,
    ngs,
    ngr,
    ngx,
    ngin,
    kvs,
    kvr,
    kz,
    kzr,
    kfin,
    fin,
    ksum,
    in_sem,
    send_sem,
    recv_sem,
):
    nA, nB, nS, nT = kvbuf.shape[0], qob.shape[0], sp_count, tp_count
    nX = nT // 2
    nR = nT // KV_HEADS
    nr, width = tgt.shape
    sr = src.shape[0]
    lh = shift.shape[0]
    tr = saved.shape[0]
    trx = tr // nX
    ds_width = width // nS
    factor = HEAD_DIM ** (-0.5)
    s = lax.axis_index("sp")
    t = lax.axis_index("tp")
    x, c = t // 2, t % 2
    other = 1 - c
    part, pair = t % nR, t // nR
    zh, zl = s % nA, s // nA

    pending = []
    counts = {"send": 0, "recv": 0, "in": 0}

    def take(kind, n=1):
        first = counts[kind]
        counts[kind] += n
        return first

    def remote(src_ref, dst_ref, recv, where, keep=True):
        copy = pltpu.make_async_remote_copy(
            src_ref=src_ref,
            dst_ref=dst_ref,
            send_sem=send_sem.at[take("send")],
            recv_sem=recv_sem.at[recv],
            device_id=where,
            device_id_type=pl.DeviceIdType.MESH,
        )
        if keep:
            copy.start()
            pending.append(copy)
        return copy

    def arrive(dst_ref, recv, where):
        pltpu.make_async_remote_copy(
            src_ref=dst_ref,
            dst_ref=dst_ref,
            send_sem=send_sem.at[0],
            recv_sem=recv_sem.at[recv],
            device_id=where,
            device_id_type=pl.DeviceIdType.MESH,
        ).wait_recv()

    def fetch(src_ref, dst_ref):
        copy = pltpu.make_async_copy(src_ref, dst_ref, in_sem.at[take("in")])
        copy.start()
        return copy

    def tp_at(xx, cc):
        return {"tp": xx * 2 + cc}

    sibling = tp_at(x, other)

    got_t = fetch(target, tgt)
    got_g = fetch(norm_gain, gain)
    got_o = fetch(out_grad, obuf.at[x, c])
    got_kv = [fetch(source, src)]
    for g in range(KV_HEADS):
        cols = pl.ds(g * HEAD_DIM, HEAD_DIM)
        got_kv.append(fetch(key_weight.at[:, cols], wkv.at[:, pl.ds(2 * g * HEAD_DIM, HEAD_DIM)]))
        got_kv.append(
            fetch(value_weight.at[:, cols], wkv.at[:, pl.ds((2 * g + 1) * HEAD_DIM, HEAD_DIM)])
        )
    got_q = [
        fetch(query_weight, wq),
        fetch(output_weight, wo),
        fetch(saved_out, saved),
        fetch(log_shift, shift),
    ]

    barrier = pltpu.get_barrier_semaphore()
    for k in range(1, nT):
        pl.semaphore_signal(
            barrier, 1, device_id={"tp": (t + k) % nT}, device_id_type=pl.DeviceIdType.MESH
        )
    for k in range(1, nS):
        pl.semaphore_signal(
            barrier, 1, device_id={"sp": (s + k) % nS}, device_id_type=pl.DeviceIdType.MESH
        )

    got_t.wait()
    got_g.wait()
    wide = tgt[...].astype(F32)
    root = jnp.sqrt(jnp.mean(wide * wide, axis=1, keepdims=True) + 1e-06)
    nbuf[x, c] = (wide / root * gain[...]).astype(BF16)
    got_o.wait()
    pl.semaphore_wait(barrier, nT - 1 + nS - 1)

    n_recv = take("recv", 2 * nX)
    o_recv = take("recv", 2 * nX)
    bufs = ((nbuf, n_recv), (obuf, o_recv))
    for k in range(1, nX):
        for buf, base in bufs:
            remote(buf.at[x, c], buf.at[x, c], base + k, tp_at((x + k) % nX, c))
    for buf, base in bufs:
        remote(buf.at[x, c], buf.at[x, c], base, sibling)

    for copy in got_kv:
        copy.wait()
    own = jnp.dot(src[...], wkv[...], preferred_element_type=F32).astype(BF16)
    for g in range(KV_HEADS):
        kvown[g] = own[:, 2 * g * HEAD_DIM : 2 * (g + 1) * HEAD_DIM]
    kvbuf[0, t] = kvown[pair]
    kv_recv = take("recv", 2 * nX)
    for k in range(1, nX):
        xx = (x + k) % nX
        remote(kvown.at[xx * 2 // nR], kvbuf.at[0, t], kv_recv + k, tp_at(xx, c))
    remote(kvown.at[pair], kvbuf.at[0, t], kv_recv, sibling)
    kz_recv = take("recv", 2 * nA * nX)

    def keys_along(a_x, slot):
        for a in range(1, nA):
            remote(
                kvbuf.at[0, slot],
                kvbuf.at[a, slot],
                kz_recv + a * nX + a_x,
                {"sp": zl * nA + (zh + a) % nA},
            )

    keys_along(0, t)

    got_q[-1].wait()
    for xx in range(nX):
        for h in range(lh):
            cols = slice(h * trx, (h + 1) * trx)
            row = (shift[h : h + 1, xx * trx : (xx + 1) * trx] + log_rows) * LOG2E
            stat[0, xx, 0:1, cols] = row
    q_recv = take("recv", 2 * nB * nX)
    st_recv = take("recv", nB * nX)

    def project(k):
        xx = (x + nX - k) % nX
        q_rows = jnp.dot(flat_rows(nbuf[xx]), wq[...], preferred_element_type=F32).astype(BF16)
        for h in range(lh):
            cols = slice(h * HEAD_DIM, (h + 1) * HEAD_DIM)
            qob[0, xx, 0, h * trx : (h + 1) * trx, :] = q_rows[:, cols]
        for b in range(1, nB):
            where = {"sp": (zl + b) % nB * nA + zh}
            remote(qob.at[0, xx, 0], qob.at[b, xx, 0], q_recv + b * nX + k, where)
        o_rows = dot_nt(flat_rows(obuf[xx]), wo[...]).astype(BF16)
        keep = saved[pl.ds(pl.multiple_of(xx * trx, trx), trx), :].astype(F32)
        lane = lax.broadcasted_iota(jnp.int32, (trx, HEAD_DIM), 1)
        drops = jnp.zeros((trx, HEAD_DIM), F32)
        for h in range(lh):
            cols = slice(h * HEAD_DIM, (h + 1) * HEAD_DIM)
            rows = slice(h * trx, (h + 1) * trx)
            qob[0, xx, 1, rows, :] = o_rows[:, cols]
            term = jnp.sum(o_rows[:, cols].astype(F32) * keep[:, cols], axis=1, keepdims=True)
            drops = jnp.where(lane == h, term, drops)
        if trx < HEAD_DIM:
            drops = jnp.concatenate([drops, jnp.zeros((HEAD_DIM - trx, HEAD_DIM), F32)], axis=0)
        drops = drops.T
        for h in range(lh):
            stat[0, xx, 1:2, h * trx : (h + 1) * trx] = drops[h : h + 1, :trx]
        for b in range(1, nB):
            where = {"sp": (zl + b) % nB * nA + zh}
            remote(stat.at[0, xx], stat.at[b, xx], st_recv + b * nX + k, where)
            remote(qob.at[0, xx, 1], qob.at[b, xx, 1], q_recv + (nB + b) * nX + k, where)

    for copy in got_q[:-1]:
        copy.wait()
    for buf, base in bufs:
        arrive(buf.at[x, other], base, sibling)
    project(0)

    slots = [(b, a) for b in range(nB) for a in range(nA)]
    nz_recv = take("recv", nS * (1 + 2 * nX))

    def ahead(b, a):
        return (zl + b) % nB * nA + (zh + a) % nA

    def behind(b, a):
        return (zl + nB - b) % nB * nA + (zh + nA - a) % nA

    for n, (b, a) in enumerate(slots[1:], 1):
        to = ahead(b, a)
        cols = pl.ds(pl.multiple_of(to * ds_width, HEAD_DIM), ds_width)
        remote(nbuf.at[x, c, :, cols], nall.at[n, x, c], nz_recv + n, {"sp": to})

    for k in range(1, nX):
        xx = (x + nX - k) % nX
        for buf, base in bufs:
            arrive(buf.at[xx, c], base + k, tp_at(xx, c))
            remote(buf.at[xx, c], buf.at[xx, c], base + nX + k, sibling)
    for k in range(1, nX):
        xx = (x + nX - k) % nX
        for buf, base in bufs:
            arrive(buf.at[xx, other], base + nX + k, sibling)
        project(k)

    for k in range(1, nX):
        xx = (x + nX - k) % nX
        slot = xx * 2 + c
        arrive(kvbuf.at[0, slot], kv_recv + k, tp_at(xx, c))
        keys_along(k, slot)
        remote(kvbuf.at[0, slot], kvbuf.at[0, slot], kv_recv + nX + k, sibling)
    nall[0] = nbuf[:, :, :, pl.ds(pl.multiple_of(s * ds_width, HEAD_DIM), ds_width)]
    for k in range(1, nX):
        xx = (x + nX - k) % nX
        arrive(kvbuf.at[0, xx * 2 + other], kv_recv + nX + k, sibling)
    arrive(kvbuf.at[0, x * 2 + other], kv_recv, sibling)

    def attend(b, k, a):
        xx = (x + nX - k) % nX

        def step(i, carry):
            keys = kvbuf[a, i, :, :HEAD_DIM]
            values = kvbuf[a, i, :, HEAD_DIM:]
            queries = qob[b, xx, 0]
            backs = qob[b, xx, 1]
            score = dot_nt(keys, queries)
            prob = jnp.exp2(score * (factor * LOG2E) - stat[b, xx, 0:1, :])
            grad = (prob * (dot_nt(values, backs) - stat[b, xx, 1:2, :])).astype(BF16)
            key_part = jnp.dot(grad, queries, preferred_element_type=F32)
            value_part = jnp.dot(prob.astype(BF16), backs, preferred_element_type=F32)
            if b == 0 and k == 0:
                kacc[a, i, :, :HEAD_DIM] = key_part
                kacc[a, i, :, HEAD_DIM:] = value_part
            else:
                kacc[a, i, :, :HEAD_DIM] += key_part
                kacc[a, i, :, HEAD_DIM:] += value_part
            qacc[b, xx] += dot_tn(keys, grad)
            return carry

        lax.fori_loop(0, nT, step, 0, unroll=min(nT, 4))

    qs_recv = take("recv", nB * nB * nX)

    def send_queries(b, k):
        xx = (x + nX - k) % nX
        block = (qacc[b, xx] * factor).T
        qfull[b, xx] = block
        qsend[b, xx] = block.astype(BF16)
        for n in range(1, nB):
            slot = (n + b) % nB
            remote(
                qsend.at[b, xx],
                qrecv.at[n, slot, xx],
                qs_recv + (n * nB + slot) * nX + k,
                {"sp": (zl + n) % nB * nA + zh},
            )

    qacc[...] = jnp.zeros(qacc.shape, F32)
    for k in range(nX):
        attend(0, k, 0)

    for a in range(1, nA):
        for a_x in range(nX):
            slot = (x + nX - a_x) % nX * 2 + c
            idx = kz_recv + a * nX + a_x
            where = {"sp": zl * nA + (zh + nA - a) % nA}
            arrive(kvbuf.at[a, slot], idx, where)
            remote(kvbuf.at[a, slot], kvbuf.at[a, slot], idx + nA * nX, sibling)
        if a == 1:
            for n, (b, aa) in enumerate(slots[1:], 1):
                arrive(nall.at[n, x, c], nz_recv + n, {"sp": behind(b, aa)})
                base = nz_recv + nS + n * 2 * nX
                for j in range(1, nX):
                    remote(nall.at[n, x, c], nall.at[n, x, c], base + j, tp_at((x + j) % nX, c))
                remote(nall.at[n, x, c], nall.at[n, x, c], base, sibling)
        for a_x in range(nX):
            slot = (x + nX - a_x) % nX * 2 + other
            arrive(kvbuf.at[a, slot], kz_recv + a * nX + a_x + nA * nX, sibling)
        for k in range(nX):
            attend(0, k, a)
            if a == nA - 1:
                send_queries(0, k)

    kr_recv = take("recv", nA * nR)

    def send_keys(a):
        def convert(i, carry):
            kvs[a, i, :, :HEAD_DIM] = (kacc[a, i, :, :HEAD_DIM] * factor).astype(BF16)
            kvs[a, i, :, HEAD_DIM:] = kacc[a, i, :, HEAD_DIM:].astype(BF16)
            return carry

        lax.fori_loop(0, nT, convert, 0)
        for k in range(1, nR):
            to = (part + k) % nR
            remote(
                kvs.at[a, pl.ds(to * KV_HEADS, KV_HEADS)],
                kvr.at[k, a],
                kr_recv + a * nR + k,
                {"tp": pair * nR + to},
            )

    for k in range(nX):
        for b in range(1, nB):
            xx = (x + nX - k) % nX
            where = {"sp": (zl + nB - b) % nB * nA + zh}
            arrive(stat.at[b, xx], st_recv + b * nX + k, where)
            arrive(qob.at[b, xx, 0], q_recv + b * nX + k, where)
            arrive(qob.at[b, xx, 1], q_recv + (nB + b) * nX + k, where)
            last = k == nX - 1 and b == nB - 1
            for a in range(nA - 1, -1, -1):
                attend(b, k, a)
                if a == 0:
                    send_queries(b, k)
                if last:
                    send_keys(a)

    qg_recv = take("recv", nS)

    def finish_queries(b):
        for k in range(nX):
            xx = (x + nX - k) % nX
            total = qfull[b, xx]
            for n in range(1, nB):
                base = qs_recv + (n * nB + b) * nX + k
                arrive(qrecv.at[n, b, xx], base, {"sp": (zl + nB - n) % nB * nA + zh})
                total += qrecv[n, b, xx].astype(F32)
            total = total.astype(BF16)
            rows = pl.ds(pl.multiple_of(xx * trx, trx), trx)
            for h in range(lh):
                cols = slice(h * HEAD_DIM, (h + 1) * HEAD_DIM)
                qgall[b * nA, rows, cols] = total[h * trx : (h + 1) * trx, :]
        for a in range(1, nA):
            remote(
                qgall.at[b * nA],
                qgall.at[b * nA + a],
                qg_recv + b * nA + a,
                {"sp": zl * nA + (zh + a) % nA},
            )

    def portion(a, i):
        block = kacc[a, part * KV_HEADS + i]
        k_lane = lax.broadcasted_iota(jnp.int32, block.shape, 1) < HEAD_DIM
        block = jnp.where(k_lane, block * factor, block)
        for k in range(1, nR):
            block += kvr[k, a, i].astype(F32)
        return block

    ka_recv = take("recv", nA)
    for a in range(nA - 1, 0, -1):
        for k in range(1, nR):
            where = {"tp": pair * nR + (part + nR - k) % nR}
            arrive(kvr.at[k, a], kr_recv + a * nR + k, where)
        for i in range(KV_HEADS):
            kz[a, i] = portion(a, i).astype(BF16)
        remote(kz.at[a], kzr.at[a], ka_recv + a, {"sp": zl * nA + (zh + nA - a) % nA})

    for b in range(1, nB):
        finish_queries(b)

    for n, (b, a) in enumerate(slots[1:], 1):
        base = nz_recv + nS + n * 2 * nX
        for j in range(1, nX):
            xx = (x + nX - j) % nX
            arrive(nall.at[n, xx, c], base + j, tp_at(xx, c))
            remote(nall.at[n, xx, c], nall.at[n, xx, c], base + nX + j, sibling)

    finish_queries(0)

    step_cols = min(512, width)
    for i in range(width // step_cols):
        cols = slice(i * step_cols, (i + 1) * step_cols)
        share = dot_nt(qgall[0], wq[cols, :])
        ngf[:, :, :, cols] = share.reshape(nX, 2, nr, step_cols)
    for xx in range(nX):
        ngs[xx] = ngf[xx, other].astype(BF16)
    ng_recv = take("recv", nX)
    remote(ngs, ngr, ng_recv, sibling)

    for k in range(1, nR):
        arrive(kvr.at[k, 0], kr_recv + k, {"tp": pair * nR + (part + nR - k) % nR})
    for i in range(KV_HEADS):
        ksum[i] = portion(0, i)

    arrive(ngr, ng_recv, sibling)
    for k in range(1, nX):
        xx = (x + k) % nX
        ngx[k] = (ngf[xx, c] + ngr[xx].astype(F32)).astype(BF16)
        remote(ngx.at[k], ngin.at[k], ng_recv + k, tp_at(xx, c))

    for a in range(1, nA):
        arrive(kzr.at[a], ka_recv + a, {"sp": zl * nA + (zh + a) % nA})
    f_recv = take("recv", KV_HEADS)
    owner_sends = []
    for i in range(KV_HEADS):
        block = ksum[i]
        for a in range(1, nA):
            block += kzr[a, i].astype(F32)
        kfin[i] = block.astype(BF16)
        owner = part * KV_HEADS + i
        copy = remote(kfin.at[i], fin.at[pair], f_recv + pair, {"tp": owner}, keep=False)
        owner_sends.append((owner, copy))

        @pl.when(owner != t)
        def _():
            copy.start()

        @pl.when(owner == t)
        def _():
            fin[pair] = kfin[i]

    for n, (b, a) in enumerate(slots):
        if n:
            base = nz_recv + nS + n * 2 * nX
            arrive(nall.at[n, x, other], base, sibling)
            for j in range(1, nX):
                arrive(nall.at[n, (x + nX - j) % nX, other], base + nX + j, sibling)
    order = [b * nA for b in range(nB)] + [b * nA + a for b in list(range(1, nB)) + [0] for a in range(1, nA)]
    for n in order:
        if n % nA:
            arrive(qgall.at[n], qg_recv + n, {"sp": zl * nA + (zh + nA - n % nA) % nA})
        piece = dot_tn(flat_rows(nall[n]), qgall[n])
        if n == 0:
            query_weight_grad[...] = piece
        else:
            query_weight_grad[...] += piece

    grad = ngf[x, c] + ngr[x].astype(F32)
    for k in range(1, nX):
        arrive(ngin.at[k], ng_recv + k, tp_at((x + nX - k) % nX, c))
        grad += ngin[k].astype(F32)
    scaled = grad * gain[...]
    wide = tgt[...].astype(F32)
    root = jnp.sqrt(jnp.mean(wide * wide, axis=1, keepdims=True) + 1e-06)
    target_grad[...] = scaled / root - wide * jnp.mean(scaled * wide, axis=1, keepdims=True) / (
        root * root * root
    )

    for g in range(KV_HEADS):
        giver = g * nR + t // KV_HEADS

        @pl.when(giver != t)
        def _():
            arrive(fin.at[g], f_recv + g, {"tp": giver})

    for i in range(width // step_cols):
        rows = pl.ds(i * step_cols, step_cols)
        part_sum = dot_nt(fin[0], wkv[rows, 0 : 2 * HEAD_DIM])
        for g in range(1, KV_HEADS):
            part_sum += dot_nt(fin[g], wkv[rows, 2 * g * HEAD_DIM : 2 * (g + 1) * HEAD_DIM])
        source_grad[:, rows] = part_sum

    for copy in pending:
        copy.wait_send()
    for owner, copy in owner_sends:

        @pl.when(owner != t)
        def _():
            copy.wait_send()


def square_kernel(
    log_rows,
    target,
    source,
    norm_gain,
    query_weight,
    key_weight,
    value_weight,
    output_weight,
    saved_out,
    log_shift,
    out_grad,
    target_grad,
    source_grad,
    query_weight_grad,
    tgt,
    src,
    gain,
    wq,
    wkv,
    wo,
    saved,
    shift,
    nbuf,
    obuf,
    kvown,
    kvbuf,
    kvpeer,
    qob,
    stat,
    nall,
    kacc,
    qacc,
    qfull,
    qsend,
    qrecv,
    qgall,
    ngf,
    ngs,
    ngr,
    ngx,
    ngin,
    kvs,
    kvr,
    kz,
    kzr,
    kfin,
    fin,
    bulk,
    in_sem,
    send_sem,
    recv_sem,
):
    nr, width = tgt.shape
    lh = shift.shape[0]
    tr = saved.shape[0]
    nS, nT = 4, 4
    trx = tr // 2
    ds_width = width // nS
    factor = HEAD_DIM ** (-0.5)
    s = lax.axis_index("sp")
    t = lax.axis_index("tp")
    x, c = t // 2, t % 2
    ox, other = 1 - x, 1 - c
    peer = s + 1 - 2 * (s % 2)
    far = (s + 2) % nS
    diag = (peer + 2) % nS
    sib = {"tp": x * 2 + other}
    across = {"tp": ox * 2 + c}
    to_peer = {"sp": peer}
    to_far = {"sp": far}
    to_diag = {"sp": diag}

    keys = {("fin", 0): 0, ("fin", 1): 1}
    counts = {"in": 0}

    def sem(*key):
        return keys.setdefault(key, len(keys))

    def fetch(src_ref, dst_ref, at=None):
        if at is None:
            at = counts["in"]
            counts["in"] += 1
        copy = pltpu.make_async_copy(src_ref, dst_ref, in_sem.at[at])
        copy.start()
        return copy

    got_t = fetch(target, tgt)
    got_g = fetch(norm_gain, gain)
    got_shift = fetch(log_shift, shift)
    got_o = fetch(out_grad, obuf.at[x, c])
    got_kv = [fetch(source, src)]
    for g in range(KV_HEADS):
        cols = pl.ds(g * HEAD_DIM, HEAD_DIM)
        got_kv.append(fetch(key_weight.at[:, cols], wkv.at[:, pl.ds(2 * g * HEAD_DIM, HEAD_DIM)]))
        got_kv.append(
            fetch(value_weight.at[:, cols], wkv.at[:, pl.ds((2 * g + 1) * HEAD_DIM, HEAD_DIM)])
        )
    got_q = fetch(query_weight, wq)
    got_w = fetch(output_weight, wo)
    got_saved = fetch(saved_out, saved)

    barrier = pltpu.get_barrier_semaphore()
    for k in range(1, nT):
        pl.semaphore_signal(
            barrier, 1, device_id={"tp": (t + k) % nT}, device_id_type=pl.DeviceIdType.MESH
        )
    for k in range(1, nS):
        pl.semaphore_signal(
            barrier, 1, device_id={"sp": (s + k) % nS}, device_id_type=pl.DeviceIdType.MESH
        )

    got_t.wait()
    got_g.wait()
    wide = tgt[...].astype(F32)
    root = jnp.sqrt(jnp.mean(wide * wide, axis=1, keepdims=True) + 1e-06)
    nbuf[x, c] = (wide / root * gain[...]).astype(BF16)
    got_o.wait()
    pl.semaphore_wait(barrier, nT - 1 + nS - 1)

    pending, sent = [], []

    def remote(src_ref, dst_ref, key, where, keep=True):
        shared = keep and src_ref.dtype == BF16
        if shared:
            sent.append(math.prod(src_ref.shape) * 2)
        copy = pltpu.make_async_remote_copy(
            src_ref=src_ref,
            dst_ref=dst_ref,
            send_sem=send_sem.at[0 if shared else len(pending) + 1],
            recv_sem=recv_sem.at[sem(*key) if isinstance(key, tuple) else key],
            device_id=where,
            device_id_type=pl.DeviceIdType.MESH,
        )
        if keep:
            copy.start()
        if not shared:
            pending.append((copy, keep))
        return copy

    def arrive(dst_ref, key, where):
        pltpu.make_async_remote_copy(
            src_ref=dst_ref,
            dst_ref=dst_ref,
            send_sem=send_sem.at[0],
            recv_sem=recv_sem.at[sem(*key)],
            device_id=where,
            device_id_type=pl.DeviceIdType.MESH,
        ).wait_recv()

    def scope(name):
        return jax.named_scope(name)

    remote(nbuf.at[x, c], nbuf.at[x, c], ("n", "x"), across)
    remote(nbuf.at[x, c], nbuf.at[x, c], ("n", "s"), sib)
    remote(obuf.at[x, c], obuf.at[x, c], ("o", "s"), sib)
    remote(obuf.at[x, c], obuf.at[x, c], ("o", "x"), across)
    for copy in got_kv:
        copy.wait()
    with scope("kvproj"):
        own = jnp.dot(src[...], wkv[...], preferred_element_type=F32).astype(BF16)
        for g in range(KV_HEADS):
            kvown[g] = own[:, 2 * g * HEAD_DIM : 2 * (g + 1) * HEAD_DIM]
        kvbuf[0, t] = kvown[x]
    remote(kvown.at[x], kvbuf.at[0, t], ("kv", "s"), sib)
    remote(kvown.at[ox], kvbuf.at[0, t], ("kv", "x"), across)
    got_shift.wait()
    for k in range(2):
        xx = x if k == 0 else ox
        for h in range(lh):
            row = jnp.where(xx == 0, shift[h : h + 1, 0:trx], shift[h : h + 1, trx : 2 * trx])
            stat[0, k, 0:1, h * trx : (h + 1) * trx] = (row + log_rows) * LOG2E

    def send_far(ref, kind, k):
        remote(ref.at[0, k], ref.at[1, k], (kind, k), to_far)

    def send_part(i, kind, k):
        remote(qob.at[0, k, i], qob.at[1, k, i], (kind, k), to_far)

    def project_q(k):
        with scope(f"project_q{k}"):
            xx = x if k == 0 else ox
            rows = jnp.dot(flat_rows(nbuf[xx]), wq[...], preferred_element_type=F32).astype(BF16)
            for h in range(lh):
                cols = slice(h * HEAD_DIM, (h + 1) * HEAD_DIM)
                qob[0, k, 0, h * trx : (h + 1) * trx, :] = rows[:, cols]
        send_part(0, "q", k)

    def project_o(k):
        with scope(f"project_o{k}"):
            xx = x if k == 0 else ox
            o_rows = dot_nt(flat_rows(obuf[xx]), wo[...]).astype(BF16)
            for h in range(lh):
                cols = slice(h * HEAD_DIM, (h + 1) * HEAD_DIM)
                qob[0, k, 1, h * trx : (h + 1) * trx, :] = o_rows[:, cols]
        send_part(1, "ob", k)
        with scope(f"drop{k}"):
            keep = saved[pl.ds(pl.multiple_of(xx * trx, trx), trx), :].astype(F32)
            lane = lax.broadcasted_iota(jnp.int32, (trx, HEAD_DIM), 1)
            drops = jnp.zeros((trx, HEAD_DIM), F32)
            for h in range(lh):
                cols = slice(h * HEAD_DIM, (h + 1) * HEAD_DIM)
                term = jnp.sum(o_rows[:, cols].astype(F32) * keep[:, cols], axis=1, keepdims=True)
                drops = jnp.where(lane == h, term, drops)
            drops = jnp.concatenate([drops, jnp.zeros((HEAD_DIM - trx, HEAD_DIM), F32)], axis=0)
            drops = drops.T
            for h in range(lh):
                stat[0, k, 1:2, h * trx : (h + 1) * trx] = drops[h : h + 1, :trx]
        send_far(stat, "st", k)

    def need(k):
        with scope(f"w_q{k}"):
            arrive(qob.at[1, k, 0], ("q", k), to_far)
        with scope(f"w_ob{k}"):
            arrive(qob.at[1, k, 1], ("ob", k), to_far)
            arrive(stat.at[1, k], ("st", k), to_far)

    got = {"kacc": set(), "qacc": set()}

    def attend(v, k, a, g):
        with scope(f"attend_{v}{k}{a}{g}"):
            attend_rows(v, k, a, g)

    def attend_rows(v, k, a, g):
        pair = pl.ds(2 * (x if g == 0 else ox), 2)
        sr = kvbuf.shape[2]
        k_rows = kvbuf[a, pair, :, :HEAD_DIM].reshape(2 * sr, HEAD_DIM)
        v_rows = kvbuf[a, pair, :, HEAD_DIM:].reshape(2 * sr, HEAD_DIM)
        queries = qob[v, k, 0]
        backs = qob[v, k, 1]
        score = dot_nt(k_rows, queries)
        prob = jnp.exp2(score * (factor * LOG2E) - stat[v, k, 0:1, :])
        grad = (prob * (dot_nt(v_rows, backs) - stat[v, k, 1:2, :])).astype(BF16)
        key_part = jnp.dot(grad, queries, preferred_element_type=F32)
        value_part = jnp.dot(prob.astype(BF16), backs, preferred_element_type=F32)
        key_part = key_part.reshape(2, sr, HEAD_DIM)
        value_part = value_part.reshape(2, sr, HEAD_DIM)
        if (a, g) not in got["kacc"]:
            kacc[a, pair, :, :HEAD_DIM] = key_part
            kacc[a, pair, :, HEAD_DIM:] = value_part
        else:
            kacc[a, pair, :, :HEAD_DIM] += key_part
            kacc[a, pair, :, HEAD_DIM:] += value_part
        if (v, k) not in got["qacc"]:
            qacc[v, k] = dot_tn(k_rows, grad)
            got["qacc"].add((v, k))
        else:
            qacc[v, k] += dot_tn(k_rows, grad)
        got["kacc"].add((a, g))

    def query_part(v, k):
        return (qacc[v, k] * factor).T

    def send_keys(a):
        with scope(f"keys{a}"):
            for i in range(2):
                slot = 2 * other + i
                kvs[a, i, :, :HEAD_DIM] = (kacc[a, slot, :, :HEAD_DIM] * factor).astype(BF16)
                kvs[a, i, :, HEAD_DIM:] = kacc[a, slot, :, HEAD_DIM:].astype(BF16)
        remote(kvs.at[a], kvr.at[a], ("kp", a), sib)

    def key_sum(a, i):
        block = kacc[a, 2 * c + i]
        k_lane = lax.broadcasted_iota(jnp.int32, block.shape, 1) < HEAD_DIM
        return jnp.where(k_lane, block * factor, block) + kvr[a, i].astype(F32)

    def keys_back():
        with scope("w_kp1"):
            arrive(kvr.at[1], ("kp", 1), sib)
        with scope("kz"):
            for i in range(2):
                kz[i] = key_sum(1, i).astype(BF16)
        remote(kz, kzr, ("kz",), to_peer)

    def slice_sends():
        for v, where, to in ((2, to_peer, peer), (1, to_far, far), (3, to_diag, diag)):
            cols = pl.ds(pl.multiple_of(to * ds_width, HEAD_DIM), ds_width)
            remote(nbuf.at[x, c, :, cols], nall.at[v, x, c], ("na", v), where)

    def slice_from(v):
        return (None, to_far, to_peer, to_diag)[v]

    def slice_pass(v):
        with scope(f"w_na{v}"):
            arrive(nall.at[v, x, c], ("na", v), slice_from(v))
        remote(nall.at[v, x, c], nall.at[v, x, c], ("na", v, "x"), across)
        remote(nall.at[v, x, c], nall.at[v, x, c], ("na", v, "s"), sib)

    def slice_turn(v):
        with scope(f"w_nx{v}"):
            arrive(nall.at[v, ox, c], ("na", v, "x"), across)
        remote(nall.at[v, ox, c], nall.at[v, ox, c], ("na", v, "t"), sib)

    def slice_end(v):
        with scope(f"w_ns{v}"):
            arrive(nall.at[v, x, other], ("na", v, "s"), sib)
            arrive(nall.at[v, ox, other], ("na", v, "t"), sib)

    def total_rows(v, k):
        xx = x if k == 0 else ox
        return qgall.at[v, pl.ds(pl.multiple_of(xx * trx, trx), trx), :]

    pieces = []

    def weight_piece(v):
        with scope(f"piece{v}"):
            piece = dot_tn(flat_rows(nall[v]), qgall[v])
            if not pieces:
                query_weight_grad[...] = piece
            else:
                query_weight_grad[...] += piece
            pieces.append(v)

    step_cols = min(512, width)

    def normed_share():
        with scope("ng_share"):
            for i in range(width // step_cols):
                cols = slice(i * step_cols, (i + 1) * step_cols)
                share = dot_nt(qgall[0], wq[cols, :])
                ngf[:, :, :, cols] = share.reshape(2, 2, nr, step_cols)
            for xx in range(2):
                ngs[xx] = ngf[xx, other].astype(BF16)
        remote(ngs, ngr, ("ng", "s"), sib)

    def normed_cross():
        with scope("w_ngs"):
            arrive(ngr, ("ng", "s"), sib)
        ngx[...] = (ngf[ox, c] + ngr[ox].astype(F32)).astype(BF16)
        remote(ngx, ngin, ("ng", "x"), across)

    def normed_end():
        with scope("w_ngx"):
            arrive(ngin, ("ng", "x"), across)
        with scope("target"):
            grad = ngf[x, c] + ngr[x].astype(F32) + ngin[...].astype(F32)
            scaled = grad * gain[...]
            wide = tgt[...].astype(F32)
            root = jnp.sqrt(jnp.mean(wide * wide, axis=1, keepdims=True) + 1e-06)
            target_grad[...] = scaled / root - wide * jnp.mean(
                scaled * wide, axis=1, keepdims=True
            ) / (root * root * root)

    owner_sends = []

    def keys_out():
        with scope("w_kp0"):
            arrive(kvr.at[0], ("kp", 0), sib)
        with scope("w_kz"):
            arrive(kzr, ("kz",), to_peer)
        with scope("keys_out"):
            for i in range(2):
                block = key_sum(0, i) + kzr[i].astype(F32)
                kfin[i] = block.astype(BF16)
                owner = c * 2 + i
                copy = remote(kfin.at[i], fin.at[x], x, {"tp": owner}, keep=False)
                owner_sends.append((owner, copy))

                @pl.when(owner != t)
                def _():
                    copy.start()

                @pl.when(owner == t)
                def _():
                    fin[x] = kfin[i]

    def source_end():
        for g in range(KV_HEADS):
            giver = g * 2 + t // 2

            @pl.when(giver != t)
            def _():
                with scope("w_fin"):
                    arrive(fin.at[g], ("fin", g), {"tp": giver})

        with scope("source"):
            for i in range(width // step_cols):
                rows = pl.ds(i * step_cols, step_cols)
                part_sum = dot_nt(fin[0], wkv[rows, 0 : 2 * HEAD_DIM])
                for g in range(1, KV_HEADS):
                    part_sum += dot_nt(fin[g], wkv[rows, 2 * g * HEAD_DIM : 2 * (g + 1) * HEAD_DIM])
                source_grad[:, rows] = part_sum

    def pass_on(buf, kind):
        with scope(f"w_{kind}x"):
            arrive(buf.at[ox, c], (kind, "x"), across)
        remote(buf.at[ox, c], buf.at[ox, c], (kind, "t"), sib)

    def passed(buf, kind):
        with scope(f"w_{kind}t"):
            arrive(buf.at[ox, other], (kind, "t"), sib)

    def grad_out(b, k):
        with scope(f"dq_{b}{k}"):
            block = query_part(b, k)
            qfull[b, k] = block
            qsend[b, k] = block.astype(BF16)
        remote(qsend.at[b, k], qrecv.at[1 - b, k], ("dq", 1 - b, k), to_far)

    def total_out(b, k):
        with scope(f"w_dq{b}{k}"):
            arrive(qrecv.at[b, k], ("dq", b, k), to_far)
        with scope(f"total_{b}{k}"):
            total = (qfull[b, k] + qrecv[b, k].astype(F32)).astype(BF16)
            rows = pl.ds(pl.multiple_of((x if k == 0 else ox) * trx, trx), trx)
            for h in range(lh):
                cols = slice(h * HEAD_DIM, (h + 1) * HEAD_DIM)
                qgall[b, rows, cols] = total[h * trx : (h + 1) * trx, :]
        remote(total_rows(b, k), total_rows(2 + b, k), ("tot", b, k), to_peer)

    def total_in(b, k):
        with scope(f"w_tot{b}{k}"):
            arrive(total_rows(2 + b, k), ("tot", b, k), to_peer)

    def peer_keys(chip, kind):
        with scope(f"w_{kind}"):
            arrive(kvbuf.at[1, 2 * chip + c], (kind,), to_peer if chip is x else across)
        remote(kvbuf.at[1, 2 * chip + c], kvbuf.at[1, 2 * chip + c], (kind, "s"), sib)

    def peer_keys_end(chip, kind):
        with scope(f"w_{kind}s"):
            arrive(kvbuf.at[1, 2 * chip + other], (kind, "s"), sib)

    remote(kvown.at[ox], kvpeer, ("kp",), to_peer)
    with scope("w_ns"):
        arrive(nbuf.at[x, other], ("n", "s"), sib)
    got_q.wait()
    project_q(0)
    with scope("w_os"):
        arrive(obuf.at[x, other], ("o", "s"), sib)
    got_w.wait()
    got_saved.wait()
    project_o(0)
    remote(kvown.at[x], kvbuf.at[1, t], ("ke",), to_peer)
    with scope("w_kvs"):
        arrive(kvbuf.at[0, x * 2 + other], ("kv", "s"), sib)
    attend(0, 0, 0, 0)
    pass_on(nbuf, "n")
    passed(nbuf, "n")
    project_q(1)
    with scope("w_kpx"):
        arrive(kvpeer, ("kp",), to_peer)
    remote(kvpeer, kvbuf.at[1, t], ("kx",), across)
    pass_on(obuf, "o")
    passed(obuf, "o")
    project_o(1)
    slice_sends()
    attend(0, 1, 0, 0)
    need(0)
    attend(1, 0, 0, 0)
    with scope("w_kvx"):
        arrive(kvbuf.at[0, 2 * ox + c], ("kv", "x"), across)
    remote(kvbuf.at[0, 2 * ox + c], kvbuf.at[0, 2 * ox + c], ("kv", "t"), sib)
    peer_keys(x, "ke")
    with scope("w_kvt"):
        arrive(kvbuf.at[0, 2 * ox + other], ("kv", "t"), sib)
    attend(0, 0, 0, 1)
    attend(1, 0, 0, 1)
    peer_keys(ox, "kx")
    attend(0, 1, 0, 1)
    peer_keys_end(x, "ke")
    attend(1, 0, 1, 0)
    peer_keys_end(ox, "kx")
    attend(1, 0, 1, 1)
    grad_out(1, 0)
    attend(0, 0, 1, 0)
    attend(0, 0, 1, 1)
    grad_out(0, 0)
    attend(0, 1, 1, 0)
    attend(0, 1, 1, 1)
    need(1)
    attend(1, 1, 1, 0)
    attend(1, 1, 1, 1)
    send_keys(1)
    attend(1, 1, 0, 0)
    attend(1, 1, 0, 1)
    grad_out(1, 1)
    send_keys(0)
    keys_back()
    grad_out(0, 1)
    for v in (1, 2, 3):
        slice_pass(v)
    nall[0] = nbuf[:, :, :, pl.ds(pl.multiple_of(s * ds_width, HEAD_DIM), ds_width)]
    total_out(0, 0)
    total_out(1, 0)
    for v in (1, 2, 3):
        slice_turn(v)
    total_out(0, 1)
    normed_share()
    for v in (1, 2, 3):
        slice_end(v)
    weight_piece(0)
    normed_cross()
    total_out(1, 1)
    weight_piece(1)
    keys_out()
    total_in(0, 0)
    total_in(1, 0)
    total_in(0, 1)
    weight_piece(2)
    normed_end()
    source_end()
    total_in(1, 1)
    weight_piece(3)

    with scope("w_send"):
        whole = bulk.at[pl.ds(0, sum(sent) // (bulk.shape[1] * 4))]
        pltpu.make_async_copy(whole, whole, send_sem.at[0]).wait()
        for copy, kept in pending:
            if kept:
                copy.wait_send()
        for owner, copy in owner_sends:

            @pl.when(owner != t)
            def _():
                copy.wait_send()


def square_scratch(nr, width, sr, tr, lh, head_width):
    vm = pltpu.VMEM
    m = lh * tr // 2
    ds_width = width // 4
    kv = 2 * HEAD_DIM
    return [
        vm((nr, width), BF16),
        vm((sr, width), BF16),
        vm((1, width), F32),
        vm((width, head_width), BF16),
        vm((width, KV_HEADS * kv), BF16),
        vm((head_width, width), BF16),
        vm((tr, head_width), BF16),
        vm((lh, tr), F32),
        vm((2, 2, nr, width), BF16),
        vm((2, 2, nr, width), BF16),
        vm((KV_HEADS, sr, kv), BF16),
        vm((2, 4, sr, kv), BF16),
        vm((sr, kv), BF16),
        vm((2, 2, 2, m, HEAD_DIM), BF16),
        vm((2, 2, 2, m), F32),
        vm((4, 2, 2, nr, ds_width), BF16),
        vm((2, 4, sr, kv), F32),
        vm((2, 2, HEAD_DIM, m), F32),
        vm((2, 2, m, HEAD_DIM), F32),
        vm((2, 2, m, HEAD_DIM), BF16),
        vm((2, 2, m, HEAD_DIM), BF16),
        vm((4, tr, head_width), BF16),
        vm((2, 2, nr, width), F32),
        vm((2, nr, width), BF16),
        vm((2, nr, width), BF16),
        vm((nr, width), BF16),
        vm((nr, width), BF16),
        vm((2, 2, sr, kv), BF16),
        vm((2, 2, sr, kv), BF16),
        vm((2, sr, kv), BF16),
        vm((2, sr, kv), BF16),
        vm((2, sr, kv), BF16),
        vm((2, sr, kv), BF16),
        vm((8 * sr, width // 2), F32),
        pltpu.SemaphoreType.DMA((12,)),
        pltpu.SemaphoreType.DMA((6,)),
        pltpu.SemaphoreType.DMA((48,)),
    ]


def shards(
    target,
    source,
    norm_gain,
    query_weight,
    key_weight,
    value_weight,
    output_weight,
    saved_out,
    log_shift,
    out_grad,
):
    nT = lax.axis_size("tp")
    nS = lax.axis_size("sp")
    nA, nB = rows_split(nS)
    nX, nR = nT // 2, nT // KV_HEADS
    nr, width = target.shape
    sr = source.shape[0]
    tr, head_width = saved_out.shape
    lh = head_width // HEAD_DIM
    m = lh * tr // nX
    ds_width = width // nS
    kv = 2 * HEAD_DIM
    log_rows = math.log(sr * nT * nS)
    vm = pltpu.VMEM
    outputs = 4 * (nr * width + sr * width + ds_width * head_width)
    limit = 67043328 - outputs - 65536
    sems = min(8 * nS * nT, 1024)
    scratch = [
        vm((nr, width), BF16),
        vm((sr, width), BF16),
        vm((1, width), F32),
        vm((width, head_width), BF16),
        vm((width, KV_HEADS * kv), BF16),
        vm((head_width, width), BF16),
        vm((tr, head_width), BF16),
        vm((lh, tr), F32),
        vm((nX, 2, nr, width), BF16),
        vm((nX, 2, nr, width), BF16),
        vm((KV_HEADS, sr, kv), BF16),
        vm((nA, nT, sr, kv), BF16),
        vm((nB, nX, 2, m, HEAD_DIM), BF16),
        vm((nB, nX, 2, m), F32),
        vm((nS, nX, 2, nr, ds_width), BF16),
        vm((nA, nT, sr, kv), F32),
        vm((nB, nX, HEAD_DIM, m), F32),
        vm((nB, nX, m, HEAD_DIM), F32),
        vm((nB, nX, m, HEAD_DIM), BF16),
        vm((nB, nB, nX, m, HEAD_DIM), BF16),
        vm((nS, tr, head_width), BF16),
        vm((nX, 2, nr, width), F32),
        vm((nX, nr, width), BF16),
        vm((nX, nr, width), BF16),
        vm((nX, nr, width), BF16),
        vm((nX, nr, width), BF16),
        vm((nA, nT, sr, kv), BF16),
        vm((nR, nA, KV_HEADS, sr, kv), BF16),
        vm((nA, KV_HEADS, sr, kv), BF16),
        vm((nA, KV_HEADS, sr, kv), BF16),
        vm((KV_HEADS, sr, kv), BF16),
        vm((KV_HEADS, sr, kv), BF16),
        vm((KV_HEADS, sr, kv), F32),
        pltpu.SemaphoreType.DMA((16,)),
        pltpu.SemaphoreType.DMA((sems,)),
        pltpu.SemaphoreType.DMA((sems,)),
    ]
    body = functools.partial(kernel, nS, nT, log_rows)
    if nS == 4 and nT == 4:
        body = functools.partial(square_kernel, log_rows)
        scratch = square_scratch(nr, width, sr, tr, lh, head_width)
    anywhere = pl.BlockSpec(memory_space=pltpu.HBM)
    return pl.pallas_call(
        body,
        out_shape=(
            pltpu.VMEM((nr, width), F32),
            pltpu.VMEM((sr, width), F32),
            pltpu.VMEM((ds_width, head_width), F32),
        ),
        in_specs=[anywhere] * 10,
        out_specs=(pl.BlockSpec(memory_space=pltpu.VMEM),) * 3,
        scratch_shapes=scratch,
        compiler_params=pltpu.CompilerParams(
            collective_id=0, has_side_effects=True, vmem_limit_bytes=limit
        ),
        name="cross_back",
    )(
        target,
        source,
        norm_gain.reshape(1, width),
        query_weight,
        key_weight,
        value_weight,
        output_weight,
        saved_out,
        log_shift,
        out_grad,
    )


def solution(mesh):
    return jax.shard_map(
        shards,
        mesh=mesh,
        in_specs=(
            P(("grp", "sp", "tp"), None),
            P(("grp", "sp", "tp"), None),
            P(),
            P(None, "tp"),
            P(),
            P(),
            P("tp", None),
            P(("grp", "sp"), "tp"),
            P("tp", ("grp", "sp")),
            P(("grp", "sp", "tp"), None),
        ),
        out_specs=(
            P(("grp", "sp", "tp"), None),
            P(("grp", "sp", "tp"), None),
            P(("grp", "sp"), "tp"),
        ),
        check_vma=False,
    )
```

```python
import functools
import math

import jax
import jax.numpy as jnp
from jax import lax
from jax.experimental import pallas as pl
from jax.experimental.pallas import tpu as pltpu
from jax.sharding import PartitionSpec as P

HEADS = 16
HEAD_DIM = 128
KV_HEADS = 2
LOG2E = 1.4426950408889634
BF16 = jnp.bfloat16
F32 = jnp.float32


def rows_split(sp_count):
    keys = 2 if sp_count % 2 == 0 else 1
    while keys * keys * 4 <= sp_count:
        keys *= 2
    return keys, sp_count // keys


def dot_nt(a, b):
    return lax.dot_general(a, b, (((1,), (1,)), ((), ())), preferred_element_type=F32)


def dot_tn(a, b):
    return lax.dot_general(a, b, (((0,), (0,)), ((), ())), preferred_element_type=F32)


def flat_rows(block):
    count = block.shape[-2]
    shape = (-1, block.shape[-1])
    if count % 16:
        return block.astype(F32).reshape(shape).astype(BF16)
    return block.reshape(shape)


def kernel(
    sp_count,
    tp_count,
    log_rows,
    target,
    source,
    norm_gain,
    query_weight,
    key_weight,
    value_weight,
    output_weight,
    saved_out,
    log_shift,
    out_grad,
    target_grad,
    source_grad,
    query_weight_grad,
    tgt,
    src,
    gain,
    wq,
    wkv,
    wo,
    saved,
    shift,
    nbuf,
    obuf,
    kvown,
    kvbuf,
    qob,
    stat,
    nall,
    kacc,
    qacc,
    qfull,
    qsend,
    qrecv,
    qgall,
    ngf,
    ngs,
    ngr,
    ngx,
    ngin,
    kvs,
    kvr,
    kz,
    kzr,
    kfin,
    fin,
    ksum,
    in_sem,
    send_sem,
    recv_sem,
):
    nA, nB, nS, nT = kvbuf.shape[0], qob.shape[0], sp_count, tp_count
    nX = nT // 2
    nR = nT // KV_HEADS
    nr, width = tgt.shape
    sr = src.shape[0]
    lh = shift.shape[0]
    tr = saved.shape[0]
    trx = tr // nX
    ds_width = width // nS
    factor = HEAD_DIM ** (-0.5)
    s = lax.axis_index("sp")
    t = lax.axis_index("tp")
    x, c = t // 2, t % 2
    other = 1 - c
    part, pair = t % nR, t // nR
    zh, zl = s % nA, s // nA

    pending = []
    counts = {"send": 0, "recv": 0, "in": 0}

    def take(kind, n=1):
        first = counts[kind]
        counts[kind] += n
        return first

    def remote(src_ref, dst_ref, recv, where, keep=True):
        copy = pltpu.make_async_remote_copy(
            src_ref=src_ref,
            dst_ref=dst_ref,
            send_sem=send_sem.at[take("send")],
            recv_sem=recv_sem.at[recv],
            device_id=where,
            device_id_type=pl.DeviceIdType.MESH,
        )
        if keep:
            copy.start()
            pending.append(copy)
        return copy

    def arrive(dst_ref, recv, where):
        pltpu.make_async_remote_copy(
            src_ref=dst_ref,
            dst_ref=dst_ref,
            send_sem=send_sem.at[0],
            recv_sem=recv_sem.at[recv],
            device_id=where,
            device_id_type=pl.DeviceIdType.MESH,
        ).wait_recv()

    def fetch(src_ref, dst_ref):
        copy = pltpu.make_async_copy(src_ref, dst_ref, in_sem.at[take("in")])
        copy.start()
        return copy

    def tp_at(xx, cc):
        return {"tp": xx * 2 + cc}

    sibling = tp_at(x, other)

    got_t = fetch(target, tgt)
    got_g = fetch(norm_gain, gain)
    got_o = fetch(out_grad, obuf.at[x, c])
    got_kv = [fetch(source, src)]
    for g in range(KV_HEADS):
        cols = pl.ds(g * HEAD_DIM, HEAD_DIM)
        got_kv.append(fetch(key_weight.at[:, cols], wkv.at[:, pl.ds(2 * g * HEAD_DIM, HEAD_DIM)]))
        got_kv.append(
            fetch(value_weight.at[:, cols], wkv.at[:, pl.ds((2 * g + 1) * HEAD_DIM, HEAD_DIM)])
        )
    got_q = [
        fetch(query_weight, wq),
        fetch(output_weight, wo),
        fetch(saved_out, saved),
        fetch(log_shift, shift),
    ]

    barrier = pltpu.get_barrier_semaphore()
    for k in range(1, nT):
        pl.semaphore_signal(
            barrier, 1, device_id={"tp": (t + k) % nT}, device_id_type=pl.DeviceIdType.MESH
        )
    for k in range(1, nS):
        pl.semaphore_signal(
            barrier, 1, device_id={"sp": (s + k) % nS}, device_id_type=pl.DeviceIdType.MESH
        )

    got_t.wait()
    got_g.wait()
    wide = tgt[...].astype(F32)
    root = jnp.sqrt(jnp.mean(wide * wide, axis=1, keepdims=True) + 1e-06)
    nbuf[x, c] = (wide / root * gain[...]).astype(BF16)
    got_o.wait()
    pl.semaphore_wait(barrier, nT - 1 + nS - 1)

    n_recv = take("recv", 2 * nX)
    o_recv = take("recv", 2 * nX)
    bufs = ((nbuf, n_recv), (obuf, o_recv))
    for k in range(1, nX):
        for buf, base in bufs:
            remote(buf.at[x, c], buf.at[x, c], base + k, tp_at((x + k) % nX, c))
    for buf, base in bufs:
        remote(buf.at[x, c], buf.at[x, c], base, sibling)

    for copy in got_kv:
        copy.wait()
    own = jnp.dot(src[...], wkv[...], preferred_element_type=F32).astype(BF16)
    for g in range(KV_HEADS):
        kvown[g] = own[:, 2 * g * HEAD_DIM : 2 * (g + 1) * HEAD_DIM]
    kvbuf[0, t] = kvown[pair]
    kv_recv = take("recv", 2 * nX)
    for k in range(1, nX):
        xx = (x + k) % nX
        remote(kvown.at[xx * 2 // nR], kvbuf.at[0, t], kv_recv + k, tp_at(xx, c))
    remote(kvown.at[pair], kvbuf.at[0, t], kv_recv, sibling)
    kz_recv = take("recv", 2 * nA * nX)

    def keys_along(a_x, slot):
        for a in range(1, nA):
            remote(
                kvbuf.at[0, slot],
                kvbuf.at[a, slot],
                kz_recv + a * nX + a_x,
                {"sp": zl * nA + (zh + a) % nA},
            )

    keys_along(0, t)

    got_q[-1].wait()
    for xx in range(nX):
        for h in range(lh):
            cols = slice(h * trx, (h + 1) * trx)
            row = (shift[h : h + 1, xx * trx : (xx + 1) * trx] + log_rows) * LOG2E
            stat[0, xx, 0:1, cols] = row
    q_recv = take("recv", 2 * nB * nX)
    st_recv = take("recv", nB * nX)

    def project(k):
        xx = (x + nX - k) % nX
        q_rows = jnp.dot(flat_rows(nbuf[xx]), wq[...], preferred_element_type=F32).astype(BF16)
        for h in range(lh):
            cols = slice(h * HEAD_DIM, (h + 1) * HEAD_DIM)
            qob[0, xx, 0, h * trx : (h + 1) * trx, :] = q_rows[:, cols]
        for b in range(1, nB):
            where = {"sp": (zl + b) % nB * nA + zh}
            remote(qob.at[0, xx, 0], qob.at[b, xx, 0], q_recv + b * nX + k, where)
        o_rows = dot_nt(flat_rows(obuf[xx]), wo[...]).astype(BF16)
        keep = saved[pl.ds(pl.multiple_of(xx * trx, trx), trx), :].astype(F32)
        lane = lax.broadcasted_iota(jnp.int32, (trx, HEAD_DIM), 1)
        drops = jnp.zeros((trx, HEAD_DIM), F32)
        for h in range(lh):
            cols = slice(h * HEAD_DIM, (h + 1) * HEAD_DIM)
            rows = slice(h * trx, (h + 1) * trx)
            qob[0, xx, 1, rows, :] = o_rows[:, cols]
            term = jnp.sum(o_rows[:, cols].astype(F32) * keep[:, cols], axis=1, keepdims=True)
            drops = jnp.where(lane == h, term, drops)
        if trx < HEAD_DIM:
            drops = jnp.concatenate([drops, jnp.zeros((HEAD_DIM - trx, HEAD_DIM), F32)], axis=0)
        drops = drops.T
        for h in range(lh):
            stat[0, xx, 1:2, h * trx : (h + 1) * trx] = drops[h : h + 1, :trx]
        for b in range(1, nB):
            where = {"sp": (zl + b) % nB * nA + zh}
            remote(stat.at[0, xx], stat.at[b, xx], st_recv + b * nX + k, where)
            remote(qob.at[0, xx, 1], qob.at[b, xx, 1], q_recv + (nB + b) * nX + k, where)

    for copy in got_q[:-1]:
        copy.wait()
    for buf, base in bufs:
        arrive(buf.at[x, other], base, sibling)
    project(0)

    slots = [(b, a) for b in range(nB) for a in range(nA)]
    nz_recv = take("recv", nS * (1 + 2 * nX))

    def ahead(b, a):
        return (zl + b) % nB * nA + (zh + a) % nA

    def behind(b, a):
        return (zl + nB - b) % nB * nA + (zh + nA - a) % nA

    for n, (b, a) in enumerate(slots[1:], 1):
        to = ahead(b, a)
        cols = pl.ds(pl.multiple_of(to * ds_width, HEAD_DIM), ds_width)
        remote(nbuf.at[x, c, :, cols], nall.at[n, x, c], nz_recv + n, {"sp": to})

    for k in range(1, nX):
        xx = (x + nX - k) % nX
        for buf, base in bufs:
            arrive(buf.at[xx, c], base + k, tp_at(xx, c))
            remote(buf.at[xx, c], buf.at[xx, c], base + nX + k, sibling)
    for k in range(1, nX):
        xx = (x + nX - k) % nX
        for buf, base in bufs:
            arrive(buf.at[xx, other], base + nX + k, sibling)
        project(k)

    for k in range(1, nX):
        xx = (x + nX - k) % nX
        slot = xx * 2 + c
        arrive(kvbuf.at[0, slot], kv_recv + k, tp_at(xx, c))
        keys_along(k, slot)
        remote(kvbuf.at[0, slot], kvbuf.at[0, slot], kv_recv + nX + k, sibling)
    nall[0] = nbuf[:, :, :, pl.ds(pl.multiple_of(s * ds_width, HEAD_DIM), ds_width)]
    for k in range(1, nX):
        xx = (x + nX - k) % nX
        arrive(kvbuf.at[0, xx * 2 + other], kv_recv + nX + k, sibling)
    arrive(kvbuf.at[0, x * 2 + other], kv_recv, sibling)

    def attend(b, k, a):
        xx = (x + nX - k) % nX

        def step(i, carry):
            keys = kvbuf[a, i, :, :HEAD_DIM]
            values = kvbuf[a, i, :, HEAD_DIM:]
            queries = qob[b, xx, 0]
            backs = qob[b, xx, 1]
            score = dot_nt(keys, queries)
            prob = jnp.exp2(score * (factor * LOG2E) - stat[b, xx, 0:1, :])
            grad = (prob * (dot_nt(values, backs) - stat[b, xx, 1:2, :])).astype(BF16)
            key_part = jnp.dot(grad, queries, preferred_element_type=F32)
            value_part = jnp.dot(prob.astype(BF16), backs, preferred_element_type=F32)
            if b == 0 and k == 0:
                kacc[a, i, :, :HEAD_DIM] = key_part
                kacc[a, i, :, HEAD_DIM:] = value_part
            else:
                kacc[a, i, :, :HEAD_DIM] += key_part
                kacc[a, i, :, HEAD_DIM:] += value_part
            qacc[b, xx] += dot_tn(keys, grad)
            return carry

        lax.fori_loop(0, nT, step, 0, unroll=min(nT, 4))

    qs_recv = take("recv", nB * nB * nX)

    def send_queries(b, k):
        xx = (x + nX - k) % nX
        block = (qacc[b, xx] * factor).T
        qfull[b, xx] = block
        qsend[b, xx] = block.astype(BF16)
        for n in range(1, nB):
            slot = (n + b) % nB
            remote(
                qsend.at[b, xx],
                qrecv.at[n, slot, xx],
                qs_recv + (n * nB + slot) * nX + k,
                {"sp": (zl + n) % nB * nA + zh},
            )

    qacc[...] = jnp.zeros(qacc.shape, F32)
    for k in range(nX):
        attend(0, k, 0)

    for a in range(1, nA):
        for a_x in range(nX):
            slot = (x + nX - a_x) % nX * 2 + c
            idx = kz_recv + a * nX + a_x
            where = {"sp": zl * nA + (zh + nA - a) % nA}
            arrive(kvbuf.at[a, slot], idx, where)
            remote(kvbuf.at[a, slot], kvbuf.at[a, slot], idx + nA * nX, sibling)
        if a == 1:
            for n, (b, aa) in enumerate(slots[1:], 1):
                arrive(nall.at[n, x, c], nz_recv + n, {"sp": behind(b, aa)})
                base = nz_recv + nS + n * 2 * nX
                for j in range(1, nX):
                    remote(nall.at[n, x, c], nall.at[n, x, c], base + j, tp_at((x + j) % nX, c))
                remote(nall.at[n, x, c], nall.at[n, x, c], base, sibling)
        for a_x in range(nX):
            slot = (x + nX - a_x) % nX * 2 + other
            arrive(kvbuf.at[a, slot], kz_recv + a * nX + a_x + nA * nX, sibling)
        for k in range(nX):
            attend(0, k, a)
            if a == nA - 1:
                send_queries(0, k)

    kr_recv = take("recv", nA * nR)

    def send_keys(a):
        def convert(i, carry):
            kvs[a, i, :, :HEAD_DIM] = (kacc[a, i, :, :HEAD_DIM] * factor).astype(BF16)
            kvs[a, i, :, HEAD_DIM:] = kacc[a, i, :, HEAD_DIM:].astype(BF16)
            return carry

        lax.fori_loop(0, nT, convert, 0)
        for k in range(1, nR):
            to = (part + k) % nR
            remote(
                kvs.at[a, pl.ds(to * KV_HEADS, KV_HEADS)],
                kvr.at[k, a],
                kr_recv + a * nR + k,
                {"tp": pair * nR + to},
            )

    for k in range(nX):
        for b in range(1, nB):
            xx = (x + nX - k) % nX
            where = {"sp": (zl + nB - b) % nB * nA + zh}
            arrive(stat.at[b, xx], st_recv + b * nX + k, where)
            arrive(qob.at[b, xx, 0], q_recv + b * nX + k, where)
            arrive(qob.at[b, xx, 1], q_recv + (nB + b) * nX + k, where)
            last = k == nX - 1 and b == nB - 1
            for a in range(nA - 1, -1, -1):
                attend(b, k, a)
                if a == 0:
                    send_queries(b, k)
                if last:
                    send_keys(a)

    qg_recv = take("recv", nS)

    def finish_queries(b):
        for k in range(nX):
            xx = (x + nX - k) % nX
            total = qfull[b, xx]
            for n in range(1, nB):
                base = qs_recv + (n * nB + b) * nX + k
                arrive(qrecv.at[n, b, xx], base, {"sp": (zl + nB - n) % nB * nA + zh})
                total += qrecv[n, b, xx].astype(F32)
            total = total.astype(BF16)
            rows = pl.ds(pl.multiple_of(xx * trx, trx), trx)
            for h in range(lh):
                cols = slice(h * HEAD_DIM, (h + 1) * HEAD_DIM)
                qgall[b * nA, rows, cols] = total[h * trx : (h + 1) * trx, :]
        for a in range(1, nA):
            remote(
                qgall.at[b * nA],
                qgall.at[b * nA + a],
                qg_recv + b * nA + a,
                {"sp": zl * nA + (zh + a) % nA},
            )

    def portion(a, i):
        block = kacc[a, part * KV_HEADS + i]
        k_lane = lax.broadcasted_iota(jnp.int32, block.shape, 1) < HEAD_DIM
        block = jnp.where(k_lane, block * factor, block)
        for k in range(1, nR):
            block += kvr[k, a, i].astype(F32)
        return block

    ka_recv = take("recv", nA)
    for a in range(nA - 1, 0, -1):
        for k in range(1, nR):
            where = {"tp": pair * nR + (part + nR - k) % nR}
            arrive(kvr.at[k, a], kr_recv + a * nR + k, where)
        for i in range(KV_HEADS):
            kz[a, i] = portion(a, i).astype(BF16)
        remote(kz.at[a], kzr.at[a], ka_recv + a, {"sp": zl * nA + (zh + nA - a) % nA})

    for b in range(1, nB):
        finish_queries(b)

    for n, (b, a) in enumerate(slots[1:], 1):
        base = nz_recv + nS + n * 2 * nX
        for j in range(1, nX):
            xx = (x + nX - j) % nX
            arrive(nall.at[n, xx, c], base + j, tp_at(xx, c))
            remote(nall.at[n, xx, c], nall.at[n, xx, c], base + nX + j, sibling)

    finish_queries(0)

    step_cols = min(512, width)
    for i in range(width // step_cols):
        cols = slice(i * step_cols, (i + 1) * step_cols)
        share = dot_nt(qgall[0], wq[cols, :])
        ngf[:, :, :, cols] = share.reshape(nX, 2, nr, step_cols)
    for xx in range(nX):
        ngs[xx] = ngf[xx, other].astype(BF16)
    ng_recv = take("recv", nX)
    remote(ngs, ngr, ng_recv, sibling)

    for k in range(1, nR):
        arrive(kvr.at[k, 0], kr_recv + k, {"tp": pair * nR + (part + nR - k) % nR})
    for i in range(KV_HEADS):
        ksum[i] = portion(0, i)

    arrive(ngr, ng_recv, sibling)
    for k in range(1, nX):
        xx = (x + k) % nX
        ngx[k] = (ngf[xx, c] + ngr[xx].astype(F32)).astype(BF16)
        remote(ngx.at[k], ngin.at[k], ng_recv + k, tp_at(xx, c))

    for a in range(1, nA):
        arrive(kzr.at[a], ka_recv + a, {"sp": zl * nA + (zh + a) % nA})
    f_recv = take("recv", KV_HEADS)
    owner_sends = []
    for i in range(KV_HEADS):
        block = ksum[i]
        for a in range(1, nA):
            block += kzr[a, i].astype(F32)
        kfin[i] = block.astype(BF16)
        owner = part * KV_HEADS + i
        copy = remote(kfin.at[i], fin.at[pair], f_recv + pair, {"tp": owner}, keep=False)
        owner_sends.append((owner, copy))

        @pl.when(owner != t)
        def _():
            copy.start()

        @pl.when(owner == t)
        def _():
            fin[pair] = kfin[i]

    for n, (b, a) in enumerate(slots):
        if n:
            base = nz_recv + nS + n * 2 * nX
            arrive(nall.at[n, x, other], base, sibling)
            for j in range(1, nX):
                arrive(nall.at[n, (x + nX - j) % nX, other], base + nX + j, sibling)
    order = [b * nA for b in range(nB)] + [b * nA + a for b in list(range(1, nB)) + [0] for a in range(1, nA)]
    for n in order:
        if n % nA:
            arrive(qgall.at[n], qg_recv + n, {"sp": zl * nA + (zh + nA - n % nA) % nA})
        piece = dot_tn(flat_rows(nall[n]), qgall[n])
        if n == 0:
            query_weight_grad[...] = piece
        else:
            query_weight_grad[...] += piece

    grad = ngf[x, c] + ngr[x].astype(F32)
    for k in range(1, nX):
        arrive(ngin.at[k], ng_recv + k, tp_at((x + nX - k) % nX, c))
        grad += ngin[k].astype(F32)
    scaled = grad * gain[...]
    wide = tgt[...].astype(F32)
    root = jnp.sqrt(jnp.mean(wide * wide, axis=1, keepdims=True) + 1e-06)
    target_grad[...] = scaled / root - wide * jnp.mean(scaled * wide, axis=1, keepdims=True) / (
        root * root * root
    )

    for g in range(KV_HEADS):
        giver = g * nR + t // KV_HEADS

        @pl.when(giver != t)
        def _():
            arrive(fin.at[g], f_recv + g, {"tp": giver})

    for i in range(width // step_cols):
        rows = pl.ds(i * step_cols, step_cols)
        part_sum = dot_nt(fin[0], wkv[rows, 0 : 2 * HEAD_DIM])
        for g in range(1, KV_HEADS):
            part_sum += dot_nt(fin[g], wkv[rows, 2 * g * HEAD_DIM : 2 * (g + 1) * HEAD_DIM])
        source_grad[:, rows] = part_sum

    for copy in pending:
        copy.wait_send()
    for owner, copy in owner_sends:

        @pl.when(owner != t)
        def _():
            copy.wait_send()


def square_kernel(
    log_rows,
    target,
    source,
    norm_gain,
    query_weight,
    key_weight,
    value_weight,
    output_weight,
    saved_out,
    log_shift,
    out_grad,
    target_grad,
    source_grad,
    query_weight_grad,
    tgt,
    src,
    gain,
    wq,
    wkv,
    wo,
    saved,
    shift,
    nbuf,
    obuf,
    kvown,
    kvbuf,
    kvpeer,
    qob,
    stat,
    nall,
    kacc,
    qacc,
    qfull,
    qsend,
    qrecv,
    qgall,
    ngf,
    ngs,
    ngr,
    ngx,
    ngin,
    kvs,
    kvr,
    kz,
    kzr,
    kfin,
    fin,
    bulk,
    in_sem,
    send_sem,
    recv_sem,
):
    nr, width = tgt.shape
    lh = shift.shape[0]
    tr = saved.shape[0]
    nS, nT = 4, 4
    trx = tr // 2
    ds_width = width // nS
    factor = HEAD_DIM ** (-0.5)
    s = lax.axis_index("sp")
    t = lax.axis_index("tp")
    x, c = t // 2, t % 2
    ox, other = 1 - x, 1 - c
    peer = s + 1 - 2 * (s % 2)
    far = (s + 2) % nS
    diag = (peer + 2) % nS
    sib = {"tp": x * 2 + other}
    across = {"tp": ox * 2 + c}
    to_peer = {"sp": peer}
    to_far = {"sp": far}
    to_diag = {"sp": diag}

    keys = {("fin", 0): 0, ("fin", 1): 1}
    counts = {"in": 0}

    def sem(*key):
        return keys.setdefault(key, len(keys))

    def fetch(src_ref, dst_ref, at=None):
        if at is None:
            at = counts["in"]
            counts["in"] += 1
        copy = pltpu.make_async_copy(src_ref, dst_ref, in_sem.at[at])
        copy.start()
        return copy

    barrier = pltpu.get_barrier_semaphore()
    for k in range(1, nT):
        pl.semaphore_signal(
            barrier, 1, device_id={"tp": (t + k) % nT}, device_id_type=pl.DeviceIdType.MESH
        )
    for k in range(1, nS):
        pl.semaphore_signal(
            barrier, 1, device_id={"sp": (s + k) % nS}, device_id_type=pl.DeviceIdType.MESH
        )

    got_t = fetch(target, tgt)
    got_g = fetch(norm_gain, gain)
    got_shift = fetch(log_shift, shift)
    got_o = fetch(out_grad, obuf.at[x, c])
    got_kv = [fetch(source, src)]
    for g in range(KV_HEADS):
        cols = pl.ds(g * HEAD_DIM, HEAD_DIM)
        got_kv.append(fetch(key_weight.at[:, cols], wkv.at[:, pl.ds(2 * g * HEAD_DIM, HEAD_DIM)]))
        got_kv.append(
            fetch(value_weight.at[:, cols], wkv.at[:, pl.ds((2 * g + 1) * HEAD_DIM, HEAD_DIM)])
        )
    got_q = fetch(query_weight, wq)
    got_w = fetch(output_weight, wo)
    got_saved = fetch(saved_out, saved)

    got_t.wait()
    got_g.wait()
    wide = tgt[...].astype(F32)
    root = jnp.sqrt(jnp.mean(wide * wide, axis=1, keepdims=True) + 1e-06)
    nbuf[x, c] = (wide / root * gain[...]).astype(BF16)
    got_o.wait()
    pl.semaphore_wait(barrier, nT - 1 + nS - 1)

    pending, sent = [], []

    def remote(src_ref, dst_ref, key, where, keep=True):
        shared = keep and src_ref.dtype == BF16
        if shared:
            sent.append(math.prod(src_ref.shape) * 2)
        copy = pltpu.make_async_remote_copy(
            src_ref=src_ref,
            dst_ref=dst_ref,
            send_sem=send_sem.at[0 if shared else len(pending) + 1],
            recv_sem=recv_sem.at[sem(*key) if isinstance(key, tuple) else key],
            device_id=where,
            device_id_type=pl.DeviceIdType.MESH,
        )
        if keep:
            copy.start()
        if not shared:
            pending.append((copy, keep))
        return copy

    def arrive(dst_ref, key, where):
        pltpu.make_async_remote_copy(
            src_ref=dst_ref,
            dst_ref=dst_ref,
            send_sem=send_sem.at[0],
            recv_sem=recv_sem.at[sem(*key)],
            device_id=where,
            device_id_type=pl.DeviceIdType.MESH,
        ).wait_recv()

    def scope(name):
        return jax.named_scope(name)

    remote(nbuf.at[x, c], nbuf.at[x, c], ("n", "x"), across)
    remote(nbuf.at[x, c], nbuf.at[x, c], ("n", "s"), sib)
    remote(obuf.at[x, c], obuf.at[x, c], ("o", "s"), sib)
    remote(obuf.at[x, c], obuf.at[x, c], ("o", "x"), across)
    def slice_sends():
        for v, where, to in ((2, to_peer, peer), (1, to_far, far), (3, to_diag, diag)):
            cols = pl.ds(pl.multiple_of(to * ds_width, HEAD_DIM), ds_width)
            remote(nbuf.at[x, c, :, cols], nall.at[v, x, c], ("na", v), where)

    slice_sends()
    for copy in got_kv:
        copy.wait()
    with scope("kvproj"):
        own = jnp.dot(src[...], wkv[...], preferred_element_type=F32).astype(BF16)
        for g in range(KV_HEADS):
            kvown[g] = own[:, 2 * g * HEAD_DIM : 2 * (g + 1) * HEAD_DIM]
        kvbuf[0, t] = kvown[x]
    remote(kvown.at[x], kvbuf.at[0, t], ("kv", "s"), sib)
    remote(kvown.at[ox], kvbuf.at[0, t], ("kv", "x"), across)
    got_shift.wait()
    for k in range(2):
        xx = x if k == 0 else ox
        for h in range(lh):
            row = jnp.where(xx == 0, shift[h : h + 1, 0:trx], shift[h : h + 1, trx : 2 * trx])
            stat[0, k, 0:1, h * trx : (h + 1) * trx] = (row + log_rows) * LOG2E

    def send_far(ref, kind, k):
        remote(ref.at[0, k], ref.at[1, k], (kind, k), to_far)

    def send_part(i, kind, k):
        remote(qob.at[0, k, i], qob.at[1, k, i], (kind, k), to_far)

    def project_q(k):
        with scope(f"project_q{k}"):
            xx = x if k == 0 else ox
            rows = jnp.dot(flat_rows(nbuf[xx]), wq[...], preferred_element_type=F32).astype(BF16)
            for h in range(lh):
                cols = slice(h * HEAD_DIM, (h + 1) * HEAD_DIM)
                qob[0, k, 0, h * trx : (h + 1) * trx, :] = rows[:, cols]
        send_part(0, "q", k)

    def project_o(k):
        with scope(f"project_o{k}"):
            xx = x if k == 0 else ox
            o_rows = dot_nt(flat_rows(obuf[xx]), wo[...]).astype(BF16)
            for h in range(lh):
                cols = slice(h * HEAD_DIM, (h + 1) * HEAD_DIM)
                qob[0, k, 1, h * trx : (h + 1) * trx, :] = o_rows[:, cols]
        send_part(1, "ob", k)
        with scope(f"drop{k}"):
            keep = saved[pl.ds(pl.multiple_of(xx * trx, trx), trx), :].astype(F32)
            lane = lax.broadcasted_iota(jnp.int32, (trx, HEAD_DIM), 1)
            drops = jnp.zeros((trx, HEAD_DIM), F32)
            for h in range(lh):
                cols = slice(h * HEAD_DIM, (h + 1) * HEAD_DIM)
                term = jnp.sum(o_rows[:, cols].astype(F32) * keep[:, cols], axis=1, keepdims=True)
                drops = jnp.where(lane == h, term, drops)
            drops = jnp.concatenate([drops, jnp.zeros((HEAD_DIM - trx, HEAD_DIM), F32)], axis=0)
            drops = drops.T
            for h in range(lh):
                stat[0, k, 1:2, h * trx : (h + 1) * trx] = drops[h : h + 1, :trx]
        send_far(stat, "st", k)

    def need(k):
        with scope(f"w_q{k}"):
            arrive(qob.at[1, k, 0], ("q", k), to_far)
        with scope(f"w_ob{k}"):
            arrive(qob.at[1, k, 1], ("ob", k), to_far)
            arrive(stat.at[1, k], ("st", k), to_far)

    got = {"kacc": set(), "qacc": set()}

    def attend(v, k, a, g):
        with scope(f"attend_{v}{k}{a}{g}"):
            attend_rows(v, k, a, g)

    def attend_rows(v, k, a, g):
        pair = pl.ds(2 * (x if g == 0 else ox), 2)
        sr = kvbuf.shape[2]
        k_rows = kvbuf[a, pair, :, :HEAD_DIM].reshape(2 * sr, HEAD_DIM)
        v_rows = kvbuf[a, pair, :, HEAD_DIM:].reshape(2 * sr, HEAD_DIM)
        queries = qob[v, k, 0]
        backs = qob[v, k, 1]
        score = dot_nt(k_rows, queries)
        prob = jnp.exp2(score * (factor * LOG2E) - stat[v, k, 0:1, :])
        grad = (prob * (dot_nt(v_rows, backs) - stat[v, k, 1:2, :])).astype(BF16)
        key_part = jnp.dot(grad, queries, preferred_element_type=F32)
        value_part = jnp.dot(prob.astype(BF16), backs, preferred_element_type=F32)
        key_part = key_part.reshape(2, sr, HEAD_DIM)
        value_part = value_part.reshape(2, sr, HEAD_DIM)
        if (a, g) not in got["kacc"]:
            kacc[a, pair, :, :HEAD_DIM] = key_part
            kacc[a, pair, :, HEAD_DIM:] = value_part
        else:
            kacc[a, pair, :, :HEAD_DIM] += key_part
            kacc[a, pair, :, HEAD_DIM:] += value_part
        if (v, k) not in got["qacc"]:
            qacc[v, k] = dot_tn(k_rows, grad)
            got["qacc"].add((v, k))
        else:
            qacc[v, k] += dot_tn(k_rows, grad)
        got["kacc"].add((a, g))

    def query_part(v, k):
        return (qacc[v, k] * factor).T

    def send_keys(a):
        with scope(f"keys{a}"):
            for i in range(2):
                slot = 2 * other + i
                kvs[a, i, :, :HEAD_DIM] = (kacc[a, slot, :, :HEAD_DIM] * factor).astype(BF16)
                kvs[a, i, :, HEAD_DIM:] = kacc[a, slot, :, HEAD_DIM:].astype(BF16)
        remote(kvs.at[a], kvr.at[a], ("kp", a), sib)

    def key_sum(a, i):
        block = kacc[a, 2 * c + i]
        k_lane = lax.broadcasted_iota(jnp.int32, block.shape, 1) < HEAD_DIM
        return jnp.where(k_lane, block * factor, block) + kvr[a, i].astype(F32)

    def keys_back():
        with scope("w_kp1"):
            arrive(kvr.at[1], ("kp", 1), sib)
        with scope("kz"):
            for i in range(2):
                kz[i] = key_sum(1, i).astype(BF16)
        remote(kz, kzr, ("kz",), to_peer)

    def slice_from(v):
        return (None, to_far, to_peer, to_diag)[v]

    def slice_pass(v):
        with scope(f"w_na{v}"):
            arrive(nall.at[v, x, c], ("na", v), slice_from(v))
        remote(nall.at[v, x, c], nall.at[v, x, c], ("na", v, "x"), across)
        remote(nall.at[v, x, c], nall.at[v, x, c], ("na", v, "s"), sib)

    def slice_turn(v):
        with scope(f"w_nx{v}"):
            arrive(nall.at[v, ox, c], ("na", v, "x"), across)
        remote(nall.at[v, ox, c], nall.at[v, ox, c], ("na", v, "t"), sib)

    def slice_end(v):
        with scope(f"w_ns{v}"):
            arrive(nall.at[v, x, other], ("na", v, "s"), sib)
            arrive(nall.at[v, ox, other], ("na", v, "t"), sib)

    def total_rows(v, k):
        xx = x if k == 0 else ox
        return qgall.at[v, pl.ds(pl.multiple_of(xx * trx, trx), trx), :]

    pieces = []

    def weight_piece(v):
        with scope(f"piece{v}"):
            piece = dot_tn(flat_rows(nall[v]), qgall[v])
            if not pieces:
                query_weight_grad[...] = piece
            else:
                query_weight_grad[...] += piece
            pieces.append(v)

    step_cols = min(512, width)

    def normed_share():
        with scope("ng_share"):
            for i in range(width // step_cols):
                cols = slice(i * step_cols, (i + 1) * step_cols)
                share = dot_nt(qgall[0], wq[cols, :])
                ngf[:, :, :, cols] = share.reshape(2, 2, nr, step_cols)
            for xx in range(2):
                ngs[xx] = ngf[xx, other].astype(BF16)
        remote(ngs, ngr, ("ng", "s"), sib)

    def normed_cross():
        with scope("w_ngs"):
            arrive(ngr, ("ng", "s"), sib)
        ngx[...] = (ngf[ox, c] + ngr[ox].astype(F32)).astype(BF16)
        remote(ngx, ngin, ("ng", "x"), across)

    def normed_end():
        with scope("w_ngx"):
            arrive(ngin, ("ng", "x"), across)
        with scope("target"):
            grad = ngf[x, c] + ngr[x].astype(F32) + ngin[...].astype(F32)
            scaled = grad * gain[...]
            wide = tgt[...].astype(F32)
            root = jnp.sqrt(jnp.mean(wide * wide, axis=1, keepdims=True) + 1e-06)
            target_grad[...] = scaled / root - wide * jnp.mean(
                scaled * wide, axis=1, keepdims=True
            ) / (root * root * root)

    owner_sends = []

    def keys_out():
        with scope("w_kp0"):
            arrive(kvr.at[0], ("kp", 0), sib)
        with scope("w_kz"):
            arrive(kzr, ("kz",), to_peer)
        with scope("keys_out"):
            for i in range(2):
                block = key_sum(0, i) + kzr[i].astype(F32)
                kfin[i] = block.astype(BF16)
                owner = c * 2 + i
                copy = remote(kfin.at[i], fin.at[x], x, {"tp": owner}, keep=False)
                owner_sends.append((owner, copy))

                @pl.when(owner != t)
                def _():
                    copy.start()

                @pl.when(owner == t)
                def _():
                    fin[x] = kfin[i]

    def source_end():
        for g in range(KV_HEADS):
            giver = g * 2 + t // 2

            @pl.when(giver != t)
            def _():
                with scope("w_fin"):
                    arrive(fin.at[g], ("fin", g), {"tp": giver})

        with scope("source"):
            for i in range(width // step_cols):
                rows = pl.ds(i * step_cols, step_cols)
                part_sum = dot_nt(fin[0], wkv[rows, 0 : 2 * HEAD_DIM])
                for g in range(1, KV_HEADS):
                    part_sum += dot_nt(fin[g], wkv[rows, 2 * g * HEAD_DIM : 2 * (g + 1) * HEAD_DIM])
                source_grad[:, rows] = part_sum

    def pass_on(buf, kind):
        with scope(f"w_{kind}x"):
            arrive(buf.at[ox, c], (kind, "x"), across)
        remote(buf.at[ox, c], buf.at[ox, c], (kind, "t"), sib)

    def passed(buf, kind):
        with scope(f"w_{kind}t"):
            arrive(buf.at[ox, other], (kind, "t"), sib)

    def grad_out(b, k):
        with scope(f"dq_{b}{k}"):
            block = query_part(b, k)
            qfull[b, k] = block
            qsend[b, k] = block.astype(BF16)
        remote(qsend.at[b, k], qrecv.at[1 - b, k], ("dq", 1 - b, k), to_far)

    def total_out(b, k):
        with scope(f"w_dq{b}{k}"):
            arrive(qrecv.at[b, k], ("dq", b, k), to_far)
        with scope(f"total_{b}{k}"):
            total = (qfull[b, k] + qrecv[b, k].astype(F32)).astype(BF16)
            rows = pl.ds(pl.multiple_of((x if k == 0 else ox) * trx, trx), trx)
            for h in range(lh):
                cols = slice(h * HEAD_DIM, (h + 1) * HEAD_DIM)
                qgall[b, rows, cols] = total[h * trx : (h + 1) * trx, :]
        remote(total_rows(b, k), total_rows(2 + b, k), ("tot", b, k), to_peer)

    def total_in(b, k):
        with scope(f"w_tot{b}{k}"):
            arrive(total_rows(2 + b, k), ("tot", b, k), to_peer)

    def peer_keys(chip, kind):
        with scope(f"w_{kind}"):
            arrive(kvbuf.at[1, 2 * chip + c], (kind,), to_peer if chip is x else across)
        remote(kvbuf.at[1, 2 * chip + c], kvbuf.at[1, 2 * chip + c], (kind, "s"), sib)

    def peer_keys_end(chip, kind):
        with scope(f"w_{kind}s"):
            arrive(kvbuf.at[1, 2 * chip + other], (kind, "s"), sib)

    remote(kvown.at[ox], kvpeer, ("kp",), to_peer)
    with scope("w_ns"):
        arrive(nbuf.at[x, other], ("n", "s"), sib)
    got_q.wait()
    project_q(0)
    with scope("w_os"):
        arrive(obuf.at[x, other], ("o", "s"), sib)
    got_w.wait()
    got_saved.wait()
    project_o(0)
    remote(kvown.at[x], kvbuf.at[1, t], ("ke",), to_peer)
    with scope("w_kvs"):
        arrive(kvbuf.at[0, x * 2 + other], ("kv", "s"), sib)
    attend(0, 0, 0, 0)
    pass_on(nbuf, "n")
    passed(nbuf, "n")
    project_q(1)
    pass_on(obuf, "o")
    with scope("w_kpx"):
        arrive(kvpeer, ("kp",), to_peer)
    remote(kvpeer, kvbuf.at[1, t], ("kx",), across)
    passed(obuf, "o")
    project_o(1)
    with scope("w_kvx"):
        arrive(kvbuf.at[0, 2 * ox + c], ("kv", "x"), across)
    remote(kvbuf.at[0, 2 * ox + c], kvbuf.at[0, 2 * ox + c], ("kv", "t"), sib)
    attend(0, 1, 0, 0)
    need(0)
    attend(1, 0, 0, 0)
    with scope("w_kvt"):
        arrive(kvbuf.at[0, 2 * ox + other], ("kv", "t"), sib)
    attend(0, 0, 0, 1)
    attend(1, 0, 0, 1)
    peer_keys(ox, "kx")
    attend(0, 1, 0, 1)
    peer_keys(x, "ke")
    peer_keys_end(ox, "kx")
    attend(1, 0, 1, 1)
    peer_keys_end(x, "ke")
    attend(1, 0, 1, 0)
    grad_out(1, 0)
    attend(0, 0, 1, 0)
    attend(0, 0, 1, 1)
    grad_out(0, 0)
    attend(0, 1, 1, 0)
    attend(0, 1, 1, 1)
    need(1)
    attend(1, 1, 1, 0)
    attend(1, 1, 1, 1)
    send_keys(1)
    attend(1, 1, 0, 0)
    attend(1, 1, 0, 1)
    grad_out(1, 1)
    grad_out(0, 1)
    send_keys(0)
    keys_back()
    for v in (1, 2, 3):
        slice_pass(v)
    nall[0] = nbuf[:, :, :, pl.ds(pl.multiple_of(s * ds_width, HEAD_DIM), ds_width)]
    total_out(0, 0)
    total_out(1, 0)
    for v in (1, 2, 3):
        slice_turn(v)
    total_out(0, 1)
    normed_share()
    for v in (1, 2, 3):
        slice_end(v)
    weight_piece(0)
    normed_cross()
    total_out(1, 1)
    weight_piece(1)
    keys_out()
    total_in(0, 0)
    total_in(1, 0)
    total_in(0, 1)
    weight_piece(2)
    normed_end()
    source_end()
    total_in(1, 1)
    weight_piece(3)

    with scope("w_send"):
        whole = bulk.at[pl.ds(0, sum(sent) // (bulk.shape[1] * 4))]
        pltpu.make_async_copy(whole, whole, send_sem.at[0]).wait()
        for copy, kept in pending:
            if kept:
                copy.wait_send()
        for owner, copy in owner_sends:

            @pl.when(owner != t)
            def _():
                copy.wait_send()


def square_scratch(nr, width, sr, tr, lh, head_width):
    vm = pltpu.VMEM
    m = lh * tr // 2
    ds_width = width // 4
    kv = 2 * HEAD_DIM
    return [
        vm((nr, width), BF16),
        vm((sr, width), BF16),
        vm((1, width), F32),
        vm((width, head_width), BF16),
        vm((width, KV_HEADS * kv), BF16),
        vm((head_width, width), BF16),
        vm((tr, head_width), BF16),
        vm((lh, tr), F32),
        vm((2, 2, nr, width), BF16),
        vm((2, 2, nr, width), BF16),
        vm((KV_HEADS, sr, kv), BF16),
        vm((2, 4, sr, kv), BF16),
        vm((sr, kv), BF16),
        vm((2, 2, 2, m, HEAD_DIM), BF16),
        vm((2, 2, 2, m), F32),
        vm((4, 2, 2, nr, ds_width), BF16),
        vm((2, 4, sr, kv), F32),
        vm((2, 2, HEAD_DIM, m), F32),
        vm((2, 2, m, HEAD_DIM), F32),
        vm((2, 2, m, HEAD_DIM), BF16),
        vm((2, 2, m, HEAD_DIM), BF16),
        vm((4, tr, head_width), BF16),
        vm((2, 2, nr, width), F32),
        vm((2, nr, width), BF16),
        vm((2, nr, width), BF16),
        vm((nr, width), BF16),
        vm((nr, width), BF16),
        vm((2, 2, sr, kv), BF16),
        vm((2, 2, sr, kv), BF16),
        vm((2, sr, kv), BF16),
        vm((2, sr, kv), BF16),
        vm((2, sr, kv), BF16),
        vm((2, sr, kv), BF16),
        vm((8 * sr, width // 2), F32),
        pltpu.SemaphoreType.DMA((12,)),
        pltpu.SemaphoreType.DMA((6,)),
        pltpu.SemaphoreType.DMA((48,)),
    ]


def shards(
    target,
    source,
    norm_gain,
    query_weight,
    key_weight,
    value_weight,
    output_weight,
    saved_out,
    log_shift,
    out_grad,
):
    nT = lax.axis_size("tp")
    nS = lax.axis_size("sp")
    nA, nB = rows_split(nS)
    nX, nR = nT // 2, nT // KV_HEADS
    nr, width = target.shape
    sr = source.shape[0]
    tr, head_width = saved_out.shape
    lh = head_width // HEAD_DIM
    m = lh * tr // nX
    ds_width = width // nS
    kv = 2 * HEAD_DIM
    log_rows = math.log(sr * nT * nS)
    vm = pltpu.VMEM
    outputs = 4 * (nr * width + sr * width + ds_width * head_width)
    limit = 67043328 - outputs - 65536
    sems = min(8 * nS * nT, 1024)
    scratch = [
        vm((nr, width), BF16),
        vm((sr, width), BF16),
        vm((1, width), F32),
        vm((width, head_width), BF16),
        vm((width, KV_HEADS * kv), BF16),
        vm((head_width, width), BF16),
        vm((tr, head_width), BF16),
        vm((lh, tr), F32),
        vm((nX, 2, nr, width), BF16),
        vm((nX, 2, nr, width), BF16),
        vm((KV_HEADS, sr, kv), BF16),
        vm((nA, nT, sr, kv), BF16),
        vm((nB, nX, 2, m, HEAD_DIM), BF16),
        vm((nB, nX, 2, m), F32),
        vm((nS, nX, 2, nr, ds_width), BF16),
        vm((nA, nT, sr, kv), F32),
        vm((nB, nX, HEAD_DIM, m), F32),
        vm((nB, nX, m, HEAD_DIM), F32),
        vm((nB, nX, m, HEAD_DIM), BF16),
        vm((nB, nB, nX, m, HEAD_DIM), BF16),
        vm((nS, tr, head_width), BF16),
        vm((nX, 2, nr, width), F32),
        vm((nX, nr, width), BF16),
        vm((nX, nr, width), BF16),
        vm((nX, nr, width), BF16),
        vm((nX, nr, width), BF16),
        vm((nA, nT, sr, kv), BF16),
        vm((nR, nA, KV_HEADS, sr, kv), BF16),
        vm((nA, KV_HEADS, sr, kv), BF16),
        vm((nA, KV_HEADS, sr, kv), BF16),
        vm((KV_HEADS, sr, kv), BF16),
        vm((KV_HEADS, sr, kv), BF16),
        vm((KV_HEADS, sr, kv), F32),
        pltpu.SemaphoreType.DMA((16,)),
        pltpu.SemaphoreType.DMA((sems,)),
        pltpu.SemaphoreType.DMA((sems,)),
    ]
    body = functools.partial(kernel, nS, nT, log_rows)
    if nS == 4 and nT == 4:
        body = functools.partial(square_kernel, log_rows)
        scratch = square_scratch(nr, width, sr, tr, lh, head_width)
    anywhere = pl.BlockSpec(memory_space=pltpu.HBM)
    return pl.pallas_call(
        body,
        out_shape=(
            pltpu.VMEM((nr, width), F32),
            pltpu.VMEM((sr, width), F32),
            pltpu.VMEM((ds_width, head_width), F32),
        ),
        in_specs=[anywhere] * 10,
        out_specs=(pl.BlockSpec(memory_space=pltpu.VMEM),) * 3,
        scratch_shapes=scratch,
        compiler_params=pltpu.CompilerParams(
            collective_id=0, has_side_effects=True, vmem_limit_bytes=limit
        ),
        name="cross_back",
    )(
        target,
        source,
        norm_gain.reshape(1, width),
        query_weight,
        key_weight,
        value_weight,
        output_weight,
        saved_out,
        log_shift,
        out_grad,
    )


def solution(mesh):
    return jax.shard_map(
        shards,
        mesh=mesh,
        in_specs=(
            P(("grp", "sp", "tp"), None),
            P(("grp", "sp", "tp"), None),
            P(),
            P(None, "tp"),
            P(),
            P(),
            P("tp", None),
            P(("grp", "sp"), "tp"),
            P("tp", ("grp", "sp")),
            P(("grp", "sp", "tp"), None),
        ),
        out_specs=(
            P(("grp", "sp", "tp"), None),
            P(("grp", "sp", "tp"), None),
            P(("grp", "sp"), "tp"),
        ),
        check_vma=False,
    )
```

```python
import functools
import math

import jax
import jax.numpy as jnp
from jax import lax
from jax.experimental import pallas as pl
from jax.experimental.pallas import tpu as pltpu
from jax.sharding import PartitionSpec as P

HEADS = 16
HEAD_DIM = 128
KV_HEADS = 2
LOG2E = 1.4426950408889634
BF16 = jnp.bfloat16
F32 = jnp.float32


def rows_split(sp_count):
    keys = 2 if sp_count % 2 == 0 else 1
    while keys * keys * 4 <= sp_count:
        keys *= 2
    return keys, sp_count // keys


def dot_nt(a, b):
    return lax.dot_general(a, b, (((1,), (1,)), ((), ())), preferred_element_type=F32)


def dot_tn(a, b):
    return lax.dot_general(a, b, (((0,), (0,)), ((), ())), preferred_element_type=F32)


def flat_rows(block):
    count = block.shape[-2]
    shape = (-1, block.shape[-1])
    if count % 16:
        return block.astype(F32).reshape(shape).astype(BF16)
    return block.reshape(shape)


def kernel(
    sp_count,
    tp_count,
    log_rows,
    target,
    source,
    norm_gain,
    query_weight,
    key_weight,
    value_weight,
    output_weight,
    saved_out,
    log_shift,
    out_grad,
    target_grad,
    source_grad,
    query_weight_grad,
    tgt,
    src,
    gain,
    wq,
    wkv,
    wo,
    saved,
    shift,
    nbuf,
    obuf,
    kvown,
    kvbuf,
    qob,
    stat,
    nall,
    kacc,
    qacc,
    qfull,
    qsend,
    qrecv,
    qgall,
    ngf,
    ngs,
    ngr,
    ngx,
    ngin,
    kvs,
    kvr,
    kz,
    kzr,
    kfin,
    fin,
    ksum,
    in_sem,
    send_sem,
    recv_sem,
):
    nA, nB, nS, nT = kvbuf.shape[0], qob.shape[0], sp_count, tp_count
    nX = nT // 2
    nR = nT // KV_HEADS
    nr, width = tgt.shape
    sr = src.shape[0]
    lh = shift.shape[0]
    tr = saved.shape[0]
    trx = tr // nX
    ds_width = width // nS
    factor = HEAD_DIM ** (-0.5)
    s = lax.axis_index("sp")
    t = lax.axis_index("tp")
    x, c = t // 2, t % 2
    other = 1 - c
    part, pair = t % nR, t // nR
    zh, zl = s % nA, s // nA

    pending = []
    counts = {"send": 0, "recv": 0, "in": 0}

    def take(kind, n=1):
        first = counts[kind]
        counts[kind] += n
        return first

    def remote(src_ref, dst_ref, recv, where, keep=True):
        copy = pltpu.make_async_remote_copy(
            src_ref=src_ref,
            dst_ref=dst_ref,
            send_sem=send_sem.at[take("send")],
            recv_sem=recv_sem.at[recv],
            device_id=where,
            device_id_type=pl.DeviceIdType.MESH,
        )
        if keep:
            copy.start()
            pending.append(copy)
        return copy

    def arrive(dst_ref, recv, where):
        pltpu.make_async_remote_copy(
            src_ref=dst_ref,
            dst_ref=dst_ref,
            send_sem=send_sem.at[0],
            recv_sem=recv_sem.at[recv],
            device_id=where,
            device_id_type=pl.DeviceIdType.MESH,
        ).wait_recv()

    def fetch(src_ref, dst_ref):
        copy = pltpu.make_async_copy(src_ref, dst_ref, in_sem.at[take("in")])
        copy.start()
        return copy

    def tp_at(xx, cc):
        return {"tp": xx * 2 + cc}

    sibling = tp_at(x, other)

    got_t = fetch(target, tgt)
    got_g = fetch(norm_gain, gain)
    got_o = fetch(out_grad, obuf.at[x, c])
    got_kv = [fetch(source, src)]
    for g in range(KV_HEADS):
        cols = pl.ds(g * HEAD_DIM, HEAD_DIM)
        got_kv.append(fetch(key_weight.at[:, cols], wkv.at[:, pl.ds(2 * g * HEAD_DIM, HEAD_DIM)]))
        got_kv.append(
            fetch(value_weight.at[:, cols], wkv.at[:, pl.ds((2 * g + 1) * HEAD_DIM, HEAD_DIM)])
        )
    got_q = [
        fetch(query_weight, wq),
        fetch(output_weight, wo),
        fetch(saved_out, saved),
        fetch(log_shift, shift),
    ]

    barrier = pltpu.get_barrier_semaphore()
    for k in range(1, nT):
        pl.semaphore_signal(
            barrier, 1, device_id={"tp": (t + k) % nT}, device_id_type=pl.DeviceIdType.MESH
        )
    for k in range(1, nS):
        pl.semaphore_signal(
            barrier, 1, device_id={"sp": (s + k) % nS}, device_id_type=pl.DeviceIdType.MESH
        )

    got_t.wait()
    got_g.wait()
    wide = tgt[...].astype(F32)
    root = jnp.sqrt(jnp.mean(wide * wide, axis=1, keepdims=True) + 1e-06)
    nbuf[x, c] = (wide / root * gain[...]).astype(BF16)
    got_o.wait()
    pl.semaphore_wait(barrier, nT - 1 + nS - 1)

    n_recv = take("recv", 2 * nX)
    o_recv = take("recv", 2 * nX)
    bufs = ((nbuf, n_recv), (obuf, o_recv))
    for k in range(1, nX):
        for buf, base in bufs:
            remote(buf.at[x, c], buf.at[x, c], base + k, tp_at((x + k) % nX, c))
    for buf, base in bufs:
        remote(buf.at[x, c], buf.at[x, c], base, sibling)

    for copy in got_kv:
        copy.wait()
    own = jnp.dot(src[...], wkv[...], preferred_element_type=F32).astype(BF16)
    for g in range(KV_HEADS):
        kvown[g] = own[:, 2 * g * HEAD_DIM : 2 * (g + 1) * HEAD_DIM]
    kvbuf[0, t] = kvown[pair]
    kv_recv = take("recv", 2 * nX)
    for k in range(1, nX):
        xx = (x + k) % nX
        remote(kvown.at[xx * 2 // nR], kvbuf.at[0, t], kv_recv + k, tp_at(xx, c))
    remote(kvown.at[pair], kvbuf.at[0, t], kv_recv, sibling)
    kz_recv = take("recv", 2 * nA * nX)

    def keys_along(a_x, slot):
        for a in range(1, nA):
            remote(
                kvbuf.at[0, slot],
                kvbuf.at[a, slot],
                kz_recv + a * nX + a_x,
                {"sp": zl * nA + (zh + a) % nA},
            )

    keys_along(0, t)

    got_q[-1].wait()
    for xx in range(nX):
        for h in range(lh):
            cols = slice(h * trx, (h + 1) * trx)
            row = (shift[h : h + 1, xx * trx : (xx + 1) * trx] + log_rows) * LOG2E
            stat[0, xx, 0:1, cols] = row
    q_recv = take("recv", 2 * nB * nX)
    st_recv = take("recv", nB * nX)

    def project(k):
        xx = (x + nX - k) % nX
        q_rows = jnp.dot(flat_rows(nbuf[xx]), wq[...], preferred_element_type=F32).astype(BF16)
        for h in range(lh):
            cols = slice(h * HEAD_DIM, (h + 1) * HEAD_DIM)
            qob[0, xx, 0, h * trx : (h + 1) * trx, :] = q_rows[:, cols]
        for b in range(1, nB):
            where = {"sp": (zl + b) % nB * nA + zh}
            remote(qob.at[0, xx, 0], qob.at[b, xx, 0], q_recv + b * nX + k, where)
        o_rows = dot_nt(flat_rows(obuf[xx]), wo[...]).astype(BF16)
        keep = saved[pl.ds(pl.multiple_of(xx * trx, trx), trx), :].astype(F32)
        lane = lax.broadcasted_iota(jnp.int32, (trx, HEAD_DIM), 1)
        drops = jnp.zeros((trx, HEAD_DIM), F32)
        for h in range(lh):
            cols = slice(h * HEAD_DIM, (h + 1) * HEAD_DIM)
            rows = slice(h * trx, (h + 1) * trx)
            qob[0, xx, 1, rows, :] = o_rows[:, cols]
            term = jnp.sum(o_rows[:, cols].astype(F32) * keep[:, cols], axis=1, keepdims=True)
            drops = jnp.where(lane == h, term, drops)
        if trx < HEAD_DIM:
            drops = jnp.concatenate([drops, jnp.zeros((HEAD_DIM - trx, HEAD_DIM), F32)], axis=0)
        drops = drops.T
        for h in range(lh):
            stat[0, xx, 1:2, h * trx : (h + 1) * trx] = drops[h : h + 1, :trx]
        for b in range(1, nB):
            where = {"sp": (zl + b) % nB * nA + zh}
            remote(stat.at[0, xx], stat.at[b, xx], st_recv + b * nX + k, where)
            remote(qob.at[0, xx, 1], qob.at[b, xx, 1], q_recv + (nB + b) * nX + k, where)

    for copy in got_q[:-1]:
        copy.wait()
    for buf, base in bufs:
        arrive(buf.at[x, other], base, sibling)
    project(0)

    slots = [(b, a) for b in range(nB) for a in range(nA)]
    nz_recv = take("recv", nS * (1 + 2 * nX))

    def ahead(b, a):
        return (zl + b) % nB * nA + (zh + a) % nA

    def behind(b, a):
        return (zl + nB - b) % nB * nA + (zh + nA - a) % nA

    for n, (b, a) in enumerate(slots[1:], 1):
        to = ahead(b, a)
        cols = pl.ds(pl.multiple_of(to * ds_width, HEAD_DIM), ds_width)
        remote(nbuf.at[x, c, :, cols], nall.at[n, x, c], nz_recv + n, {"sp": to})

    for k in range(1, nX):
        xx = (x + nX - k) % nX
        for buf, base in bufs:
            arrive(buf.at[xx, c], base + k, tp_at(xx, c))
            remote(buf.at[xx, c], buf.at[xx, c], base + nX + k, sibling)
    for k in range(1, nX):
        xx = (x + nX - k) % nX
        for buf, base in bufs:
            arrive(buf.at[xx, other], base + nX + k, sibling)
        project(k)

    for k in range(1, nX):
        xx = (x + nX - k) % nX
        slot = xx * 2 + c
        arrive(kvbuf.at[0, slot], kv_recv + k, tp_at(xx, c))
        keys_along(k, slot)
        remote(kvbuf.at[0, slot], kvbuf.at[0, slot], kv_recv + nX + k, sibling)
    nall[0] = nbuf[:, :, :, pl.ds(pl.multiple_of(s * ds_width, HEAD_DIM), ds_width)]
    for k in range(1, nX):
        xx = (x + nX - k) % nX
        arrive(kvbuf.at[0, xx * 2 + other], kv_recv + nX + k, sibling)
    arrive(kvbuf.at[0, x * 2 + other], kv_recv, sibling)

    def attend(b, k, a):
        xx = (x + nX - k) % nX

        def step(i, carry):
            keys = kvbuf[a, i, :, :HEAD_DIM]
            values = kvbuf[a, i, :, HEAD_DIM:]
            queries = qob[b, xx, 0]
            backs = qob[b, xx, 1]
            score = dot_nt(keys, queries)
            prob = jnp.exp2(score * (factor * LOG2E) - stat[b, xx, 0:1, :])
            grad = (prob * (dot_nt(values, backs) - stat[b, xx, 1:2, :])).astype(BF16)
            key_part = jnp.dot(grad, queries, preferred_element_type=F32)
            value_part = jnp.dot(prob.astype(BF16), backs, preferred_element_type=F32)
            if b == 0 and k == 0:
                kacc[a, i, :, :HEAD_DIM] = key_part
                kacc[a, i, :, HEAD_DIM:] = value_part
            else:
                kacc[a, i, :, :HEAD_DIM] += key_part
                kacc[a, i, :, HEAD_DIM:] += value_part
            qacc[b, xx] += dot_tn(keys, grad)
            return carry

        lax.fori_loop(0, nT, step, 0, unroll=min(nT, 4))

    qs_recv = take("recv", nB * nB * nX)

    def send_queries(b, k):
        xx = (x + nX - k) % nX
        block = (qacc[b, xx] * factor).T
        qfull[b, xx] = block
        qsend[b, xx] = block.astype(BF16)
        for n in range(1, nB):
            slot = (n + b) % nB
            remote(
                qsend.at[b, xx],
                qrecv.at[n, slot, xx],
                qs_recv + (n * nB + slot) * nX + k,
                {"sp": (zl + n) % nB * nA + zh},
            )

    qacc[...] = jnp.zeros(qacc.shape, F32)
    for k in range(nX):
        attend(0, k, 0)

    for a in range(1, nA):
        for a_x in range(nX):
            slot = (x + nX - a_x) % nX * 2 + c
            idx = kz_recv + a * nX + a_x
            where = {"sp": zl * nA + (zh + nA - a) % nA}
            arrive(kvbuf.at[a, slot], idx, where)
            remote(kvbuf.at[a, slot], kvbuf.at[a, slot], idx + nA * nX, sibling)
        if a == 1:
            for n, (b, aa) in enumerate(slots[1:], 1):
                arrive(nall.at[n, x, c], nz_recv + n, {"sp": behind(b, aa)})
                base = nz_recv + nS + n * 2 * nX
                for j in range(1, nX):
                    remote(nall.at[n, x, c], nall.at[n, x, c], base + j, tp_at((x + j) % nX, c))
                remote(nall.at[n, x, c], nall.at[n, x, c], base, sibling)
        for a_x in range(nX):
            slot = (x + nX - a_x) % nX * 2 + other
            arrive(kvbuf.at[a, slot], kz_recv + a * nX + a_x + nA * nX, sibling)
        for k in range(nX):
            attend(0, k, a)
            if a == nA - 1:
                send_queries(0, k)

    kr_recv = take("recv", nA * nR)

    def send_keys(a):
        def convert(i, carry):
            kvs[a, i, :, :HEAD_DIM] = (kacc[a, i, :, :HEAD_DIM] * factor).astype(BF16)
            kvs[a, i, :, HEAD_DIM:] = kacc[a, i, :, HEAD_DIM:].astype(BF16)
            return carry

        lax.fori_loop(0, nT, convert, 0)
        for k in range(1, nR):
            to = (part + k) % nR
            remote(
                kvs.at[a, pl.ds(to * KV_HEADS, KV_HEADS)],
                kvr.at[k, a],
                kr_recv + a * nR + k,
                {"tp": pair * nR + to},
            )

    for k in range(nX):
        for b in range(1, nB):
            xx = (x + nX - k) % nX
            where = {"sp": (zl + nB - b) % nB * nA + zh}
            arrive(stat.at[b, xx], st_recv + b * nX + k, where)
            arrive(qob.at[b, xx, 0], q_recv + b * nX + k, where)
            arrive(qob.at[b, xx, 1], q_recv + (nB + b) * nX + k, where)
            last = k == nX - 1 and b == nB - 1
            for a in range(nA - 1, -1, -1):
                attend(b, k, a)
                if a == 0:
                    send_queries(b, k)
                if last:
                    send_keys(a)

    qg_recv = take("recv", nS)

    def finish_queries(b):
        for k in range(nX):
            xx = (x + nX - k) % nX
            total = qfull[b, xx]
            for n in range(1, nB):
                base = qs_recv + (n * nB + b) * nX + k
                arrive(qrecv.at[n, b, xx], base, {"sp": (zl + nB - n) % nB * nA + zh})
                total += qrecv[n, b, xx].astype(F32)
            total = total.astype(BF16)
            rows = pl.ds(pl.multiple_of(xx * trx, trx), trx)
            for h in range(lh):
                cols = slice(h * HEAD_DIM, (h + 1) * HEAD_DIM)
                qgall[b * nA, rows, cols] = total[h * trx : (h + 1) * trx, :]
        for a in range(1, nA):
            remote(
                qgall.at[b * nA],
                qgall.at[b * nA + a],
                qg_recv + b * nA + a,
                {"sp": zl * nA + (zh + a) % nA},
            )

    def portion(a, i):
        block = kacc[a, part * KV_HEADS + i]
        k_lane = lax.broadcasted_iota(jnp.int32, block.shape, 1) < HEAD_DIM
        block = jnp.where(k_lane, block * factor, block)
        for k in range(1, nR):
            block += kvr[k, a, i].astype(F32)
        return block

    ka_recv = take("recv", nA)
    for a in range(nA - 1, 0, -1):
        for k in range(1, nR):
            where = {"tp": pair * nR + (part + nR - k) % nR}
            arrive(kvr.at[k, a], kr_recv + a * nR + k, where)
        for i in range(KV_HEADS):
            kz[a, i] = portion(a, i).astype(BF16)
        remote(kz.at[a], kzr.at[a], ka_recv + a, {"sp": zl * nA + (zh + nA - a) % nA})

    for b in range(1, nB):
        finish_queries(b)

    for n, (b, a) in enumerate(slots[1:], 1):
        base = nz_recv + nS + n * 2 * nX
        for j in range(1, nX):
            xx = (x + nX - j) % nX
            arrive(nall.at[n, xx, c], base + j, tp_at(xx, c))
            remote(nall.at[n, xx, c], nall.at[n, xx, c], base + nX + j, sibling)

    finish_queries(0)

    step_cols = min(512, width)
    for i in range(width // step_cols):
        cols = slice(i * step_cols, (i + 1) * step_cols)
        share = dot_nt(qgall[0], wq[cols, :])
        ngf[:, :, :, cols] = share.reshape(nX, 2, nr, step_cols)
    for xx in range(nX):
        ngs[xx] = ngf[xx, other].astype(BF16)
    ng_recv = take("recv", nX)
    remote(ngs, ngr, ng_recv, sibling)

    for k in range(1, nR):
        arrive(kvr.at[k, 0], kr_recv + k, {"tp": pair * nR + (part + nR - k) % nR})
    for i in range(KV_HEADS):
        ksum[i] = portion(0, i)

    arrive(ngr, ng_recv, sibling)
    for k in range(1, nX):
        xx = (x + k) % nX
        ngx[k] = (ngf[xx, c] + ngr[xx].astype(F32)).astype(BF16)
        remote(ngx.at[k], ngin.at[k], ng_recv + k, tp_at(xx, c))

    for a in range(1, nA):
        arrive(kzr.at[a], ka_recv + a, {"sp": zl * nA + (zh + a) % nA})
    f_recv = take("recv", KV_HEADS)
    owner_sends = []
    for i in range(KV_HEADS):
        block = ksum[i]
        for a in range(1, nA):
            block += kzr[a, i].astype(F32)
        kfin[i] = block.astype(BF16)
        owner = part * KV_HEADS + i
        copy = remote(kfin.at[i], fin.at[pair], f_recv + pair, {"tp": owner}, keep=False)
        owner_sends.append((owner, copy))

        @pl.when(owner != t)
        def _():
            copy.start()

        @pl.when(owner == t)
        def _():
            fin[pair] = kfin[i]

    for n, (b, a) in enumerate(slots):
        if n:
            base = nz_recv + nS + n * 2 * nX
            arrive(nall.at[n, x, other], base, sibling)
            for j in range(1, nX):
                arrive(nall.at[n, (x + nX - j) % nX, other], base + nX + j, sibling)
    order = [b * nA for b in range(nB)] + [b * nA + a for b in list(range(1, nB)) + [0] for a in range(1, nA)]
    for n in order:
        if n % nA:
            arrive(qgall.at[n], qg_recv + n, {"sp": zl * nA + (zh + nA - n % nA) % nA})
        piece = dot_tn(flat_rows(nall[n]), qgall[n])
        if n == 0:
            query_weight_grad[...] = piece
        else:
            query_weight_grad[...] += piece

    grad = ngf[x, c] + ngr[x].astype(F32)
    for k in range(1, nX):
        arrive(ngin.at[k], ng_recv + k, tp_at((x + nX - k) % nX, c))
        grad += ngin[k].astype(F32)
    scaled = grad * gain[...]
    wide = tgt[...].astype(F32)
    root = jnp.sqrt(jnp.mean(wide * wide, axis=1, keepdims=True) + 1e-06)
    target_grad[...] = scaled / root - wide * jnp.mean(scaled * wide, axis=1, keepdims=True) / (
        root * root * root
    )

    for g in range(KV_HEADS):
        giver = g * nR + t // KV_HEADS

        @pl.when(giver != t)
        def _():
            arrive(fin.at[g], f_recv + g, {"tp": giver})

    for i in range(width // step_cols):
        rows = pl.ds(i * step_cols, step_cols)
        part_sum = dot_nt(fin[0], wkv[rows, 0 : 2 * HEAD_DIM])
        for g in range(1, KV_HEADS):
            part_sum += dot_nt(fin[g], wkv[rows, 2 * g * HEAD_DIM : 2 * (g + 1) * HEAD_DIM])
        source_grad[:, rows] = part_sum

    for copy in pending:
        copy.wait_send()
    for owner, copy in owner_sends:

        @pl.when(owner != t)
        def _():
            copy.wait_send()


def square_kernel(
    log_rows,
    target,
    source,
    norm_gain,
    query_weight,
    key_weight,
    value_weight,
    output_weight,
    saved_out,
    log_shift,
    out_grad,
    target_grad,
    source_grad,
    query_weight_grad,
    tgt,
    src,
    gain,
    wq,
    wkv,
    wo,
    saved,
    shift,
    nbuf,
    obuf,
    kvown,
    kvbuf,
    kvpeer,
    qob,
    stat,
    nall,
    kacc,
    qacc,
    qfull,
    qsend,
    qrecv,
    qgall,
    ngf,
    ngs,
    ngr,
    ngx,
    ngin,
    kvs,
    kvr,
    kz,
    kzr,
    kfin,
    fin,
    bulk,
    in_sem,
    send_sem,
    recv_sem,
):
    nr, width = tgt.shape
    lh = shift.shape[0]
    tr = saved.shape[0]
    nS, nT = 4, 4
    trx = tr // 2
    ds_width = width // nS
    factor = HEAD_DIM ** (-0.5)
    s = lax.axis_index("sp")
    t = lax.axis_index("tp")
    x, c = t // 2, t % 2
    ox, other = 1 - x, 1 - c
    peer = s + 1 - 2 * (s % 2)
    far = (s + 2) % nS
    diag = (peer + 2) % nS
    sib = {"tp": x * 2 + other}
    across = {"tp": ox * 2 + c}
    to_peer = {"sp": peer}
    to_far = {"sp": far}
    to_diag = {"sp": diag}

    keys = {("fin", 0): 0, ("fin", 1): 1}
    counts = {"in": 0}

    def sem(*key):
        return keys.setdefault(key, len(keys))

    def fetch(src_ref, dst_ref, at=None):
        if at is None:
            at = counts["in"]
            counts["in"] += 1
        copy = pltpu.make_async_copy(src_ref, dst_ref, in_sem.at[at])
        copy.start()
        return copy

    barrier = pltpu.get_barrier_semaphore()
    for k in range(1, nT):
        pl.semaphore_signal(
            barrier, 1, device_id={"tp": (t + k) % nT}, device_id_type=pl.DeviceIdType.MESH
        )
    for k in range(1, nS):
        pl.semaphore_signal(
            barrier, 1, device_id={"sp": (s + k) % nS}, device_id_type=pl.DeviceIdType.MESH
        )

    got_t = fetch(target, tgt)
    got_g = fetch(norm_gain, gain)
    got_shift = fetch(log_shift, shift)
    got_o = fetch(out_grad, obuf.at[x, c])
    got_kv = [fetch(source, src)]
    for g in range(KV_HEADS):
        cols = pl.ds(g * HEAD_DIM, HEAD_DIM)
        got_kv.append(fetch(key_weight.at[:, cols], wkv.at[:, pl.ds(2 * g * HEAD_DIM, HEAD_DIM)]))
        got_kv.append(
            fetch(value_weight.at[:, cols], wkv.at[:, pl.ds((2 * g + 1) * HEAD_DIM, HEAD_DIM)])
        )
    got_q = fetch(query_weight, wq)
    got_w = fetch(output_weight, wo)
    got_saved = fetch(saved_out, saved)

    got_t.wait()
    got_g.wait()
    wide = tgt[...].astype(F32)
    root = jnp.sqrt(jnp.mean(wide * wide, axis=1, keepdims=True) + 1e-06)
    nbuf[x, c] = (wide / root * gain[...]).astype(BF16)
    got_o.wait()
    pl.semaphore_wait(barrier, nT - 1 + nS - 1)

    pending, sent = [], []

    def remote(src_ref, dst_ref, key, where, keep=True):
        shared = keep and src_ref.dtype == BF16
        if shared:
            sent.append(math.prod(src_ref.shape) * 2)
        copy = pltpu.make_async_remote_copy(
            src_ref=src_ref,
            dst_ref=dst_ref,
            send_sem=send_sem.at[0 if shared else len(pending) + 1],
            recv_sem=recv_sem.at[sem(*key) if isinstance(key, tuple) else key],
            device_id=where,
            device_id_type=pl.DeviceIdType.MESH,
        )
        if keep:
            copy.start()
        if not shared:
            pending.append((copy, keep))
        return copy

    def arrive(dst_ref, key, where):
        pltpu.make_async_remote_copy(
            src_ref=dst_ref,
            dst_ref=dst_ref,
            send_sem=send_sem.at[0],
            recv_sem=recv_sem.at[sem(*key)],
            device_id=where,
            device_id_type=pl.DeviceIdType.MESH,
        ).wait_recv()

    def scope(name):
        return jax.named_scope(name)

    remote(nbuf.at[x, c], nbuf.at[x, c], ("n", "x"), across)
    remote(nbuf.at[x, c], nbuf.at[x, c], ("n", "s"), sib)
    remote(obuf.at[x, c], obuf.at[x, c], ("o", "s"), sib)
    remote(obuf.at[x, c], obuf.at[x, c], ("o", "x"), across)
    def slice_sends():
        for v, where, to in ((2, to_peer, peer), (1, to_far, far), (3, to_diag, diag)):
            cols = pl.ds(pl.multiple_of(to * ds_width, HEAD_DIM), ds_width)
            remote(nbuf.at[x, c, :, cols], nall.at[v, x, c], ("na", v), where)

    slice_sends()
    for copy in got_kv:
        copy.wait()
    with scope("kvproj"):
        own = jnp.dot(src[...], wkv[...], preferred_element_type=F32).astype(BF16)
        for g in range(KV_HEADS):
            kvown[g] = own[:, 2 * g * HEAD_DIM : 2 * (g + 1) * HEAD_DIM]
        kvbuf[0, t] = kvown[x]
    remote(kvown.at[x], kvbuf.at[0, t], ("kv", "s"), sib)
    remote(kvown.at[ox], kvbuf.at[0, t], ("kv", "x"), across)
    got_shift.wait()
    for k in range(2):
        xx = x if k == 0 else ox
        for h in range(lh):
            row = jnp.where(xx == 0, shift[h : h + 1, 0:trx], shift[h : h + 1, trx : 2 * trx])
            stat[0, k, 0:1, h * trx : (h + 1) * trx] = (row + log_rows) * LOG2E

    def send_far(ref, kind, k):
        remote(ref.at[0, k], ref.at[1, k], (kind, k), to_far)

    def send_part(i, kind, k):
        remote(qob.at[0, k, i], qob.at[1, k, i], (kind, k), to_far)

    def project_q(k):
        with scope(f"project_q{k}"):
            xx = x if k == 0 else ox
            rows = jnp.dot(flat_rows(nbuf[xx]), wq[...], preferred_element_type=F32).astype(BF16)
            for h in range(lh):
                cols = slice(h * HEAD_DIM, (h + 1) * HEAD_DIM)
                qob[0, k, 0, h * trx : (h + 1) * trx, :] = rows[:, cols]
        send_part(0, "q", k)

    def project_o(k):
        with scope(f"project_o{k}"):
            xx = x if k == 0 else ox
            o_rows = dot_nt(flat_rows(obuf[xx]), wo[...]).astype(BF16)
            for h in range(lh):
                cols = slice(h * HEAD_DIM, (h + 1) * HEAD_DIM)
                qob[0, k, 1, h * trx : (h + 1) * trx, :] = o_rows[:, cols]
        send_part(1, "ob", k)
        with scope(f"drop{k}"):
            keep = saved[pl.ds(pl.multiple_of(xx * trx, trx), trx), :].astype(F32)
            lane = lax.broadcasted_iota(jnp.int32, (trx, HEAD_DIM), 1)
            drops = jnp.zeros((trx, HEAD_DIM), F32)
            for h in range(lh):
                cols = slice(h * HEAD_DIM, (h + 1) * HEAD_DIM)
                term = jnp.sum(o_rows[:, cols].astype(F32) * keep[:, cols], axis=1, keepdims=True)
                drops = jnp.where(lane == h, term, drops)
            drops = jnp.concatenate([drops, jnp.zeros((HEAD_DIM - trx, HEAD_DIM), F32)], axis=0)
            drops = drops.T
            for h in range(lh):
                stat[0, k, 1:2, h * trx : (h + 1) * trx] = drops[h : h + 1, :trx]
        send_far(stat, "st", k)

    def need(k):
        with scope(f"w_q{k}"):
            arrive(qob.at[1, k, 0], ("q", k), to_far)
        with scope(f"w_ob{k}"):
            arrive(qob.at[1, k, 1], ("ob", k), to_far)
            arrive(stat.at[1, k], ("st", k), to_far)

    got = {"kacc": set(), "qacc": set()}

    def attend(v, k, a, g):
        with scope(f"attend_{v}{k}{a}{g}"):
            attend_rows(v, k, a, g, x if g == 0 else ox)

    def attend_last(a, mine):
        with scope(f"last_{a}{mine}"):
            attend_rows(1, 1, a, 2, c if mine else other)

    def attend_rows(v, k, a, g, chip):
        pair = pl.ds(2 * chip, 2)
        sr = kvbuf.shape[2]
        k_rows = kvbuf[a, pair, :, :HEAD_DIM].reshape(2 * sr, HEAD_DIM)
        v_rows = kvbuf[a, pair, :, HEAD_DIM:].reshape(2 * sr, HEAD_DIM)
        queries = qob[v, k, 0]
        backs = qob[v, k, 1]
        score = dot_nt(k_rows, queries)
        prob = jnp.exp2(score * (factor * LOG2E) - stat[v, k, 0:1, :])
        grad = (prob * (dot_nt(v_rows, backs) - stat[v, k, 1:2, :])).astype(BF16)
        key_part = jnp.dot(grad, queries, preferred_element_type=F32)
        value_part = jnp.dot(prob.astype(BF16), backs, preferred_element_type=F32)
        key_part = key_part.reshape(2, sr, HEAD_DIM)
        value_part = value_part.reshape(2, sr, HEAD_DIM)
        if g < 2 and (a, g) not in got["kacc"]:
            kacc[a, pair, :, :HEAD_DIM] = key_part
            kacc[a, pair, :, HEAD_DIM:] = value_part
        else:
            kacc[a, pair, :, :HEAD_DIM] += key_part
            kacc[a, pair, :, HEAD_DIM:] += value_part
        if (v, k) not in got["qacc"]:
            qacc[v, k] = dot_tn(k_rows, grad)
            got["qacc"].add((v, k))
        else:
            qacc[v, k] += dot_tn(k_rows, grad)
        got["kacc"].add((a, g))

    def query_part(v, k):
        return (qacc[v, k] * factor).T

    def send_keys(a):
        with scope(f"keys{a}"):
            for i in range(2):
                slot = 2 * other + i
                kvs[a, i, :, :HEAD_DIM] = (kacc[a, slot, :, :HEAD_DIM] * factor).astype(BF16)
                kvs[a, i, :, HEAD_DIM:] = kacc[a, slot, :, HEAD_DIM:].astype(BF16)
        remote(kvs.at[a], kvr.at[a], ("kp", a), sib)

    def key_sum(a, i):
        block = kacc[a, 2 * c + i]
        k_lane = lax.broadcasted_iota(jnp.int32, block.shape, 1) < HEAD_DIM
        return jnp.where(k_lane, block * factor, block) + kvr[a, i].astype(F32)

    def keys_back():
        with scope("w_kp1"):
            arrive(kvr.at[1], ("kp", 1), sib)
        with scope("kz"):
            for i in range(2):
                kz[i] = key_sum(1, i).astype(BF16)
        remote(kz, kzr, ("kz",), to_peer)

    def slice_from(v):
        return (None, to_far, to_peer, to_diag)[v]

    def slice_pass(v):
        with scope(f"w_na{v}"):
            arrive(nall.at[v, x, c], ("na", v), slice_from(v))
        remote(nall.at[v, x, c], nall.at[v, x, c], ("na", v, "x"), across)
        remote(nall.at[v, x, c], nall.at[v, x, c], ("na", v, "s"), sib)

    def slice_turn(v):
        with scope(f"w_nx{v}"):
            arrive(nall.at[v, ox, c], ("na", v, "x"), across)
        remote(nall.at[v, ox, c], nall.at[v, ox, c], ("na", v, "t"), sib)

    def slice_end(v):
        with scope(f"w_ns{v}"):
            arrive(nall.at[v, x, other], ("na", v, "s"), sib)
            arrive(nall.at[v, ox, other], ("na", v, "t"), sib)

    def total_rows(v, k):
        xx = x if k == 0 else ox
        return qgall.at[v, pl.ds(pl.multiple_of(xx * trx, trx), trx), :]

    pieces = []

    def weight_piece(v):
        with scope(f"piece{v}"):
            piece = dot_tn(flat_rows(nall[v]), qgall[v])
            if not pieces:
                query_weight_grad[...] = piece
            else:
                query_weight_grad[...] += piece
            pieces.append(v)

    step_cols = min(512, width)

    def normed_share():
        with scope("ng_share"):
            for i in range(width // step_cols):
                cols = slice(i * step_cols, (i + 1) * step_cols)
                share = dot_nt(qgall[0], wq[cols, :])
                ngf[:, :, :, cols] = share.reshape(2, 2, nr, step_cols)
            for xx in range(2):
                ngs[xx] = ngf[xx, other].astype(BF16)
        remote(ngs, ngr, ("ng", "s"), sib)

    def normed_cross():
        with scope("w_ngs"):
            arrive(ngr, ("ng", "s"), sib)
        ngx[...] = (ngf[ox, c] + ngr[ox].astype(F32)).astype(BF16)
        remote(ngx, ngin, ("ng", "x"), across)

    def normed_end():
        with scope("w_ngx"):
            arrive(ngin, ("ng", "x"), across)
        with scope("target"):
            grad = ngf[x, c] + ngr[x].astype(F32) + ngin[...].astype(F32)
            scaled = grad * gain[...]
            wide = tgt[...].astype(F32)
            root = jnp.sqrt(jnp.mean(wide * wide, axis=1, keepdims=True) + 1e-06)
            target_grad[...] = scaled / root - wide * jnp.mean(
                scaled * wide, axis=1, keepdims=True
            ) / (root * root * root)

    owner_sends = []

    def keys_out():
        with scope("w_kp0"):
            arrive(kvr.at[0], ("kp", 0), sib)
        with scope("w_kz"):
            arrive(kzr, ("kz",), to_peer)
        with scope("keys_out"):
            for i in range(2):
                block = key_sum(0, i) + kzr[i].astype(F32)
                kfin[i] = block.astype(BF16)
                owner = c * 2 + i
                copy = remote(kfin.at[i], fin.at[x], x, {"tp": owner}, keep=False)
                owner_sends.append((owner, copy))

                @pl.when(owner != t)
                def _():
                    copy.start()

                @pl.when(owner == t)
                def _():
                    fin[x] = kfin[i]

    def source_end():
        for g in range(KV_HEADS):
            giver = g * 2 + t // 2

            @pl.when(giver != t)
            def _():
                with scope("w_fin"):
                    arrive(fin.at[g], ("fin", g), {"tp": giver})

        with scope("source"):
            for i in range(width // step_cols):
                rows = pl.ds(i * step_cols, step_cols)
                part_sum = dot_nt(fin[0], wkv[rows, 0 : 2 * HEAD_DIM])
                for g in range(1, KV_HEADS):
                    part_sum += dot_nt(fin[g], wkv[rows, 2 * g * HEAD_DIM : 2 * (g + 1) * HEAD_DIM])
                source_grad[:, rows] = part_sum

    def pass_on(buf, kind):
        with scope(f"w_{kind}x"):
            arrive(buf.at[ox, c], (kind, "x"), across)
        remote(buf.at[ox, c], buf.at[ox, c], (kind, "t"), sib)

    def passed(buf, kind):
        with scope(f"w_{kind}t"):
            arrive(buf.at[ox, other], (kind, "t"), sib)

    def grad_out(b, k):
        with scope(f"dq_{b}{k}"):
            block = query_part(b, k)
            qfull[b, k] = block
            qsend[b, k] = block.astype(BF16)
        remote(qsend.at[b, k], qrecv.at[1 - b, k], ("dq", 1 - b, k), to_far)

    def total_out(b, k):
        with scope(f"w_dq{b}{k}"):
            arrive(qrecv.at[b, k], ("dq", b, k), to_far)
        with scope(f"total_{b}{k}"):
            total = (qfull[b, k] + qrecv[b, k].astype(F32)).astype(BF16)
            rows = pl.ds(pl.multiple_of((x if k == 0 else ox) * trx, trx), trx)
            for h in range(lh):
                cols = slice(h * HEAD_DIM, (h + 1) * HEAD_DIM)
                qgall[b, rows, cols] = total[h * trx : (h + 1) * trx, :]
        remote(total_rows(b, k), total_rows(2 + b, k), ("tot", b, k), to_peer)

    def total_in(b, k):
        with scope(f"w_tot{b}{k}"):
            arrive(total_rows(2 + b, k), ("tot", b, k), to_peer)

    def peer_keys(chip, kind):
        with scope(f"w_{kind}"):
            arrive(kvbuf.at[1, 2 * chip + c], (kind,), to_peer if chip is x else across)
        remote(kvbuf.at[1, 2 * chip + c], kvbuf.at[1, 2 * chip + c], (kind, "s"), sib)

    def peer_keys_end(chip, kind):
        with scope(f"w_{kind}s"):
            arrive(kvbuf.at[1, 2 * chip + other], (kind, "s"), sib)

    remote(kvown.at[ox], kvpeer, ("kp",), to_peer)
    with scope("w_ns"):
        arrive(nbuf.at[x, other], ("n", "s"), sib)
    got_q.wait()
    project_q(0)
    with scope("w_os"):
        arrive(obuf.at[x, other], ("o", "s"), sib)
    got_w.wait()
    got_saved.wait()
    project_o(0)
    remote(kvown.at[x], kvbuf.at[1, t], ("ke",), to_peer)
    with scope("w_kvs"):
        arrive(kvbuf.at[0, x * 2 + other], ("kv", "s"), sib)
    attend(0, 0, 0, 0)
    pass_on(nbuf, "n")
    passed(nbuf, "n")
    project_q(1)
    pass_on(obuf, "o")
    with scope("w_kpx"):
        arrive(kvpeer, ("kp",), to_peer)
    remote(kvpeer, kvbuf.at[1, t], ("kx",), across)
    passed(obuf, "o")
    project_o(1)
    with scope("w_kvx"):
        arrive(kvbuf.at[0, 2 * ox + c], ("kv", "x"), across)
    remote(kvbuf.at[0, 2 * ox + c], kvbuf.at[0, 2 * ox + c], ("kv", "t"), sib)
    attend(0, 1, 0, 0)
    need(0)
    attend(1, 0, 0, 0)
    with scope("w_kvt"):
        arrive(kvbuf.at[0, 2 * ox + other], ("kv", "t"), sib)
    attend(0, 0, 0, 1)
    attend(1, 0, 0, 1)
    peer_keys(ox, "kx")
    attend(0, 1, 0, 1)
    peer_keys(x, "ke")
    peer_keys_end(ox, "kx")
    attend(1, 0, 1, 1)
    peer_keys_end(x, "ke")
    attend(1, 0, 1, 0)
    grad_out(1, 0)
    attend(0, 0, 1, 0)
    attend(0, 0, 1, 1)
    grad_out(0, 0)
    attend(0, 1, 1, 0)
    attend(0, 1, 1, 1)
    need(1)
    attend_last(1, 0)
    send_keys(1)
    attend_last(1, 1)
    attend_last(0, 0)
    send_keys(0)
    attend_last(0, 1)
    grad_out(1, 1)
    keys_back()
    grad_out(0, 1)
    for v in (1, 2, 3):
        slice_pass(v)
    nall[0] = nbuf[:, :, :, pl.ds(pl.multiple_of(s * ds_width, HEAD_DIM), ds_width)]
    total_out(0, 0)
    total_out(1, 0)
    for v in (1, 2, 3):
        slice_turn(v)
    total_out(0, 1)
    normed_share()
    for v in (1, 2, 3):
        slice_end(v)
    weight_piece(0)
    normed_cross()
    total_out(1, 1)
    weight_piece(1)
    keys_out()
    total_in(0, 0)
    total_in(1, 0)
    total_in(0, 1)
    weight_piece(2)
    normed_end()
    source_end()
    total_in(1, 1)
    weight_piece(3)

    with scope("w_send"):
        whole = bulk.at[pl.ds(0, sum(sent) // (bulk.shape[1] * 4))]
        pltpu.make_async_copy(whole, whole, send_sem.at[0]).wait()
        for copy, kept in pending:
            if kept:
                copy.wait_send()
        for owner, copy in owner_sends:

            @pl.when(owner != t)
            def _():
                copy.wait_send()


def square_scratch(nr, width, sr, tr, lh, head_width):
    vm = pltpu.VMEM
    m = lh * tr // 2
    ds_width = width // 4
    kv = 2 * HEAD_DIM
    return [
        vm((nr, width), BF16),
        vm((sr, width), BF16),
        vm((1, width), F32),
        vm((width, head_width), BF16),
        vm((width, KV_HEADS * kv), BF16),
        vm((head_width, width), BF16),
        vm((tr, head_width), BF16),
        vm((lh, tr), F32),
        vm((2, 2, nr, width), BF16),
        vm((2, 2, nr, width), BF16),
        vm((KV_HEADS, sr, kv), BF16),
        vm((2, 4, sr, kv), BF16),
        vm((sr, kv), BF16),
        vm((2, 2, 2, m, HEAD_DIM), BF16),
        vm((2, 2, 2, m), F32),
        vm((4, 2, 2, nr, ds_width), BF16),
        vm((2, 4, sr, kv), F32),
        vm((2, 2, HEAD_DIM, m), F32),
        vm((2, 2, m, HEAD_DIM), F32),
        vm((2, 2, m, HEAD_DIM), BF16),
        vm((2, 2, m, HEAD_DIM), BF16),
        vm((4, tr, head_width), BF16),
        vm((2, 2, nr, width), F32),
        vm((2, nr, width), BF16),
        vm((2, nr, width), BF16),
        vm((nr, width), BF16),
        vm((nr, width), BF16),
        vm((2, 2, sr, kv), BF16),
        vm((2, 2, sr, kv), BF16),
        vm((2, sr, kv), BF16),
        vm((2, sr, kv), BF16),
        vm((2, sr, kv), BF16),
        vm((2, sr, kv), BF16),
        vm((8 * sr, width // 2), F32),
        pltpu.SemaphoreType.DMA((12,)),
        pltpu.SemaphoreType.DMA((6,)),
        pltpu.SemaphoreType.DMA((48,)),
    ]


def shards(
    target,
    source,
    norm_gain,
    query_weight,
    key_weight,
    value_weight,
    output_weight,
    saved_out,
    log_shift,
    out_grad,
):
    nT = lax.axis_size("tp")
    nS = lax.axis_size("sp")
    nA, nB = rows_split(nS)
    nX, nR = nT // 2, nT // KV_HEADS
    nr, width = target.shape
    sr = source.shape[0]
    tr, head_width = saved_out.shape
    lh = head_width // HEAD_DIM
    m = lh * tr // nX
    ds_width = width // nS
    kv = 2 * HEAD_DIM
    log_rows = math.log(sr * nT * nS)
    vm = pltpu.VMEM
    outputs = 4 * (nr * width + sr * width + ds_width * head_width)
    limit = 67043328 - outputs - 65536
    sems = min(8 * nS * nT, 1024)
    scratch = [
        vm((nr, width), BF16),
        vm((sr, width), BF16),
        vm((1, width), F32),
        vm((width, head_width), BF16),
        vm((width, KV_HEADS * kv), BF16),
        vm((head_width, width), BF16),
        vm((tr, head_width), BF16),
        vm((lh, tr), F32),
        vm((nX, 2, nr, width), BF16),
        vm((nX, 2, nr, width), BF16),
        vm((KV_HEADS, sr, kv), BF16),
        vm((nA, nT, sr, kv), BF16),
        vm((nB, nX, 2, m, HEAD_DIM), BF16),
        vm((nB, nX, 2, m), F32),
        vm((nS, nX, 2, nr, ds_width), BF16),
        vm((nA, nT, sr, kv), F32),
        vm((nB, nX, HEAD_DIM, m), F32),
        vm((nB, nX, m, HEAD_DIM), F32),
        vm((nB, nX, m, HEAD_DIM), BF16),
        vm((nB, nB, nX, m, HEAD_DIM), BF16),
        vm((nS, tr, head_width), BF16),
        vm((nX, 2, nr, width), F32),
        vm((nX, nr, width), BF16),
        vm((nX, nr, width), BF16),
        vm((nX, nr, width), BF16),
        vm((nX, nr, width), BF16),
        vm((nA, nT, sr, kv), BF16),
        vm((nR, nA, KV_HEADS, sr, kv), BF16),
        vm((nA, KV_HEADS, sr, kv), BF16),
        vm((nA, KV_HEADS, sr, kv), BF16),
        vm((KV_HEADS, sr, kv), BF16),
        vm((KV_HEADS, sr, kv), BF16),
        vm((KV_HEADS, sr, kv), F32),
        pltpu.SemaphoreType.DMA((16,)),
        pltpu.SemaphoreType.DMA((sems,)),
        pltpu.SemaphoreType.DMA((sems,)),
    ]
    body = functools.partial(kernel, nS, nT, log_rows)
    if nS == 4 and nT == 4:
        body = functools.partial(square_kernel, log_rows)
        scratch = square_scratch(nr, width, sr, tr, lh, head_width)
    anywhere = pl.BlockSpec(memory_space=pltpu.HBM)
    return pl.pallas_call(
        body,
        out_shape=(
            pltpu.VMEM((nr, width), F32),
            pltpu.VMEM((sr, width), F32),
            pltpu.VMEM((ds_width, head_width), F32),
        ),
        in_specs=[anywhere] * 10,
        out_specs=(pl.BlockSpec(memory_space=pltpu.VMEM),) * 3,
        scratch_shapes=scratch,
        compiler_params=pltpu.CompilerParams(
            collective_id=0, has_side_effects=True, vmem_limit_bytes=limit
        ),
        name="cross_back",
    )(
        target,
        source,
        norm_gain.reshape(1, width),
        query_weight,
        key_weight,
        value_weight,
        output_weight,
        saved_out,
        log_shift,
        out_grad,
    )


def solution(mesh):
    return jax.shard_map(
        shards,
        mesh=mesh,
        in_specs=(
            P(("grp", "sp", "tp"), None),
            P(("grp", "sp", "tp"), None),
            P(),
            P(None, "tp"),
            P(),
            P(),
            P("tp", None),
            P(("grp", "sp"), "tp"),
            P("tp", ("grp", "sp")),
            P(("grp", "sp", "tp"), None),
        ),
        out_specs=(
            P(("grp", "sp", "tp"), None),
            P(("grp", "sp", "tp"), None),
            P(("grp", "sp"), "tp"),
        ),
        check_vma=False,
    )
```

```python
import functools
import math

import jax
import jax.numpy as jnp
from jax import lax
from jax.experimental import pallas as pl
from jax.experimental.pallas import tpu as pltpu
from jax.sharding import PartitionSpec as P

HEADS = 16
HEAD_DIM = 128
KV_HEADS = 2
LOG2E = 1.4426950408889634
BF16 = jnp.bfloat16
F32 = jnp.float32


def rows_split(sp_count):
    keys = 2 if sp_count % 2 == 0 else 1
    while keys * keys * 4 <= sp_count:
        keys *= 2
    return keys, sp_count // keys


def dot_nt(a, b):
    return lax.dot_general(a, b, (((1,), (1,)), ((), ())), preferred_element_type=F32)


def dot_tn(a, b):
    return lax.dot_general(a, b, (((0,), (0,)), ((), ())), preferred_element_type=F32)


def flat_rows(block):
    count = block.shape[-2]
    shape = (-1, block.shape[-1])
    if count % 16:
        return block.astype(F32).reshape(shape).astype(BF16)
    return block.reshape(shape)


def kernel(
    sp_count,
    tp_count,
    log_rows,
    target,
    source,
    norm_gain,
    query_weight,
    key_weight,
    value_weight,
    output_weight,
    saved_out,
    log_shift,
    out_grad,
    target_grad,
    source_grad,
    query_weight_grad,
    tgt,
    src,
    gain,
    wq,
    wkv,
    wo,
    saved,
    shift,
    nbuf,
    obuf,
    kvown,
    kvbuf,
    qob,
    stat,
    nall,
    kacc,
    qacc,
    qfull,
    qsend,
    qrecv,
    qgall,
    ngf,
    ngs,
    ngr,
    ngx,
    ngin,
    kvs,
    kvr,
    kz,
    kzr,
    kfin,
    fin,
    ksum,
    in_sem,
    send_sem,
    recv_sem,
):
    nA, nB, nS, nT = kvbuf.shape[0], qob.shape[0], sp_count, tp_count
    nX = nT // 2
    nR = nT // KV_HEADS
    nr, width = tgt.shape
    sr = src.shape[0]
    lh = shift.shape[0]
    tr = saved.shape[0]
    trx = tr // nX
    ds_width = width // nS
    factor = HEAD_DIM ** (-0.5)
    s = lax.axis_index("sp")
    t = lax.axis_index("tp")
    x, c = t // 2, t % 2
    other = 1 - c
    part, pair = t % nR, t // nR
    zh, zl = s % nA, s // nA

    pending = []
    counts = {"send": 0, "recv": 0, "in": 0}

    def take(kind, n=1):
        first = counts[kind]
        counts[kind] += n
        return first

    def remote(src_ref, dst_ref, recv, where, keep=True):
        copy = pltpu.make_async_remote_copy(
            src_ref=src_ref,
            dst_ref=dst_ref,
            send_sem=send_sem.at[take("send")],
            recv_sem=recv_sem.at[recv],
            device_id=where,
            device_id_type=pl.DeviceIdType.MESH,
        )
        if keep:
            copy.start()
            pending.append(copy)
        return copy

    def arrive(dst_ref, recv, where):
        pltpu.make_async_remote_copy(
            src_ref=dst_ref,
            dst_ref=dst_ref,
            send_sem=send_sem.at[0],
            recv_sem=recv_sem.at[recv],
            device_id=where,
            device_id_type=pl.DeviceIdType.MESH,
        ).wait_recv()

    def fetch(src_ref, dst_ref):
        copy = pltpu.make_async_copy(src_ref, dst_ref, in_sem.at[take("in")])
        copy.start()
        return copy

    def tp_at(xx, cc):
        return {"tp": xx * 2 + cc}

    sibling = tp_at(x, other)

    got_t = fetch(target, tgt)
    got_g = fetch(norm_gain, gain)
    got_o = fetch(out_grad, obuf.at[x, c])
    got_kv = [fetch(source, src)]
    for g in range(KV_HEADS):
        cols = pl.ds(g * HEAD_DIM, HEAD_DIM)
        got_kv.append(fetch(key_weight.at[:, cols], wkv.at[:, pl.ds(2 * g * HEAD_DIM, HEAD_DIM)]))
        got_kv.append(
            fetch(value_weight.at[:, cols], wkv.at[:, pl.ds((2 * g + 1) * HEAD_DIM, HEAD_DIM)])
        )
    got_q = [
        fetch(query_weight, wq),
        fetch(output_weight, wo),
        fetch(saved_out, saved),
        fetch(log_shift, shift),
    ]

    barrier = pltpu.get_barrier_semaphore()
    for k in range(1, nT):
        pl.semaphore_signal(
            barrier, 1, device_id={"tp": (t + k) % nT}, device_id_type=pl.DeviceIdType.MESH
        )
    for k in range(1, nS):
        pl.semaphore_signal(
            barrier, 1, device_id={"sp": (s + k) % nS}, device_id_type=pl.DeviceIdType.MESH
        )

    got_t.wait()
    got_g.wait()
    wide = tgt[...].astype(F32)
    root = jnp.sqrt(jnp.mean(wide * wide, axis=1, keepdims=True) + 1e-06)
    nbuf[x, c] = (wide / root * gain[...]).astype(BF16)
    got_o.wait()
    pl.semaphore_wait(barrier, nT - 1 + nS - 1)

    n_recv = take("recv", 2 * nX)
    o_recv = take("recv", 2 * nX)
    bufs = ((nbuf, n_recv), (obuf, o_recv))
    for k in range(1, nX):
        for buf, base in bufs:
            remote(buf.at[x, c], buf.at[x, c], base + k, tp_at((x + k) % nX, c))
    for buf, base in bufs:
        remote(buf.at[x, c], buf.at[x, c], base, sibling)

    for copy in got_kv:
        copy.wait()
    own = jnp.dot(src[...], wkv[...], preferred_element_type=F32).astype(BF16)
    for g in range(KV_HEADS):
        kvown[g] = own[:, 2 * g * HEAD_DIM : 2 * (g + 1) * HEAD_DIM]
    kvbuf[0, t] = kvown[pair]
    kv_recv = take("recv", 2 * nX)
    for k in range(1, nX):
        xx = (x + k) % nX
        remote(kvown.at[xx * 2 // nR], kvbuf.at[0, t], kv_recv + k, tp_at(xx, c))
    remote(kvown.at[pair], kvbuf.at[0, t], kv_recv, sibling)
    kz_recv = take("recv", 2 * nA * nX)

    def keys_along(a_x, slot):
        for a in range(1, nA):
            remote(
                kvbuf.at[0, slot],
                kvbuf.at[a, slot],
                kz_recv + a * nX + a_x,
                {"sp": zl * nA + (zh + a) % nA},
            )

    keys_along(0, t)

    got_q[-1].wait()
    for xx in range(nX):
        for h in range(lh):
            cols = slice(h * trx, (h + 1) * trx)
            row = (shift[h : h + 1, xx * trx : (xx + 1) * trx] + log_rows) * LOG2E
            stat[0, xx, 0:1, cols] = row
    q_recv = take("recv", 2 * nB * nX)
    st_recv = take("recv", nB * nX)

    def project(k):
        xx = (x + nX - k) % nX
        q_rows = jnp.dot(flat_rows(nbuf[xx]), wq[...], preferred_element_type=F32).astype(BF16)
        for h in range(lh):
            cols = slice(h * HEAD_DIM, (h + 1) * HEAD_DIM)
            qob[0, xx, 0, h * trx : (h + 1) * trx, :] = q_rows[:, cols]
        for b in range(1, nB):
            where = {"sp": (zl + b) % nB * nA + zh}
            remote(qob.at[0, xx, 0], qob.at[b, xx, 0], q_recv + b * nX + k, where)
        o_rows = dot_nt(flat_rows(obuf[xx]), wo[...]).astype(BF16)
        keep = saved[pl.ds(pl.multiple_of(xx * trx, trx), trx), :].astype(F32)
        lane = lax.broadcasted_iota(jnp.int32, (trx, HEAD_DIM), 1)
        drops = jnp.zeros((trx, HEAD_DIM), F32)
        for h in range(lh):
            cols = slice(h * HEAD_DIM, (h + 1) * HEAD_DIM)
            rows = slice(h * trx, (h + 1) * trx)
            qob[0, xx, 1, rows, :] = o_rows[:, cols]
            term = jnp.sum(o_rows[:, cols].astype(F32) * keep[:, cols], axis=1, keepdims=True)
            drops = jnp.where(lane == h, term, drops)
        if trx < HEAD_DIM:
            drops = jnp.concatenate([drops, jnp.zeros((HEAD_DIM - trx, HEAD_DIM), F32)], axis=0)
        drops = drops.T
        for h in range(lh):
            stat[0, xx, 1:2, h * trx : (h + 1) * trx] = drops[h : h + 1, :trx]
        for b in range(1, nB):
            where = {"sp": (zl + b) % nB * nA + zh}
            remote(stat.at[0, xx], stat.at[b, xx], st_recv + b * nX + k, where)
            remote(qob.at[0, xx, 1], qob.at[b, xx, 1], q_recv + (nB + b) * nX + k, where)

    for copy in got_q[:-1]:
        copy.wait()
    for buf, base in bufs:
        arrive(buf.at[x, other], base, sibling)
    project(0)

    slots = [(b, a) for b in range(nB) for a in range(nA)]
    nz_recv = take("recv", nS * (1 + 2 * nX))

    def ahead(b, a):
        return (zl + b) % nB * nA + (zh + a) % nA

    def behind(b, a):
        return (zl + nB - b) % nB * nA + (zh + nA - a) % nA

    for n, (b, a) in enumerate(slots[1:], 1):
        to = ahead(b, a)
        cols = pl.ds(pl.multiple_of(to * ds_width, HEAD_DIM), ds_width)
        remote(nbuf.at[x, c, :, cols], nall.at[n, x, c], nz_recv + n, {"sp": to})

    for k in range(1, nX):
        xx = (x + nX - k) % nX
        for buf, base in bufs:
            arrive(buf.at[xx, c], base + k, tp_at(xx, c))
            remote(buf.at[xx, c], buf.at[xx, c], base + nX + k, sibling)
    for k in range(1, nX):
        xx = (x + nX - k) % nX
        for buf, base in bufs:
            arrive(buf.at[xx, other], base + nX + k, sibling)
        project(k)

    for k in range(1, nX):
        xx = (x + nX - k) % nX
        slot = xx * 2 + c
        arrive(kvbuf.at[0, slot], kv_recv + k, tp_at(xx, c))
        keys_along(k, slot)
        remote(kvbuf.at[0, slot], kvbuf.at[0, slot], kv_recv + nX + k, sibling)
    nall[0] = nbuf[:, :, :, pl.ds(pl.multiple_of(s * ds_width, HEAD_DIM), ds_width)]
    for k in range(1, nX):
        xx = (x + nX - k) % nX
        arrive(kvbuf.at[0, xx * 2 + other], kv_recv + nX + k, sibling)
    arrive(kvbuf.at[0, x * 2 + other], kv_recv, sibling)

    def attend(b, k, a):
        xx = (x + nX - k) % nX

        def step(i, carry):
            keys = kvbuf[a, i, :, :HEAD_DIM]
            values = kvbuf[a, i, :, HEAD_DIM:]
            queries = qob[b, xx, 0]
            backs = qob[b, xx, 1]
            score = dot_nt(keys, queries)
            prob = jnp.exp2(score * (factor * LOG2E) - stat[b, xx, 0:1, :])
            grad = (prob * (dot_nt(values, backs) - stat[b, xx, 1:2, :])).astype(BF16)
            key_part = jnp.dot(grad, queries, preferred_element_type=F32)
            value_part = jnp.dot(prob.astype(BF16), backs, preferred_element_type=F32)
            if b == 0 and k == 0:
                kacc[a, i, :, :HEAD_DIM] = key_part
                kacc[a, i, :, HEAD_DIM:] = value_part
            else:
                kacc[a, i, :, :HEAD_DIM] += key_part
                kacc[a, i, :, HEAD_DIM:] += value_part
            qacc[b, xx] += dot_tn(keys, grad)
            return carry

        lax.fori_loop(0, nT, step, 0, unroll=min(nT, 4))

    qs_recv = take("recv", nB * nB * nX)

    def send_queries(b, k):
        xx = (x + nX - k) % nX
        block = (qacc[b, xx] * factor).T
        qfull[b, xx] = block
        qsend[b, xx] = block.astype(BF16)
        for n in range(1, nB):
            slot = (n + b) % nB
            remote(
                qsend.at[b, xx],
                qrecv.at[n, slot, xx],
                qs_recv + (n * nB + slot) * nX + k,
                {"sp": (zl + n) % nB * nA + zh},
            )

    qacc[...] = jnp.zeros(qacc.shape, F32)
    for k in range(nX):
        attend(0, k, 0)

    for a in range(1, nA):
        for a_x in range(nX):
            slot = (x + nX - a_x) % nX * 2 + c
            idx = kz_recv + a * nX + a_x
            where = {"sp": zl * nA + (zh + nA - a) % nA}
            arrive(kvbuf.at[a, slot], idx, where)
            remote(kvbuf.at[a, slot], kvbuf.at[a, slot], idx + nA * nX, sibling)
        if a == 1:
            for n, (b, aa) in enumerate(slots[1:], 1):
                arrive(nall.at[n, x, c], nz_recv + n, {"sp": behind(b, aa)})
                base = nz_recv + nS + n * 2 * nX
                for j in range(1, nX):
                    remote(nall.at[n, x, c], nall.at[n, x, c], base + j, tp_at((x + j) % nX, c))
                remote(nall.at[n, x, c], nall.at[n, x, c], base, sibling)
        for a_x in range(nX):
            slot = (x + nX - a_x) % nX * 2 + other
            arrive(kvbuf.at[a, slot], kz_recv + a * nX + a_x + nA * nX, sibling)
        for k in range(nX):
            attend(0, k, a)
            if a == nA - 1:
                send_queries(0, k)

    kr_recv = take("recv", nA * nR)

    def send_keys(a):
        def convert(i, carry):
            kvs[a, i, :, :HEAD_DIM] = (kacc[a, i, :, :HEAD_DIM] * factor).astype(BF16)
            kvs[a, i, :, HEAD_DIM:] = kacc[a, i, :, HEAD_DIM:].astype(BF16)
            return carry

        lax.fori_loop(0, nT, convert, 0)
        for k in range(1, nR):
            to = (part + k) % nR
            remote(
                kvs.at[a, pl.ds(to * KV_HEADS, KV_HEADS)],
                kvr.at[k, a],
                kr_recv + a * nR + k,
                {"tp": pair * nR + to},
            )

    for k in range(nX):
        for b in range(1, nB):
            xx = (x + nX - k) % nX
            where = {"sp": (zl + nB - b) % nB * nA + zh}
            arrive(stat.at[b, xx], st_recv + b * nX + k, where)
            arrive(qob.at[b, xx, 0], q_recv + b * nX + k, where)
            arrive(qob.at[b, xx, 1], q_recv + (nB + b) * nX + k, where)
            last = k == nX - 1 and b == nB - 1
            for a in range(nA - 1, -1, -1):
                attend(b, k, a)
                if a == 0:
                    send_queries(b, k)
                if last:
                    send_keys(a)

    qg_recv = take("recv", nS)

    def finish_queries(b):
        for k in range(nX):
            xx = (x + nX - k) % nX
            total = qfull[b, xx]
            for n in range(1, nB):
                base = qs_recv + (n * nB + b) * nX + k
                arrive(qrecv.at[n, b, xx], base, {"sp": (zl + nB - n) % nB * nA + zh})
                total += qrecv[n, b, xx].astype(F32)
            total = total.astype(BF16)
            rows = pl.ds(pl.multiple_of(xx * trx, trx), trx)
            for h in range(lh):
                cols = slice(h * HEAD_DIM, (h + 1) * HEAD_DIM)
                qgall[b * nA, rows, cols] = total[h * trx : (h + 1) * trx, :]
        for a in range(1, nA):
            remote(
                qgall.at[b * nA],
                qgall.at[b * nA + a],
                qg_recv + b * nA + a,
                {"sp": zl * nA + (zh + a) % nA},
            )

    def portion(a, i):
        block = kacc[a, part * KV_HEADS + i]
        k_lane = lax.broadcasted_iota(jnp.int32, block.shape, 1) < HEAD_DIM
        block = jnp.where(k_lane, block * factor, block)
        for k in range(1, nR):
            block += kvr[k, a, i].astype(F32)
        return block

    ka_recv = take("recv", nA)
    for a in range(nA - 1, 0, -1):
        for k in range(1, nR):
            where = {"tp": pair * nR + (part + nR - k) % nR}
            arrive(kvr.at[k, a], kr_recv + a * nR + k, where)
        for i in range(KV_HEADS):
            kz[a, i] = portion(a, i).astype(BF16)
        remote(kz.at[a], kzr.at[a], ka_recv + a, {"sp": zl * nA + (zh + nA - a) % nA})

    for b in range(1, nB):
        finish_queries(b)

    for n, (b, a) in enumerate(slots[1:], 1):
        base = nz_recv + nS + n * 2 * nX
        for j in range(1, nX):
            xx = (x + nX - j) % nX
            arrive(nall.at[n, xx, c], base + j, tp_at(xx, c))
            remote(nall.at[n, xx, c], nall.at[n, xx, c], base + nX + j, sibling)

    finish_queries(0)

    step_cols = min(512, width)
    for i in range(width // step_cols):
        cols = slice(i * step_cols, (i + 1) * step_cols)
        share = dot_nt(qgall[0], wq[cols, :])
        ngf[:, :, :, cols] = share.reshape(nX, 2, nr, step_cols)
    for xx in range(nX):
        ngs[xx] = ngf[xx, other].astype(BF16)
    ng_recv = take("recv", nX)
    remote(ngs, ngr, ng_recv, sibling)

    for k in range(1, nR):
        arrive(kvr.at[k, 0], kr_recv + k, {"tp": pair * nR + (part + nR - k) % nR})
    for i in range(KV_HEADS):
        ksum[i] = portion(0, i)

    arrive(ngr, ng_recv, sibling)
    for k in range(1, nX):
        xx = (x + k) % nX
        ngx[k] = (ngf[xx, c] + ngr[xx].astype(F32)).astype(BF16)
        remote(ngx.at[k], ngin.at[k], ng_recv + k, tp_at(xx, c))

    for a in range(1, nA):
        arrive(kzr.at[a], ka_recv + a, {"sp": zl * nA + (zh + a) % nA})
    f_recv = take("recv", KV_HEADS)
    owner_sends = []
    for i in range(KV_HEADS):
        block = ksum[i]
        for a in range(1, nA):
            block += kzr[a, i].astype(F32)
        kfin[i] = block.astype(BF16)
        owner = part * KV_HEADS + i
        copy = remote(kfin.at[i], fin.at[pair], f_recv + pair, {"tp": owner}, keep=False)
        owner_sends.append((owner, copy))

        @pl.when(owner != t)
        def _():
            copy.start()

        @pl.when(owner == t)
        def _():
            fin[pair] = kfin[i]

    for n, (b, a) in enumerate(slots):
        if n:
            base = nz_recv + nS + n * 2 * nX
            arrive(nall.at[n, x, other], base, sibling)
            for j in range(1, nX):
                arrive(nall.at[n, (x + nX - j) % nX, other], base + nX + j, sibling)
    order = [b * nA for b in range(nB)] + [b * nA + a for b in list(range(1, nB)) + [0] for a in range(1, nA)]
    for n in order:
        if n % nA:
            arrive(qgall.at[n], qg_recv + n, {"sp": zl * nA + (zh + nA - n % nA) % nA})
        piece = dot_tn(flat_rows(nall[n]), qgall[n])
        if n == 0:
            query_weight_grad[...] = piece
        else:
            query_weight_grad[...] += piece

    grad = ngf[x, c] + ngr[x].astype(F32)
    for k in range(1, nX):
        arrive(ngin.at[k], ng_recv + k, tp_at((x + nX - k) % nX, c))
        grad += ngin[k].astype(F32)
    scaled = grad * gain[...]
    wide = tgt[...].astype(F32)
    root = jnp.sqrt(jnp.mean(wide * wide, axis=1, keepdims=True) + 1e-06)
    target_grad[...] = scaled / root - wide * jnp.mean(scaled * wide, axis=1, keepdims=True) / (
        root * root * root
    )

    for g in range(KV_HEADS):
        giver = g * nR + t // KV_HEADS

        @pl.when(giver != t)
        def _():
            arrive(fin.at[g], f_recv + g, {"tp": giver})

    for i in range(width // step_cols):
        rows = pl.ds(i * step_cols, step_cols)
        part_sum = dot_nt(fin[0], wkv[rows, 0 : 2 * HEAD_DIM])
        for g in range(1, KV_HEADS):
            part_sum += dot_nt(fin[g], wkv[rows, 2 * g * HEAD_DIM : 2 * (g + 1) * HEAD_DIM])
        source_grad[:, rows] = part_sum

    for copy in pending:
        copy.wait_send()
    for owner, copy in owner_sends:

        @pl.when(owner != t)
        def _():
            copy.wait_send()


def square_kernel(
    log_rows,
    target,
    source,
    norm_gain,
    query_weight,
    key_weight,
    value_weight,
    output_weight,
    saved_out,
    log_shift,
    out_grad,
    target_grad,
    source_grad,
    query_weight_grad,
    tgt,
    src,
    gain,
    wq,
    wkv,
    wo,
    saved,
    shift,
    nbuf,
    obuf,
    kvown,
    kvbuf,
    kvpeer,
    qob,
    stat,
    nall,
    kacc,
    qacc,
    qfull,
    qsend,
    qrecv,
    qgall,
    ngf,
    ngs,
    ngr,
    ngx,
    ngin,
    kvs,
    kvr,
    kz,
    kzr,
    kfin,
    fin,
    bulk,
    in_sem,
    send_sem,
    recv_sem,
):
    nr, width = tgt.shape
    lh = shift.shape[0]
    tr = saved.shape[0]
    nS, nT = 4, 4
    trx = tr // 2
    ds_width = width // nS
    factor = HEAD_DIM ** (-0.5)
    s = lax.axis_index("sp")
    t = lax.axis_index("tp")
    x, c = t // 2, t % 2
    ox, other = 1 - x, 1 - c
    peer = s + 1 - 2 * (s % 2)
    far = (s + 2) % nS
    diag = (peer + 2) % nS
    sib = {"tp": x * 2 + other}
    across = {"tp": ox * 2 + c}
    to_peer = {"sp": peer}
    to_far = {"sp": far}
    to_diag = {"sp": diag}

    keys = {("fin", 0): 0, ("fin", 1): 1}
    counts = {"in": 0}

    def sem(*key):
        return keys.setdefault(key, len(keys))

    def fetch(src_ref, dst_ref, at=None):
        if at is None:
            at = counts["in"]
            counts["in"] += 1
        copy = pltpu.make_async_copy(src_ref, dst_ref, in_sem.at[at])
        copy.start()
        return copy

    barrier = pltpu.get_barrier_semaphore()
    for k in range(1, nT):
        pl.semaphore_signal(
            barrier, 1, device_id={"tp": (t + k) % nT}, device_id_type=pl.DeviceIdType.MESH
        )
    for k in range(1, nS):
        pl.semaphore_signal(
            barrier, 1, device_id={"sp": (s + k) % nS}, device_id_type=pl.DeviceIdType.MESH
        )

    got_t = fetch(target, tgt)
    got_g = fetch(norm_gain, gain)
    got_shift = fetch(log_shift, shift)
    got_o = fetch(out_grad, obuf.at[x, c])
    got_kv = [fetch(source, src)]
    for g in range(KV_HEADS):
        cols = pl.ds(g * HEAD_DIM, HEAD_DIM)
        got_kv.append(fetch(key_weight.at[:, cols], wkv.at[:, pl.ds(2 * g * HEAD_DIM, HEAD_DIM)]))
        got_kv.append(
            fetch(value_weight.at[:, cols], wkv.at[:, pl.ds((2 * g + 1) * HEAD_DIM, HEAD_DIM)])
        )
    got_q = fetch(query_weight, wq)
    got_w = fetch(output_weight, wo)
    got_saved = fetch(saved_out, saved)

    got_t.wait()
    got_g.wait()
    wide = tgt[...].astype(F32)
    root = jnp.sqrt(jnp.mean(wide * wide, axis=1, keepdims=True) + 1e-06)
    nbuf[x, c] = (wide / root * gain[...]).astype(BF16)
    got_o.wait()
    pl.semaphore_wait(barrier, nT - 1 + nS - 1)

    pending, sent = [], []

    def remote(src_ref, dst_ref, key, where, keep=True):
        shared = keep and src_ref.dtype == BF16
        if shared:
            sent.append(math.prod(src_ref.shape) * 2)
        copy = pltpu.make_async_remote_copy(
            src_ref=src_ref,
            dst_ref=dst_ref,
            send_sem=send_sem.at[0 if shared else len(pending) + 1],
            recv_sem=recv_sem.at[sem(*key) if isinstance(key, tuple) else key],
            device_id=where,
            device_id_type=pl.DeviceIdType.MESH,
        )
        if keep:
            copy.start()
        if not shared:
            pending.append((copy, keep))
        return copy

    def arrive(dst_ref, key, where):
        pltpu.make_async_remote_copy(
            src_ref=dst_ref,
            dst_ref=dst_ref,
            send_sem=send_sem.at[0],
            recv_sem=recv_sem.at[sem(*key)],
            device_id=where,
            device_id_type=pl.DeviceIdType.MESH,
        ).wait_recv()

    def scope(name):
        return jax.named_scope(name)

    remote(nbuf.at[x, c], nbuf.at[x, c], ("n", "x"), across)
    remote(nbuf.at[x, c], nbuf.at[x, c], ("n", "s"), sib)
    remote(obuf.at[x, c], obuf.at[x, c], ("o", "s"), sib)
    remote(obuf.at[x, c], obuf.at[x, c], ("o", "x"), across)
    def slice_sends():
        for v, where, to in ((2, to_peer, peer), (1, to_far, far), (3, to_diag, diag)):
            cols = pl.ds(pl.multiple_of(to * ds_width, HEAD_DIM), ds_width)
            remote(nbuf.at[x, c, :, cols], nall.at[v, x, c], ("na", v), where)

    slice_sends()
    for copy in got_kv:
        copy.wait()
    with scope("kvproj"):
        own = jnp.dot(src[...], wkv[...], preferred_element_type=F32).astype(BF16)
        for g in range(KV_HEADS):
            kvown[g] = own[:, 2 * g * HEAD_DIM : 2 * (g + 1) * HEAD_DIM]
        kvbuf[0, t] = kvown[x]
    remote(kvown.at[x], kvbuf.at[0, t], ("kv", "s"), sib)
    remote(kvown.at[ox], kvbuf.at[0, t], ("kv", "x"), across)
    got_shift.wait()
    for k in range(2):
        xx = x if k == 0 else ox
        for h in range(lh):
            row = jnp.where(xx == 0, shift[h : h + 1, 0:trx], shift[h : h + 1, trx : 2 * trx])
            stat[0, k, 0:1, h * trx : (h + 1) * trx] = (row + log_rows) * LOG2E

    def send_far(ref, kind, k):
        remote(ref.at[0, k], ref.at[1, k], (kind, k), to_far)

    def send_part(i, kind, k):
        remote(qob.at[0, k, i], qob.at[1, k, i], (kind, k), to_far)

    def project_q(k):
        with scope(f"project_q{k}"):
            xx = x if k == 0 else ox
            rows = jnp.dot(flat_rows(nbuf[xx]), wq[...], preferred_element_type=F32).astype(BF16)
            for h in range(lh):
                cols = slice(h * HEAD_DIM, (h + 1) * HEAD_DIM)
                qob[0, k, 0, h * trx : (h + 1) * trx, :] = rows[:, cols]
        send_part(0, "q", k)

    def project_o(k):
        with scope(f"project_o{k}"):
            xx = x if k == 0 else ox
            o_rows = dot_nt(flat_rows(obuf[xx]), wo[...]).astype(BF16)
            for h in range(lh):
                cols = slice(h * HEAD_DIM, (h + 1) * HEAD_DIM)
                qob[0, k, 1, h * trx : (h + 1) * trx, :] = o_rows[:, cols]
        send_part(1, "ob", k)
        with scope(f"drop{k}"):
            keep = saved[pl.ds(pl.multiple_of(xx * trx, trx), trx), :].astype(F32)
            lane = lax.broadcasted_iota(jnp.int32, (trx, HEAD_DIM), 1)
            drops = jnp.zeros((trx, HEAD_DIM), F32)
            for h in range(lh):
                cols = slice(h * HEAD_DIM, (h + 1) * HEAD_DIM)
                term = jnp.sum(o_rows[:, cols].astype(F32) * keep[:, cols], axis=1, keepdims=True)
                drops = jnp.where(lane == h, term, drops)
            drops = jnp.concatenate([drops, jnp.zeros((HEAD_DIM - trx, HEAD_DIM), F32)], axis=0)
            drops = drops.T
            for h in range(lh):
                stat[0, k, 1:2, h * trx : (h + 1) * trx] = drops[h : h + 1, :trx]
        send_far(stat, "st", k)

    def need(k):
        with scope(f"w_q{k}"):
            arrive(qob.at[1, k, 0], ("q", k), to_far)
        with scope(f"w_ob{k}"):
            arrive(qob.at[1, k, 1], ("ob", k), to_far)
            arrive(stat.at[1, k], ("st", k), to_far)

    got = {"kacc": set(), "qacc": set()}

    def attend(v, k, a, g):
        with scope(f"attend_{v}{k}{a}{g}"):
            attend_rows(v, k, a, g, x if g == 0 else ox)

    def attend_last(a, mine):
        with scope(f"last_{a}{mine}"):
            attend_rows(1, 1, a, 2, c if mine else other)

    def attend_rows(v, k, a, g, chip):
        pair = pl.ds(2 * chip, 2)
        sr = kvbuf.shape[2]
        k_rows = kvbuf[a, pair, :, :HEAD_DIM].reshape(2 * sr, HEAD_DIM)
        v_rows = kvbuf[a, pair, :, HEAD_DIM:].reshape(2 * sr, HEAD_DIM)
        queries = qob[v, k, 0]
        backs = qob[v, k, 1]
        score = dot_nt(k_rows, queries)
        prob = jnp.exp2(score * (factor * LOG2E) - stat[v, k, 0:1, :])
        grad = (prob * (dot_nt(v_rows, backs) - stat[v, k, 1:2, :])).astype(BF16)
        key_part = jnp.dot(grad, queries, preferred_element_type=F32)
        value_part = jnp.dot(prob.astype(BF16), backs, preferred_element_type=F32)
        key_part = key_part.reshape(2, sr, HEAD_DIM)
        value_part = value_part.reshape(2, sr, HEAD_DIM)
        if g < 2 and (a, g) not in got["kacc"]:
            kacc[a, pair, :, :HEAD_DIM] = key_part
            kacc[a, pair, :, HEAD_DIM:] = value_part
        else:
            kacc[a, pair, :, :HEAD_DIM] += key_part
            kacc[a, pair, :, HEAD_DIM:] += value_part
        if (v, k) not in got["qacc"]:
            qacc[v, k] = dot_tn(k_rows, grad)
            got["qacc"].add((v, k))
        else:
            qacc[v, k] += dot_tn(k_rows, grad)
        got["kacc"].add((a, g))

    def query_part(v, k):
        return (qacc[v, k] * factor).T

    def send_keys(a):
        with scope(f"keys{a}"):
            for i in range(2):
                slot = 2 * other + i
                kvs[a, i, :, :HEAD_DIM] = (kacc[a, slot, :, :HEAD_DIM] * factor).astype(BF16)
                kvs[a, i, :, HEAD_DIM:] = kacc[a, slot, :, HEAD_DIM:].astype(BF16)
        remote(kvs.at[a], kvr.at[a], ("kp", a), sib)

    def key_sum(a, i):
        block = kacc[a, 2 * c + i]
        k_lane = lax.broadcasted_iota(jnp.int32, block.shape, 1) < HEAD_DIM
        return jnp.where(k_lane, block * factor, block) + kvr[a, i].astype(F32)

    def keys_back():
        with scope("w_kp1"):
            arrive(kvr.at[1], ("kp", 1), sib)
        with scope("kz"):
            for i in range(2):
                kz[i] = key_sum(1, i).astype(BF16)
        remote(kz, kzr, ("kz",), to_peer)

    def slice_from(v):
        return (None, to_far, to_peer, to_diag)[v]

    def slice_pass(v):
        with scope(f"w_na{v}"):
            arrive(nall.at[v, x, c], ("na", v), slice_from(v))
        remote(nall.at[v, x, c], nall.at[v, x, c], ("na", v, "x"), across)
        remote(nall.at[v, x, c], nall.at[v, x, c], ("na", v, "s"), sib)

    def slice_turn(v):
        with scope(f"w_nx{v}"):
            arrive(nall.at[v, ox, c], ("na", v, "x"), across)
        remote(nall.at[v, ox, c], nall.at[v, ox, c], ("na", v, "t"), sib)

    def slice_end(v):
        with scope(f"w_ns{v}"):
            arrive(nall.at[v, x, other], ("na", v, "s"), sib)
            arrive(nall.at[v, ox, other], ("na", v, "t"), sib)

    def total_rows(v, k):
        xx = x if k == 0 else ox
        return qgall.at[v, pl.ds(pl.multiple_of(xx * trx, trx), trx), :]

    pieces = []

    def weight_piece(v):
        with scope(f"piece{v}"):
            piece = dot_tn(flat_rows(nall[v]), qgall[v])
            if not pieces:
                query_weight_grad[...] = piece
            else:
                query_weight_grad[...] += piece
            pieces.append(v)

    step_cols = min(512, width)

    def normed_share():
        with scope("ng_share"):
            for i in range(width // step_cols):
                cols = slice(i * step_cols, (i + 1) * step_cols)
                share = dot_nt(qgall[0], wq[cols, :])
                ngf[:, :, :, cols] = share.reshape(2, 2, nr, step_cols)
            for xx in range(2):
                ngs[xx] = ngf[xx, other].astype(BF16)
        remote(ngs, ngr, ("ng", "s"), sib)

    def normed_cross():
        with scope("w_ngs"):
            arrive(ngr, ("ng", "s"), sib)
        ngx[...] = (ngf[ox, c] + ngr[ox].astype(F32)).astype(BF16)
        remote(ngx, ngin, ("ng", "x"), across)

    def normed_end():
        with scope("w_ngx"):
            arrive(ngin, ("ng", "x"), across)
        with scope("target"):
            grad = ngf[x, c] + ngr[x].astype(F32) + ngin[...].astype(F32)
            scaled = grad * gain[...]
            wide = tgt[...].astype(F32)
            root = jnp.sqrt(jnp.mean(wide * wide, axis=1, keepdims=True) + 1e-06)
            target_grad[...] = scaled / root - wide * jnp.mean(
                scaled * wide, axis=1, keepdims=True
            ) / (root * root * root)

    owner_sends = []

    def keys_out():
        with scope("w_kp0"):
            arrive(kvr.at[0], ("kp", 0), sib)
        with scope("w_kz"):
            arrive(kzr, ("kz",), to_peer)
        with scope("keys_out"):
            for i in range(2):
                block = key_sum(0, i) + kzr[i].astype(F32)
                kfin[i] = block.astype(BF16)
                owner = c * 2 + i
                copy = remote(kfin.at[i], fin.at[x], x, {"tp": owner}, keep=False)
                owner_sends.append((owner, copy))

                @pl.when(owner != t)
                def _():
                    copy.start()

                @pl.when(owner == t)
                def _():
                    fin[x] = kfin[i]

    def source_end():
        for g in range(KV_HEADS):
            giver = g * 2 + t // 2

            @pl.when(giver != t)
            def _():
                with scope("w_fin"):
                    arrive(fin.at[g], ("fin", g), {"tp": giver})

        with scope("source"):
            for i in range(width // step_cols):
                rows = pl.ds(i * step_cols, step_cols)
                part_sum = dot_nt(fin[0], wkv[rows, 0 : 2 * HEAD_DIM])
                for g in range(1, KV_HEADS):
                    part_sum += dot_nt(fin[g], wkv[rows, 2 * g * HEAD_DIM : 2 * (g + 1) * HEAD_DIM])
                source_grad[:, rows] = part_sum

    def pass_on(buf, kind):
        with scope(f"w_{kind}x"):
            arrive(buf.at[ox, c], (kind, "x"), across)
        remote(buf.at[ox, c], buf.at[ox, c], (kind, "t"), sib)

    def passed(buf, kind):
        with scope(f"w_{kind}t"):
            arrive(buf.at[ox, other], (kind, "t"), sib)

    def grad_out(b, k):
        with scope(f"dq_{b}{k}"):
            block = query_part(b, k)
            qfull[b, k] = block
            qsend[b, k] = block.astype(BF16)
        remote(qsend.at[b, k], qrecv.at[1 - b, k], ("dq", 1 - b, k), to_far)

    def total_out(b, k):
        with scope(f"w_dq{b}{k}"):
            arrive(qrecv.at[b, k], ("dq", b, k), to_far)
        with scope(f"total_{b}{k}"):
            total = (qfull[b, k] + qrecv[b, k].astype(F32)).astype(BF16)
            rows = pl.ds(pl.multiple_of((x if k == 0 else ox) * trx, trx), trx)
            for h in range(lh):
                cols = slice(h * HEAD_DIM, (h + 1) * HEAD_DIM)
                qgall[b, rows, cols] = total[h * trx : (h + 1) * trx, :]
        remote(total_rows(b, k), total_rows(2 + b, k), ("tot", b, k), to_peer)

    def total_in(b, k):
        with scope(f"w_tot{b}{k}"):
            arrive(total_rows(2 + b, k), ("tot", b, k), to_peer)

    def peer_keys(chip, kind):
        with scope(f"w_{kind}"):
            arrive(kvbuf.at[1, 2 * chip + c], (kind,), to_peer if chip is x else across)
        remote(kvbuf.at[1, 2 * chip + c], kvbuf.at[1, 2 * chip + c], (kind, "s"), sib)

    def peer_keys_end(chip, kind):
        with scope(f"w_{kind}s"):
            arrive(kvbuf.at[1, 2 * chip + other], (kind, "s"), sib)

    remote(kvown.at[ox], kvpeer, ("kp",), to_peer)
    with scope("w_ns"):
        arrive(nbuf.at[x, other], ("n", "s"), sib)
    got_q.wait()
    project_q(0)
    with scope("w_os"):
        arrive(obuf.at[x, other], ("o", "s"), sib)
    got_w.wait()
    got_saved.wait()
    project_o(0)
    remote(kvown.at[x], kvbuf.at[1, t], ("ke",), to_peer)
    with scope("w_kvs"):
        arrive(kvbuf.at[0, x * 2 + other], ("kv", "s"), sib)
    attend(0, 0, 0, 0)
    pass_on(nbuf, "n")
    passed(nbuf, "n")
    project_q(1)
    pass_on(obuf, "o")
    with scope("w_kpx"):
        arrive(kvpeer, ("kp",), to_peer)
    remote(kvpeer, kvbuf.at[1, t], ("kx",), across)
    passed(obuf, "o")
    project_o(1)
    with scope("w_kvx"):
        arrive(kvbuf.at[0, 2 * ox + c], ("kv", "x"), across)
    remote(kvbuf.at[0, 2 * ox + c], kvbuf.at[0, 2 * ox + c], ("kv", "t"), sib)
    attend(0, 1, 0, 0)
    need(0)
    attend(1, 0, 0, 0)
    with scope("w_kvt"):
        arrive(kvbuf.at[0, 2 * ox + other], ("kv", "t"), sib)
    attend(0, 0, 0, 1)
    attend(1, 0, 0, 1)
    peer_keys(ox, "kx")
    attend(0, 1, 0, 1)
    peer_keys(x, "ke")
    peer_keys_end(ox, "kx")
    attend(1, 0, 1, 1)
    peer_keys_end(x, "ke")
    attend(1, 0, 1, 0)
    grad_out(1, 0)
    attend(0, 0, 1, 0)
    attend(0, 0, 1, 1)
    grad_out(0, 0)
    attend(0, 1, 1, 0)
    attend(0, 1, 1, 1)
    need(1)
    attend_last(1, 0)
    send_keys(1)
    attend_last(1, 1)
    attend_last(0, 0)
    send_keys(0)
    ends = (s == 0) | (s == nS - 1)

    @pl.when(jnp.logical_not(ends))
    def _():
        keys_back()

    attend_last(0, 1)
    grad_out(1, 1)

    @pl.when(ends)
    def _():
        keys_back()

    sent.pop()
    grad_out(0, 1)
    for v in (1, 2, 3):
        slice_pass(v)
    nall[0] = nbuf[:, :, :, pl.ds(pl.multiple_of(s * ds_width, HEAD_DIM), ds_width)]
    total_out(0, 0)
    total_out(1, 0)
    for v in (1, 2, 3):
        slice_turn(v)
    total_out(0, 1)
    normed_share()
    for v in (1, 2, 3):
        slice_end(v)
    weight_piece(0)
    normed_cross()
    total_out(1, 1)
    weight_piece(1)
    keys_out()
    total_in(0, 0)
    total_in(1, 0)
    total_in(0, 1)
    weight_piece(2)
    normed_end()
    source_end()
    total_in(1, 1)
    weight_piece(3)

    with scope("w_send"):
        whole = bulk.at[pl.ds(0, sum(sent) // (bulk.shape[1] * 4))]
        pltpu.make_async_copy(whole, whole, send_sem.at[0]).wait()
        for copy, kept in pending:
            if kept:
                copy.wait_send()
        for owner, copy in owner_sends:

            @pl.when(owner != t)
            def _():
                copy.wait_send()


def square_scratch(nr, width, sr, tr, lh, head_width):
    vm = pltpu.VMEM
    m = lh * tr // 2
    ds_width = width // 4
    kv = 2 * HEAD_DIM
    return [
        vm((nr, width), BF16),
        vm((sr, width), BF16),
        vm((1, width), F32),
        vm((width, head_width), BF16),
        vm((width, KV_HEADS * kv), BF16),
        vm((head_width, width), BF16),
        vm((tr, head_width), BF16),
        vm((lh, tr), F32),
        vm((2, 2, nr, width), BF16),
        vm((2, 2, nr, width), BF16),
        vm((KV_HEADS, sr, kv), BF16),
        vm((2, 4, sr, kv), BF16),
        vm((sr, kv), BF16),
        vm((2, 2, 2, m, HEAD_DIM), BF16),
        vm((2, 2, 2, m), F32),
        vm((4, 2, 2, nr, ds_width), BF16),
        vm((2, 4, sr, kv), F32),
        vm((2, 2, HEAD_DIM, m), F32),
        vm((2, 2, m, HEAD_DIM), F32),
        vm((2, 2, m, HEAD_DIM), BF16),
        vm((2, 2, m, HEAD_DIM), BF16),
        vm((4, tr, head_width), BF16),
        vm((2, 2, nr, width), F32),
        vm((2, nr, width), BF16),
        vm((2, nr, width), BF16),
        vm((nr, width), BF16),
        vm((nr, width), BF16),
        vm((2, 2, sr, kv), BF16),
        vm((2, 2, sr, kv), BF16),
        vm((2, sr, kv), BF16),
        vm((2, sr, kv), BF16),
        vm((2, sr, kv), BF16),
        vm((2, sr, kv), BF16),
        vm((8 * sr, width // 2), F32),
        pltpu.SemaphoreType.DMA((12,)),
        pltpu.SemaphoreType.DMA((6,)),
        pltpu.SemaphoreType.DMA((48,)),
    ]


def shards(
    target,
    source,
    norm_gain,
    query_weight,
    key_weight,
    value_weight,
    output_weight,
    saved_out,
    log_shift,
    out_grad,
):
    nT = lax.axis_size("tp")
    nS = lax.axis_size("sp")
    nA, nB = rows_split(nS)
    nX, nR = nT // 2, nT // KV_HEADS
    nr, width = target.shape
    sr = source.shape[0]
    tr, head_width = saved_out.shape
    lh = head_width // HEAD_DIM
    m = lh * tr // nX
    ds_width = width // nS
    kv = 2 * HEAD_DIM
    log_rows = math.log(sr * nT * nS)
    vm = pltpu.VMEM
    outputs = 4 * (nr * width + sr * width + ds_width * head_width)
    limit = 67043328 - outputs - 65536
    sems = min(8 * nS * nT, 1024)
    scratch = [
        vm((nr, width), BF16),
        vm((sr, width), BF16),
        vm((1, width), F32),
        vm((width, head_width), BF16),
        vm((width, KV_HEADS * kv), BF16),
        vm((head_width, width), BF16),
        vm((tr, head_width), BF16),
        vm((lh, tr), F32),
        vm((nX, 2, nr, width), BF16),
        vm((nX, 2, nr, width), BF16),
        vm((KV_HEADS, sr, kv), BF16),
        vm((nA, nT, sr, kv), BF16),
        vm((nB, nX, 2, m, HEAD_DIM), BF16),
        vm((nB, nX, 2, m), F32),
        vm((nS, nX, 2, nr, ds_width), BF16),
        vm((nA, nT, sr, kv), F32),
        vm((nB, nX, HEAD_DIM, m), F32),
        vm((nB, nX, m, HEAD_DIM), F32),
        vm((nB, nX, m, HEAD_DIM), BF16),
        vm((nB, nB, nX, m, HEAD_DIM), BF16),
        vm((nS, tr, head_width), BF16),
        vm((nX, 2, nr, width), F32),
        vm((nX, nr, width), BF16),
        vm((nX, nr, width), BF16),
        vm((nX, nr, width), BF16),
        vm((nX, nr, width), BF16),
        vm((nA, nT, sr, kv), BF16),
        vm((nR, nA, KV_HEADS, sr, kv), BF16),
        vm((nA, KV_HEADS, sr, kv), BF16),
        vm((nA, KV_HEADS, sr, kv), BF16),
        vm((KV_HEADS, sr, kv), BF16),
        vm((KV_HEADS, sr, kv), BF16),
        vm((KV_HEADS, sr, kv), F32),
        pltpu.SemaphoreType.DMA((16,)),
        pltpu.SemaphoreType.DMA((sems,)),
        pltpu.SemaphoreType.DMA((sems,)),
    ]
    body = functools.partial(kernel, nS, nT, log_rows)
    if nS == 4 and nT == 4:
        body = functools.partial(square_kernel, log_rows)
        scratch = square_scratch(nr, width, sr, tr, lh, head_width)
    anywhere = pl.BlockSpec(memory_space=pltpu.HBM)
    return pl.pallas_call(
        body,
        out_shape=(
            pltpu.VMEM((nr, width), F32),
            pltpu.VMEM((sr, width), F32),
            pltpu.VMEM((ds_width, head_width), F32),
        ),
        in_specs=[anywhere] * 10,
        out_specs=(pl.BlockSpec(memory_space=pltpu.VMEM),) * 3,
        scratch_shapes=scratch,
        compiler_params=pltpu.CompilerParams(
            collective_id=0, has_side_effects=True, vmem_limit_bytes=limit
        ),
        name="cross_back",
    )(
        target,
        source,
        norm_gain.reshape(1, width),
        query_weight,
        key_weight,
        value_weight,
        output_weight,
        saved_out,
        log_shift,
        out_grad,
    )


def solution(mesh):
    return jax.shard_map(
        shards,
        mesh=mesh,
        in_specs=(
            P(("grp", "sp", "tp"), None),
            P(("grp", "sp", "tp"), None),
            P(),
            P(None, "tp"),
            P(),
            P(),
            P("tp", None),
            P(("grp", "sp"), "tp"),
            P("tp", ("grp", "sp")),
            P(("grp", "sp", "tp"), None),
        ),
        out_specs=(
            P(("grp", "sp", "tp"), None),
            P(("grp", "sp", "tp"), None),
            P(("grp", "sp"), "tp"),
        ),
        check_vma=False,
    )
```
